32 devices in a mesh: sp: 4 (over y, x), dp: 8 (over z, core).
Axes of the slice: x: 2, y: 2, z: 4, core: 2. Of those that a mesh axis runs over, the one named last changes fastest.
Arguments:
- tokens: bfloat16 [8, 1024, 2048], P('dp', 'sp'), may hold values from -6 to 6
- key_weight: bfloat16 [2048, 2048], P('dp'), may hold values from -0.125 to 0.125
- queries: bfloat16 [8, 1024, 16, 128], P('dp', None, 'sp'), may hold values from -1.5 to 1.5
- values: bfloat16 [8, 1024, 16, 256], P('dp', None, 'sp'), may hold values from -1.5 to 1.5
- cotangent: bfloat16 [8, 1024, 4096], P('dp', 'sp'), may hold values from -6 to 6
- log_decay: float32 [16], replicated, may hold values from -0.034 to 0, as said below
Outputs:
- grad_tokens: bfloat16 [8, 1024, 2048], P('dp', 'sp')
- grad_queries: bfloat16 [8, 1024, 16, 128], P('dp', None, 'sp')
- grad_values: bfloat16 [8, 1024, 16, 256], P('dp', None, 'sp')
- grad_key_weight: float32 [2048, 2048], P('dp')
The draws below stay inside these ranges and needn't reach their ends.
Inputs may be any that keep to these rules, and one draw needn't show every extreme that they name: `log_decay`: every entry is below zero.
All inputs are finite; a program needn't handle non-finite values.
Results may differ from the reference program's by a relative error of at most 0.0075.
Values may be sent and summed in bfloat16 or wider, within the bound.
A program may use at most 128 MiB of HBM per device.

```python
import jax
import jax.numpy as jnp
from jax import lax

D = 2048
HEADS = 16
KEY_DIM = 128
VALUE_DIM = 256
BLOCK = 128
LENGTH = 1024
SEQS = 8


def draw_log_decay(key, part):
    ranking = jax.random.permutation(jax.random.fold_in(key, 11), HEADS)
    fast_count = HEADS // 2
    spread = jax.random.uniform(jax.random.fold_in(key, 12), (HEADS,), jnp.float32)
    slow_rate = jnp.minimum(jnp.exp(jnp.log(0.2 / LENGTH) + spread * jnp.log(10.0)), 0.01)
    fast_rate = jnp.exp(jnp.log(0.01) + spread * jnp.log(100.0 / 30.0))
    return -jnp.where(ranking < fast_count, fast_rate, slow_rate).astype(jnp.float32)


def raised(result, rng, source, target, shards_of, factor):
    def block_of(dim):
        return (jnp.arange(result.shape[dim]) // (result.shape[dim] // shards_of)).reshape((-1,) + (1,) * (result.ndim - 1 - dim))

    first = jax.random.permutation(rng, shards_of)[block_of(target)]
    second = (block_of(target) + shards_of // 2) % shards_of
    return jnp.where((block_of(source) == first) | (block_of(source) == second), factor * result, result)


def block_scale(own_key, shape, shards, smallest, high):
    gain, own = 1.0, jax.random.fold_in(own_key, 6)
    for axis_at, shards_of in shards:
        heights = jnp.exp(jax.random.uniform(jax.random.fold_in(own, axis_at), (shards_of,), jnp.float32, smallest / len(shards), high / len(shards)))
        gain = gain * jnp.repeat(heights, shape[axis_at] // shards_of).reshape([-1 if axis == axis_at else 1 for axis in range(len(shape))])
    return gain


def gaussian(key, shape, scale, reach, pieces=(), kind=jnp.bfloat16):
    factor_of = block_scale(key, shape, pieces, -0.22, 0.18) if pieces else 1.0
    result = jax.random.normal(key, shape, jnp.float32) * scale * factor_of
    return jnp.minimum(jnp.maximum(result, -reach), reach).astype(kind)


def bell_draw_with(stream_key, extent, deviation, bound, pieces, heavy, kind=jnp.bfloat16):
    result = deviation * jax.random.normal(stream_key, extent, jnp.float32)
    if pieces:
        result = result * block_scale(stream_key, extent, pieces, -0.22, 0.18)
    return jnp.clip(raised(result, jax.random.fold_in(stream_key, 3), *heavy), -bound, bound).astype(kind)


def setup_inputs(seed: int = 0) -> dict:
    arg_keys = jax.random.split(jax.random.key(seed), 7)
    tokens = gaussian(arg_keys[0], (SEQS, LENGTH, D), 1.0, 6.0, ((0, 8), (1, 4)))
    key_weight = gaussian(arg_keys[1], (HEADS * KEY_DIM, D), D ** -0.5, 0.125, ((0, 8),))
    queries = gaussian(arg_keys[2], (SEQS, LENGTH, HEADS, KEY_DIM), 0.1, 1.5, ((0, 8), (2, 4)))
    values = gaussian(arg_keys[3], (SEQS, LENGTH, HEADS, VALUE_DIM), 0.1, 1.5, ((0, 8), (2, 4)))
    cotangent = bell_draw_with(arg_keys[4], (SEQS, LENGTH, HEADS * VALUE_DIM), 1.0, 6.0, ((0, 8), (1, 4)), (0, 2, 8, 2.0))
    log_decay = draw_log_decay(jax.random.fold_in(arg_keys[6], 71), 0)
    return {"tokens": tokens, "key_weight": key_weight, "queries": queries, "values": values, "cotangent": cotangent, "log_decay": log_decay}


def product(form, left, right):
    return jnp.einsum(form, left.astype(jnp.float32), right.astype(jnp.float32))


def rotation(seq_len, half):
    position = jnp.arange(seq_len, dtype=jnp.float32)
    frequency = 10000.0 ** (-jnp.arange(half, dtype=jnp.float32) / half)
    angle = position[:, None] * frequency[None, :]
    return jnp.cos(angle)[:, None, :], jnp.sin(angle)[:, None, :]


def rotate(vectors, cosine, sine):
    half = vectors.shape[-1] // 2
    front, back = vectors[..., :half], vectors[..., half:]
    return jnp.concatenate([front * cosine - back * sine, front * sine + back * cosine], axis=-1)


def unrotate(grads, cosine, sine):
    half = grads.shape[-1] // 2
    front, back = grads[..., :half], grads[..., half:]
    return jnp.concatenate([front * cosine + back * sine, back * cosine - front * sine], axis=-1)


def retention_backward(query_rows, key_rows, value_rows, cotan_rows, head_decay):
    seq_len, heads_here, key_width = query_rows.shape
    nblocks = seq_len // BLOCK
    cosine, sine = rotation(seq_len, key_width // 2)
    factor = key_width ** -0.5
    rot_query = rotate(query_rows.astype(jnp.float32), cosine, sine).astype(jnp.bfloat16)
    rot_key = (rotate(key_rows.astype(jnp.float32), cosine, sine) * factor).astype(jnp.bfloat16)

    def blocks(array):
        return array.reshape(nblocks, BLOCK, heads_here, array.shape[-1])

    block_query, block_key = blocks(rot_query), blocks(rot_key)
    block_value, block_cotan = blocks(value_rows), blocks(cotan_rows)
    inside = jnp.arange(BLOCK, dtype=jnp.float32)
    offset = inside[:, None] - inside[None, :]
    within = jnp.where(offset[None] >= 0, jnp.exp(jnp.maximum(offset, 0.0)[None] * head_decay[:, None, None]), 0.0)
    rising = jnp.exp((inside + 1.0)[:, None] * head_decay[None, :])[None, :, :, None]
    falling = jnp.exp((BLOCK - 1.0 - inside)[:, None] * head_decay[None, :])[None, :, :, None]
    scores = (product("nihd,njhd->nhij", block_query, block_key) * within[None]).astype(jnp.bfloat16)
    mixing = (product("nihe,njhe->nhij", block_cotan, block_value) * within[None]).astype(jnp.bfloat16)
    decayed_queries = (block_query.astype(jnp.float32) * rising).astype(jnp.bfloat16)
    decayed_keys = (block_key.astype(jnp.float32) * falling).astype(jnp.bfloat16)
    block_states = product("nihd,nihe->nhde", decayed_keys, block_value)
    block_trails = product("nihd,nihe->nhde", decayed_queries, block_cotan)
    block_index = jnp.arange(nblocks, dtype=jnp.float32)
    spacing = block_index[:, None] - block_index[None, :] - 1.0
    earlier = jnp.where(spacing[None] >= 0,
                        jnp.exp(jnp.maximum(spacing, 0.0)[None] * BLOCK * head_decay[:, None, None]), 0.0)
    later = jnp.transpose(earlier, (0, 2, 1))
    entering = jnp.einsum("hnm,mhde->nhde", earlier, block_states,
                          precision=lax.Precision.HIGHEST).astype(jnp.bfloat16)
    trailing = jnp.einsum("hnm,mhde->nhde", later, block_trails,
                          precision=lax.Precision.HIGHEST).astype(jnp.bfloat16)
    grad_rq = product("nhij,njhd->nihd", mixing, block_key) + rising * product("nihe,nhde->nihd", block_cotan, entering)
    grad_rk = product("nhij,nihd->njhd", mixing, block_query) + falling * product("nihe,nhde->nihd", block_value, trailing)
    grad_value = product("nhij,nihe->njhe", scores, block_cotan) + falling * product("nihd,nhde->nihe", block_key, trailing)
    grad_rq = grad_rq.reshape(seq_len, heads_here, key_width)
    grad_rk = grad_rk.reshape(seq_len, heads_here, key_width)
    grad_query = unrotate(grad_rq, cosine, sine).astype(jnp.bfloat16)
    grad_key = (unrotate(grad_rk, cosine, sine) * factor).astype(jnp.bfloat16)
    grad_value = grad_value.reshape(seq_len, heads_here, -1).astype(jnp.bfloat16)
    return grad_query, grad_key, grad_value


def reference(tokens, key_weight, queries, values, cotangent, log_decay):
    seq_len = tokens.shape[1]

    def one_sequence(weight_sum, item):
        token_rows, query_rows, value_rows, cotan_rows = item
        key_proj = jnp.dot(token_rows, key_weight.T, preferred_element_type=jnp.float32).astype(jnp.bfloat16)
        grad_query, grad_key, grad_value = retention_backward(
            query_rows, key_proj.reshape(seq_len, HEADS, KEY_DIM), value_rows,
            cotan_rows.reshape(seq_len, HEADS, VALUE_DIM), log_decay)
        key_grads = grad_key.reshape(seq_len, HEADS * KEY_DIM)
        grad_token = jnp.dot(key_grads, key_weight, preferred_element_type=jnp.float32).astype(jnp.bfloat16)
        weight_sum = weight_sum + jnp.dot(key_grads.T, token_rows, preferred_element_type=jnp.float32)
        return weight_sum, (grad_token, grad_query, grad_value)

    start_sum = jnp.zeros((HEADS * KEY_DIM, D), jnp.float32)
    weight_grad, outputs = lax.scan(one_sequence, start_sum, (tokens, queries, values, cotangent))
    return outputs[0], outputs[1], outputs[2], weight_grad
```

```python
import functools

import jax
import jax.numpy as jnp
import numpy as np
from jax import lax
from jax.experimental import pallas as pl
from jax.experimental.pallas import tpu as pltpu
from jax.sharding import PartitionSpec as P

BLOCK = 128
CORES = 2
MESH = pl.DeviceIdType.MESH
F32 = jnp.float32
BF16 = jnp.bfloat16
VMEM_LIMIT = 60 * 1024 * 1024


def rotation_tables(seq_len, half):
    position = np.arange(seq_len, dtype=np.float32)
    frequency = (10000.0 ** (-np.arange(half, dtype=np.float32) / half)).astype(np.float32)
    angle = (position[:, None] * frequency[None, :]).astype(np.float32)
    cosine, sine = np.cos(angle), np.sin(angle)
    return (
        np.concatenate([cosine, cosine], axis=1).astype(np.float32),
        np.concatenate([-sine, sine], axis=1).astype(np.float32),
    )


def dot_nt(a, b):
    return lax.dot_general(a, b, (((1,), (1,)), ((), ())), preferred_element_type=F32)


def dot_tn(a, b):
    return lax.dot_general(a, b, (((0,), (0,)), ((), ())), preferred_element_type=F32)


def dot_nn(a, b):
    return lax.dot_general(a, b, (((1,), (0,)), ((), ())), preferred_element_type=F32)


def retention_kernel(
    decay_ref, q_ref, k_ref, v_ref, c_ref, cos_ref, sin_ref,
    gq_ref, gk_ref, gkt_ref, gv_ref, rq_ref, rk_ref, mix_ref,
):
    seq_len, key_width = q_ref.shape
    value_width = v_ref.shape[1]
    nblocks = seq_len // BLOCK
    half = key_width // 2
    factor = key_width ** (-0.5)
    decay = decay_ref[lax.axis_index("sp") * pl.num_programs(0) + pl.program_id(0)]
    row = lax.broadcasted_iota(jnp.int32, (BLOCK, BLOCK), 0).astype(F32)
    col = lax.broadcasted_iota(jnp.int32, (BLOCK, BLOCK), 1).astype(F32)
    within = jnp.where(row >= col, jnp.exp(jnp.maximum(row - col, 0.0) * decay), 0.0)
    inside = lax.broadcasted_iota(jnp.int32, (BLOCK, key_width), 0).astype(F32)
    rising = jnp.exp((inside + 1.0) * decay)
    falling = jnp.exp((BLOCK - 1.0 - inside) * decay)
    wide = lax.broadcasted_iota(jnp.int32, (BLOCK, value_width), 0).astype(F32)
    falling_wide = jnp.exp((BLOCK - 1.0 - wide) * decay)
    carry_decay = jnp.exp(jnp.full((key_width, value_width), BLOCK * 1.0, F32) * decay)
    zero = jnp.zeros((key_width, value_width), F32)

    def forward(n, entering):
        rows = pl.ds(pl.multiple_of(n * BLOCK, BLOCK), BLOCK)
        cosine, sine = cos_ref[rows, :], sin_ref[rows, :]
        q = q_ref[rows, :].astype(F32)
        k = k_ref[rows, :].astype(F32)
        rq = (q * cosine + pltpu.roll(q, half, 1) * sine).astype(BF16)
        rk = ((k * cosine + pltpu.roll(k, half, 1) * sine) * factor).astype(BF16)
        rq_ref[rows, :] = rq
        rk_ref[rows, :] = rk
        v, c = v_ref[rows, :], c_ref[rows, :]
        mixing = (dot_nt(c, v) * within).astype(BF16)
        mix_ref[rows, :] = mixing
        grad = dot_nn(mixing, rk) + rising * dot_nt(c, entering.astype(BF16))
        gq_ref[rows, :] = (grad * cosine - pltpu.roll(grad, half, 1) * sine).astype(BF16)
        decayed = (rk.astype(F32) * falling).astype(BF16)
        return entering * carry_decay + dot_tn(decayed, v)

    def backward(step, trailing):
        n = nblocks - 1 - step
        rows = pl.ds(pl.multiple_of(n * BLOCK, BLOCK), BLOCK)
        cosine, sine = cos_ref[rows, :], sin_ref[rows, :]
        rq, rk, mixing = rq_ref[rows, :], rk_ref[rows, :], mix_ref[rows, :]
        v, c = v_ref[rows, :], c_ref[rows, :]
        held = trailing.astype(BF16)
        scores = (dot_nt(rq, rk) * within).astype(BF16)
        grad = dot_tn(mixing, rq) + falling * dot_nt(v, held)
        back = (grad * cosine - pltpu.roll(grad, half, 1) * sine) * factor
        gk_ref[rows, :] = back.astype(BF16)
        gkt_ref[:, rows] = back.T.astype(BF16)
        gv_ref[rows, :] = (dot_tn(scores, c) + falling_wide * dot_nn(rk, held)).astype(BF16)
        decayed = (rq.astype(F32) * rising).astype(BF16)
        return trailing * carry_decay + dot_tn(decayed, c)

    unroll = min(nblocks, 8)
    lax.fori_loop(0, nblocks, forward, zero, unroll=unroll)
    lax.fori_loop(0, nblocks, backward, zero, unroll=unroll)


def retention_backward(queries, keys, values, cotan, decay, heads):
    seq_len = queries.shape[0]
    kw = queries.shape[1] // heads
    vw = values.shape[1] // heads
    cosine, sine = rotation_tables(seq_len, kw // 2)
    narrow = pl.BlockSpec((seq_len, kw), lambda h: (0, h))
    wide = pl.BlockSpec((seq_len, vw), lambda h: (0, h))
    table = pl.BlockSpec((seq_len, kw), lambda h: (0, 0))
    flops = 2 * seq_len * heads * BLOCK * (3 * kw + 2 * vw + 5 * vw)
    return pl.pallas_call(
        retention_kernel,
        grid=(heads,),
        in_specs=[pl.BlockSpec(memory_space=pltpu.SMEM), narrow, narrow, wide, wide, table, table],
        out_specs=[narrow, narrow, pl.BlockSpec((kw, seq_len), lambda h: (h, 0)), wide],
        out_shape=[
            jax.ShapeDtypeStruct(queries.shape, BF16),
            jax.ShapeDtypeStruct(queries.shape, BF16),
            jax.ShapeDtypeStruct(queries.shape[::-1], BF16),
            jax.ShapeDtypeStruct(values.shape, BF16),
        ],
        scratch_shapes=[
            pltpu.VMEM((seq_len, kw), BF16),
            pltpu.VMEM((seq_len, kw), BF16),
            pltpu.VMEM((seq_len, BLOCK), BF16),
        ],
        compiler_params=pltpu.CompilerParams(vmem_limit_bytes=VMEM_LIMIT),
        cost_estimate=pl.CostEstimate(
            flops=flops, bytes_accessed=8 * seq_len * heads * (kw + vw), transcendentals=0
        ),
        name="retention",
    )(decay, queries, keys, values, cotan, jnp.asarray(cosine), jnp.asarray(sine))


def remote(src, dst, send, recv, target):
    return pltpu.make_async_remote_copy(
        src_ref=src, dst_ref=dst, send_sem=send, recv_sem=recv,
        device_id=target, device_id_type=MESH,
    )


def greet(nsp, nz, s, z, core):
    barrier = pltpu.get_barrier_semaphore()
    others = [{"dp": z * CORES + 1 - core}]
    others += [{"sp": (s + j) % nsp} for j in range(1, nsp)]
    others += [{"dp": (z + j) % nz * CORES + core} for j in range(1, nz)]
    for other in others:
        pl.semaphore_signal(barrier, inc=1, device_id=other, device_id_type=MESH)
    pl.semaphore_wait(barrier, len(others))


TILE = 256
LANES = 128
COLS = 256


def whole_kernel(
    nsp, nz, heads,
    decay_ref, tok_in, w_in, q_in, v_in, cot_in, cos_in, sin_in,
    gt_out, gq_out, gv_out, gw_out,
    cotv, tall, wall, call, q4, v8, cosv, sinv, rq, vals, mix, held, gk, gkt, gkall,
    keys, gq4, gv8, gt, acc, pwo, rp, lrecv, lsend, fin, xs, ys,
    within, rising, falling, carry, entering,
    load, cot_send, cot_recv, tok_send, tok_recv,
    up_send, up_recv, down_send, down_recv, pair_send, pair_recv,
    gk_send, gk_recv, half_send, half_recv, line_send, line_recv,
    cast_send, cast_recv, gq_store, gv_store, gw_store, gt_store,
):
    s = lax.axis_index("sp")
    k = lax.axis_index("dp")
    z, core = k // CORES, k % CORES
    x, y = s % 2, s // 2
    xn, yn = y * 2 + (1 - x), (1 - y) * 2 + x
    diagonal = (1 - y) * 2 + (1 - x)
    partner = {"dp": z * CORES + 1 - core}
    up, down = {"dp": k + CORES}, {"dp": k - CORES}
    rows, width = tok_in.shape
    wrows = w_in.shape[0]
    seq_len, feats = gk.shape
    kw = feats // heads
    cwidth = call.shape[1]
    vw = cwidth // heads
    parts = vw // LANES
    nblocks = seq_len // BLOCK
    half = kw // 2
    factor = kw ** (-0.5)
    hrows = rows // 2
    nchunks = width // COLS
    pieces = heads
    prow = wrows // pieces

    loads = [
        pltpu.make_async_copy(cot_in, cotv, load.at[0]),
        pltpu.make_async_copy(w_in, wall.at[pl.ds(pl.multiple_of(k * wrows, wrows), wrows), :], load.at[1]),
        pltpu.make_async_copy(tok_in, tall.at[pl.ds(pl.multiple_of(s * rows, rows), rows), :], load.at[2]),
        pltpu.make_async_copy(
            cot_in.at[:, pl.ds(pl.multiple_of(s * cwidth, cwidth), cwidth)],
            call.at[pl.ds(pl.multiple_of(s * rows, rows), rows), :], load.at[3],
        ),
        pltpu.make_async_copy(q_in, q4, load.at[4]),
        pltpu.make_async_copy(v_in, v8, load.at[5]),
        pltpu.make_async_copy(cos_in, cosv, load.at[6]),
        pltpu.make_async_copy(sin_in, sinv, load.at[7]),
    ]
    for copy in loads:
        copy.start()
    greet(nsp, nz, s, z, core)

    def cot_copy(j, h, source):
        peer = (s + j) % nsp
        columns = pl.ds(pl.multiple_of(peer * cwidth + h * vw, vw), vw)
        to = call.at[
            pl.ds(pl.multiple_of(source * rows, rows), rows), pl.ds(pl.multiple_of(h * vw, vw), vw)
        ]
        i = j * heads + h
        return remote(cotv.at[:, columns], to, cot_send.at[i], cot_recv.at[i], {"sp": peer})

    loads[0].wait()
    for h in range(heads):
        for j in range(1, nsp):
            cot_copy(j, h, s).start()

    def piece(zb, c, p):
        start = pl.multiple_of((zb * CORES + c) * wrows + p * prow, prow)
        return wall.at[pl.ds(start, prow), :]

    def up_copy(d, p):
        ref, i = piece(z - d, core, p), d * pieces + p
        return remote(ref, ref, up_send.at[i], up_recv.at[i], up)

    def down_copy(d, p):
        ref, i = piece(z + d, core, p), d * pieces + p
        return remote(ref, ref, down_send.at[i], down_recv.at[i], down)

    def up_arrival(d, p):
        ref, i = piece(z - d, core, p), (d - 1) * pieces + p
        return remote(ref, ref, up_send.at[i], up_recv.at[i], partner)

    def down_arrival(d, p):
        ref, i = piece(z + d, core, p), (d - 1) * pieces + p
        return remote(ref, ref, down_send.at[i], down_recv.at[i], partner)

    def pair_copy(zb, p):
        ref, i = piece(zb, core, p), zb * pieces + p
        return remote(ref, ref, pair_send.at[i], pair_recv.at[i], partner)

    def pair_arrival(zb, p):
        ref, i = piece(zb, 1 - core, p), zb * pieces + p
        return remote(ref, ref, pair_send.at[i], pair_recv.at[i], partner)

    loads[1].wait()
    for p in range(pieces):
        @pl.when(z < nz - 1)
        def _():
            up_copy(0, p).start()

        @pl.when(z > 0)
        def _():
            down_copy(0, p).start()

        pair_copy(z, p).start()

    def relay(d, p):
        @pl.when(z >= d)
        def _():
            up_arrival(d, p).wait_recv()
            if d < nz - 1:
                @pl.when(z < nz - 1)
                def _():
                    up_copy(d, p).start()
            pair_copy(z - d, p).start()

        @pl.when(z + d < nz)
        def _():
            down_arrival(d, p).wait_recv()
            if d < nz - 1:
                @pl.when(z > 0)
                def _():
                    down_copy(d, p).start()
            pair_copy(z + d, p).start()

    def token(j, i, who, h, target):
        at = tall.at[
            pl.ds(pl.multiple_of(who * rows + h * hrows, hrows), hrows),
            pl.ds(pl.multiple_of(j * COLS, COLS), COLS),
        ]
        n = j * 6 + i
        return remote(at, at, tok_send.at[n], tok_recv.at[n], {"sp": target})

    def token_send(j, i):
        who, h, target = [
            (s, 0, xn), (s, 1, yn), (s, 1, xn), (s, 0, yn), (xn, 0, yn), (yn, 1, xn)
        ][i]
        return token(j, i, who, h, target)

    def token_arrival(j, i):
        who, h, target = [
            (xn, 0, xn), (yn, 1, yn), (xn, 1, xn), (yn, 0, yn), (diagonal, 0, yn), (diagonal, 1, xn)
        ][i]
        return token(j, i, who, h, target)

    loads[2].wait()
    for i in range(4):
        token_send(0, i).start()
    for copy in loads[3:]:
        copy.wait()

    def prepare(n, _):
        at = pl.ds(pl.multiple_of(n * BLOCK, BLOCK), BLOCK)
        cosine, sine = cosv[at, :], sinv[at, :]
        span = BLOCK * heads
        xs[...] = q4[pl.ds(pl.multiple_of(n * span, span), span), :].astype(F32)
        for h in range(heads):
            q = xs[pl.ds(h, BLOCK, stride=heads), :]
            rq[at, h * kw:(h + 1) * kw] = (q * cosine + pltpu.roll(q, half, 1) * sine).astype(BF16)
        span = BLOCK * heads * parts
        ys[...] = v8[pl.ds(pl.multiple_of(n * span, span), span), :].astype(F32)
        for h in range(heads):
            for i in range(parts):
                left = h * vw + i * LANES
                vals[at, left:left + LANES] = ys[
                    pl.ds(i * heads + h, BLOCK, stride=heads * parts), :
                ].astype(BF16)
        return 0

    lax.fori_loop(0, nblocks, prepare, 0)

    def key_head(h, _):
        relay(1, h)
        for j in range(1, nsp):
            cot_copy(j, h, (s - j + nsp) % nsp).wait_recv()
        kc = pl.ds(pl.multiple_of(h * kw, kw), kw)
        vc = pl.ds(pl.multiple_of(h * vw, vw), vw)
        decay = decay_ref[s * heads + h]
        row = lax.broadcasted_iota(jnp.int32, (BLOCK, BLOCK), 0).astype(F32)
        col = lax.broadcasted_iota(jnp.int32, (BLOCK, BLOCK), 1).astype(F32)
        inside = lax.broadcasted_iota(jnp.int32, (BLOCK, kw), 0).astype(F32)
        mask = jnp.where(row >= col, jnp.exp(jnp.maximum(row - col, 0.0) * decay), 0.0)
        rise = jnp.exp((inside + 1.0) * decay)
        fall = jnp.exp((BLOCK - 1.0 - inside) * decay)
        step = jnp.exp(jnp.full((8, vw), BLOCK * 1.0, F32) * decay)
        within[h] = mask
        rising[h] = rise
        falling[h] = fall
        carry[h] = step
        trailing = jnp.zeros((kw, vw), F32)
        for n in reversed(range(nblocks)):
            at = slice(n * BLOCK, (n + 1) * BLOCK)
            cosine, sine = cosv[at, :], sinv[at, :]
            q, v, c = rq[at, kc], vals[at, vc], call[at, vc]
            mixing = (dot_nt(c, v) * mask).astype(BF16)
            mix[at, pl.ds(pl.multiple_of(h * BLOCK, BLOCK), BLOCK)] = mixing
            trail = trailing.astype(BF16)
            held[h * nblocks + n] = trail
            grad = dot_tn(mixing, q) + fall * dot_nt(v, trail)
            back = (grad * cosine - pltpu.roll(grad, half, 1) * sine) * factor
            gk[at, kc] = back.astype(BF16)
            gkt[kc, at] = back.T.astype(BF16)
            decayed = (q.astype(F32) * rise).astype(BF16)
            trailing = trailing * step[0:1, :] + dot_tn(decayed, c)
        entering[h] = jnp.zeros((kw, vw), F32)
        return 0

    lax.fori_loop(0, heads, key_head, 0)

    def gk_copy(j, source):
        peer = (s + j) % nsp
        to = gkall.at[:, pl.ds(pl.multiple_of(source * feats, feats), feats)]
        return remote(
            gk.at[pl.ds(pl.multiple_of(peer * rows, rows), rows), :], to,
            gk_send.at[j], gk_recv.at[j], {"sp": peer},
        )

    def half_copy(j):
        return remote(pwo.at[j], rp.at[j], half_send.at[j], half_recv.at[j], partner)

    def line_copy(j, side, target):
        return remote(
            lsend.at[j], lrecv.at[side, j], line_send.at[j],
            line_recv.at[side * nchunks + j], target,
        )

    def cast_copy(j, h, target):
        ref = fin.at[j, pl.ds(h * (wrows // 2), wrows // 2), :]
        i = 2 * j + h
        return remote(ref, ref, cast_send.at[i], cast_recv.at[i], {"sp": target})

    far = jnp.maximum(z, nz - 1 - z)
    behind = jnp.where(z > s, nz - 1 - z, jnp.where(z < s, z, far))
    owner = z == s
    dx, dy = x != z % 2, y != z // 2
    on_x = dx & jnp.logical_not(dy)
    on_y = dy & jnp.logical_not(dx)
    on_d = dx & dy
    apart = jnp.maximum(z - s, s - z)
    key_step = jnp.where(apart == nz - 1, nchunks + 2, nchunks)

    def gradient_columns(j):
        for i in range(2, 6):
            token_arrival(j, i).wait_recv()
        at = pl.ds(pl.multiple_of(j * COLS, COLS), COLS)
        theirs = pl.ds(pl.multiple_of((1 - core) * wrows, wrows), wrows)
        mine = pl.ds(pl.multiple_of(core * wrows, wrows), wrows)
        pwo[j] = dot_nn(gkt[theirs, :], tall[:, at]).astype(BF16)
        half_copy(j).start()
        acc[j] = dot_nn(gkt[mine, :], tall[:, at])

    def sum_line(j):
        half_copy(j).wait_recv()
        acc[j] = acc[j] + rp[j].astype(F32)

        @pl.when((z >= s) & (z < nz - 1))
        def _():
            line_copy(j, 1, down).wait_recv()
            acc[j] = acc[j] + lrecv[1, j].astype(F32)

        @pl.when((z <= s) & (z > 0))
        def _():
            line_copy(j, 0, up).wait_recv()
            acc[j] = acc[j] + lrecv[0, j].astype(F32)

        @pl.when(owner)
        def _():
            fin[j] = acc[j].astype(BF16)
            cast_copy(j, 0, xn).start()
            cast_copy(j, 1, yn).start()

        @pl.when(jnp.logical_not(owner))
        def _():
            lsend[j] = acc[j].astype(BF16)

        @pl.when(z > s)
        def _():
            line_copy(j, 1, down).start()

        @pl.when(z < s)
        def _():
            line_copy(j, 0, up).start()

    def make_keys():
        for p in range(pieces):
            pair_arrival(s, p).wait_recv()
        left = pl.ds(pl.multiple_of(s * feats, feats), feats)

        def tile(i, _):
            at = pl.ds(pl.multiple_of(i * TILE, TILE), TILE)
            keys[at, :] = dot_nt(tall[at, :], wall[left, :]).astype(BF16)
            return 0

        lax.fori_loop(0, seq_len // TILE, tile, 0)

    def gq_copy(n):
        span = BLOCK * heads
        at = pl.ds(pl.multiple_of(n * span, span), span)
        return pltpu.make_async_copy(gq4.at[at, :], gq_out.at[at, :], gq_store.at[n])

    def gv_copy(n):
        span = BLOCK * heads * parts
        at = pl.ds(pl.multiple_of(n * span, span), span)
        return pltpu.make_async_copy(gv8.at[at, :], gv_out.at[at, :], gv_store.at[n])

    def query_block(n):
        at = pl.ds(pl.multiple_of(n * BLOCK, BLOCK), BLOCK)
        cosine, sine = cosv[at, :], sinv[at, :]
        for h in range(heads):
            kc, vc = slice(h * kw, (h + 1) * kw), slice(h * vw, (h + 1) * vw)
            key = keys[at, kc].astype(F32)
            rk = ((key * cosine + pltpu.roll(key, half, 1) * sine) * factor).astype(BF16)
            q, v, c = rq[at, kc], vals[at, vc], call[at, vc]
            state = entering[h]
            grad = dot_nn(mix[at, h * BLOCK:(h + 1) * BLOCK], rk)
            grad = grad + rising[h] * dot_nt(c, state.astype(BF16))
            xs[pl.ds(h, BLOCK, stride=heads), :] = (
                grad * cosine - pltpu.roll(grad, half, 1) * sine
            )
            scores = (dot_nt(q, rk) * within[h]).astype(BF16)
            fall = falling[h]
            inner = dot_tn(scores, c)
            outer = dot_nn(rk, held[h * nblocks + n])
            for i in range(parts):
                lane = slice(i * LANES, (i + 1) * LANES)
                ys[pl.ds(i * heads + h, BLOCK, stride=heads * parts), :] = (
                    inner[:, lane] + fall * outer[:, lane]
                )
            decayed = (rk.astype(F32) * fall).astype(BF16)
            entering[h] = state * carry[h, 0:1, :] + dot_tn(decayed, v)
        span = BLOCK * heads
        gq4[pl.ds(pl.multiple_of(n * span, span), span), :] = xs[...].astype(BF16)
        span = BLOCK * heads * parts
        gv8[pl.ds(pl.multiple_of(n * span, span), span), :] = ys[...].astype(BF16)
        gq_copy(n).start()
        gv_copy(n).start()

    def token_gradient():
        for j in range(1, nsp):
            gk_copy(j, (s - j + nsp) % nsp).wait_recv()
        gkall[:, pl.ds(pl.multiple_of(s * feats, feats), feats)] = gk[
            pl.ds(pl.multiple_of(s * rows, rows), rows), :
        ]
        for zb in range(nz):
            @pl.when(zb != s)
            def _():
                for p in range(pieces):
                    pair_arrival(zb, p).wait_recv()

        def tile(i, _):
            at = pl.ds(pl.multiple_of(i * TILE, TILE), TILE)
            gt[:, at] = dot_nn(gkall[...], wall[:, at]).astype(BF16)
            return 0

        lax.fori_loop(0, width // TILE, tile, 0)
        pltpu.make_async_copy(gt, gt_out, gt_store.at[0]).start()

    last = nchunks + 3 + (nz - 1)

    def turn(t, _):
        @pl.when(t + 1 < nchunks)
        def _():
            for i in range(4):
                token_send(t + 1, i).start()

        @pl.when(t < nchunks)
        def _():
            token_arrival(t, 0).wait_recv()
            token_send(t, 4).start()
            token_arrival(t, 1).wait_recv()
            token_send(t, 5).start()

        @pl.when(t == nchunks - 1)
        def _():
            for j in range(1, nsp):
                gk_copy(j, s).start()

        @pl.when((t >= 1) & (t <= nchunks))
        def _():
            gradient_columns(t - 1)

        j = t - 2 - behind

        @pl.when((j >= 0) & (j < nchunks))
        def _():
            sum_line(j)

        jx = t - 3 - far

        @pl.when(on_x & (jx >= 0) & (jx < nchunks))
        def _():
            cast_copy(jx, 0, xn).wait_recv()
            cast_copy(jx, 0, yn).start()

        @pl.when(on_y & (jx >= 0) & (jx < nchunks))
        def _():
            cast_copy(jx, 1, yn).wait_recv()
            cast_copy(jx, 1, xn).start()

        jd = t - 4 - far

        @pl.when(on_d & (jd >= 0) & (jd < nchunks))
        def _():
            cast_copy(jd, 0, yn).wait_recv()
            cast_copy(jd, 0, xn).start()
            cast_copy(jd, 1, xn).wait_recv()
            cast_copy(jd, 1, yn).start()

        @pl.when((t >= 1) & (t <= pieces))
        def _():
            relay(2, t - 1)

        @pl.when((t >= nchunks + 3 - pieces) & (t < nchunks + 3))
        def _():
            relay(3, t - (nchunks + 3 - pieces))

        @pl.when(t == key_step)
        def _():
            make_keys()

        n = (t - key_step - 1) * 2

        @pl.when((n >= 0) & (n < nblocks))
        def _():
            query_block(n)
            query_block(n + 1)

        @pl.when(t == last - 1)
        def _():
            token_gradient()

        return 0

    lax.fori_loop(0, last + 1, turn, 0)

    def gw_copy(j):
        at = pl.ds(pl.multiple_of(j * COLS, COLS), COLS)
        return pltpu.make_async_copy(fin.at[j], gw_out.at[:, at], gw_store.at[j])

    def finish(j, _):
        @pl.when(on_x)
        def _():
            cast_copy(j, 1, xn).wait_recv()

        @pl.when(on_y)
        def _():
            cast_copy(j, 0, yn).wait_recv()

        gw_copy(j).start()
        return 0

    lax.fori_loop(0, nchunks, finish, 0)

    for h in range(heads):
        for j in range(1, nsp):
            cot_copy(j, h, s).wait_send()
    for j in range(1, nsp):
        gk_copy(j, s).wait_send()

    def settle(j, _):
        for i in range(6):
            token_send(j, i).wait_send()
        half_copy(j).wait_send()

        @pl.when(jnp.logical_not(owner))
        def _():
            line_copy(j, 0, partner).wait_send()

        @pl.when(jnp.logical_not(on_y))
        def _():
            cast_copy(j, 0, xn).wait_send()

        @pl.when(jnp.logical_not(on_x))
        def _():
            cast_copy(j, 1, xn).wait_send()

        gw_copy(j).wait()
        return 0

    lax.fori_loop(0, nchunks, settle, 0)

    for p in range(pieces):
        for d in range(nz - 1):
            @pl.when((z >= d) & (z < nz - 1))
            def _():
                up_copy(d, p).wait_send()

            @pl.when((z + d < nz) & (z > 0))
            def _():
                down_copy(d, p).wait_send()

        for zb in range(nz):
            pair_copy(zb, p).wait_send()

    def drain(n, _):
        gq_copy(n).wait()
        gv_copy(n).wait()
        return 0

    lax.fori_loop(0, nblocks, drain, 0)
    pltpu.make_async_copy(gt, gt_out, gt_store.at[0]).wait()


def whole(tokens, weight, queries, values, cotan, decay, nsp, ndp, heads):
    nz = ndp // CORES
    rows, width = tokens.shape
    wrows = weight.shape[0]
    seq_len = rows * nsp
    kw = queries.shape[1]
    feats = heads * kw
    cwidth = cotan.shape[1] // nsp
    vw = cwidth // heads
    nblocks = seq_len // BLOCK
    nchunks = width // COLS
    cosine, sine = rotation_tables(seq_len, kw // 2)
    dma = pltpu.SemaphoreType.DMA
    anywhere = pl.BlockSpec(memory_space=pl.ANY)

    def buffer(*shape):
        return pltpu.VMEM(shape, BF16)

    def wide(*shape):
        return pltpu.VMEM(shape, F32)

    return pl.pallas_call(
        functools.partial(whole_kernel, nsp, nz, heads),
        in_specs=[pl.BlockSpec(memory_space=pltpu.SMEM)] + [anywhere] * 7,
        out_specs=[anywhere] * 4,
        out_shape=[
            jax.ShapeDtypeStruct((rows, width), BF16),
            jax.ShapeDtypeStruct(queries.shape, BF16),
            jax.ShapeDtypeStruct(values.shape, BF16),
            jax.ShapeDtypeStruct((wrows, width), BF16),
        ],
        scratch_shapes=[
            buffer(rows, nsp * cwidth),
            buffer(seq_len, width),
            buffer(wrows * ndp, width),
            buffer(seq_len, cwidth),
            buffer(*queries.shape),
            buffer(*values.shape),
            wide(seq_len, kw),
            wide(seq_len, kw),
            buffer(seq_len, feats),
            buffer(seq_len, cwidth),
            buffer(seq_len, heads * BLOCK),
            buffer(heads * nblocks, kw, vw),
            buffer(seq_len, feats),
            buffer(feats, seq_len),
            buffer(rows, nsp * feats),
            buffer(seq_len, feats),
            buffer(*queries.shape),
            buffer(*values.shape),
            buffer(rows, width),
            wide(nchunks, wrows, COLS),
            buffer(nchunks, wrows, COLS),
            buffer(nchunks, wrows, COLS),
            buffer(2, nchunks, wrows, COLS),
            buffer(nchunks, wrows, COLS),
            buffer(nchunks, wrows, COLS),
            wide(BLOCK * heads, kw),
            wide(BLOCK * heads * (vw // LANES), LANES),
            wide(heads, BLOCK, BLOCK),
            wide(heads, BLOCK, kw),
            wide(heads, BLOCK, kw),
            wide(heads, 8, vw),
            wide(heads, kw, vw),
            dma((8,)),
            dma((nsp * heads,)), dma((nsp * heads,)),
            dma((6 * nchunks,)), dma((6 * nchunks,)),
            dma((nz * heads,)), dma((nz * heads,)),
            dma((nz * heads,)), dma((nz * heads,)),
            dma((nz * heads,)), dma((nz * heads,)),
            dma((nsp,)), dma((nsp,)),
            dma((nchunks,)), dma((nchunks,)),
            dma((nchunks,)), dma((2 * nchunks,)),
            dma((2 * nchunks,)), dma((2 * nchunks,)),
            dma((nblocks,)), dma((nblocks,)), dma((nchunks,)), dma((1,)),
        ],
        compiler_params=pltpu.CompilerParams(
            has_side_effects=True, vmem_limit_bytes=VMEM_LIMIT, collective_id=0
        ),
        name="whole",
    )(decay, tokens, weight, queries, values, cotan, jnp.asarray(cosine), jnp.asarray(sine))


def gather_general(tokens, weight, cotan):
    gathered = lax.all_gather(weight, "dp", axis=0, tiled=True)
    rows = gathered.shape[0] // lax.axis_size("sp")
    chosen = lax.dynamic_slice_in_dim(gathered, lax.axis_index("sp") * rows, rows)
    return (
        lax.all_gather(tokens, "sp", axis=0, tiled=True),
        chosen,
        lax.all_to_all(cotan, "sp", split_axis=1, concat_axis=0, tiled=True),
    )


def scatter_general(partial_tokens, partial_weight):
    grad_tokens = lax.psum_scatter(
        partial_tokens, "sp", scatter_dimension=0, tiled=True
    ).astype(BF16)
    owned = lax.psum_scatter(
        partial_weight, "dp", scatter_dimension=0, tiled=True
    )
    everything = lax.all_gather(owned, ("sp", "dp"), axis=0, tiled=True)
    rows = everything.shape[0] // lax.axis_size("dp")
    return grad_tokens, lax.dynamic_slice_in_dim(
        everything, lax.axis_index("dp") * rows, rows
    )


def body(nsp, ndp, tokens, key_weight, queries, values, cotangent, log_decay):
    seq_len, heads, kw = queries.shape[1:]
    vw = values.shape[3]
    if nsp == 4 and ndp == CORES * nsp and kw == BLOCK:
        parts = vw // LANES
        flat = values.reshape(seq_len, heads, parts, LANES).transpose(0, 2, 1, 3)
        grad_tokens, grad_query, grad_value, weight_grad = whole(
            tokens[0], key_weight, queries.reshape(-1, kw), flat.reshape(-1, LANES),
            cotangent[0], log_decay, nsp, ndp, heads,
        )
        grad_value = grad_value.reshape(seq_len, parts, heads, LANES).transpose(0, 2, 1, 3)
        weight_grad = weight_grad.astype(F32)
    else:
        all_tokens, weight, cotan = gather_general(tokens[0], key_weight, cotangent[0])
        keys = dot_nt(all_tokens, weight).astype(BF16)
        grad_query, grad_key, _, grad_value = retention_backward(
            queries.reshape(seq_len, -1), keys, values.reshape(seq_len, -1), cotan, log_decay, heads
        )
        grad_tokens, weight_grad = scatter_general(
            dot_nn(grad_key, weight), dot_tn(grad_key, all_tokens)
        )
    return (
        grad_tokens[None],
        grad_query.reshape(queries.shape),
        grad_value.reshape(values.shape),
        weight_grad,
    )


def solution(mesh):
    return jax.shard_map(
        functools.partial(body, mesh.shape["sp"], mesh.shape["dp"]),
        mesh=mesh,
        in_specs=(
            P("dp", "sp", None),
            P("dp", None),
            P("dp", None, "sp", None),
            P("dp", None, "sp", None),
            P("dp", "sp", None),
            P(),
        ),
        out_specs=(
            P("dp", "sp", None),
            P("dp", None, "sp", None),
            P("dp", None, "sp", None),
            P("dp", None),
        ),
        check_vma=False,
    )
```

```python
import functools

import jax
import jax.numpy as jnp
import numpy as np
from jax import lax
from jax.experimental import pallas as pl
from jax.experimental.pallas import tpu as pltpu
from jax.sharding import PartitionSpec as P

BLOCK = 128
CORES = 2
MESH = pl.DeviceIdType.MESH
F32 = jnp.float32
BF16 = jnp.bfloat16
VMEM_LIMIT = 60 * 1024 * 1024


def rotation_tables(seq_len, half):
    position = np.arange(seq_len, dtype=np.float32)
    frequency = (10000.0 ** (-np.arange(half, dtype=np.float32) / half)).astype(np.float32)
    angle = (position[:, None] * frequency[None, :]).astype(np.float32)
    cosine, sine = np.cos(angle), np.sin(angle)
    return (
        np.concatenate([cosine, cosine], axis=1).astype(np.float32),
        np.concatenate([-sine, sine], axis=1).astype(np.float32),
    )


def dot_nt(a, b):
    return lax.dot_general(a, b, (((1,), (1,)), ((), ())), preferred_element_type=F32)


def dot_tn(a, b):
    return lax.dot_general(a, b, (((0,), (0,)), ((), ())), preferred_element_type=F32)


def dot_nn(a, b):
    return lax.dot_general(a, b, (((1,), (0,)), ((), ())), preferred_element_type=F32)


def retention_kernel(
    decay_ref, q_ref, k_ref, v_ref, c_ref, cos_ref, sin_ref,
    gq_ref, gk_ref, gkt_ref, gv_ref, rq_ref, rk_ref, mix_ref,
):
    seq_len, key_width = q_ref.shape
    value_width = v_ref.shape[1]
    nblocks = seq_len // BLOCK
    half = key_width // 2
    factor = key_width ** (-0.5)
    decay = decay_ref[lax.axis_index("sp") * pl.num_programs(0) + pl.program_id(0)]
    row = lax.broadcasted_iota(jnp.int32, (BLOCK, BLOCK), 0).astype(F32)
    col = lax.broadcasted_iota(jnp.int32, (BLOCK, BLOCK), 1).astype(F32)
    within = jnp.where(row >= col, jnp.exp(jnp.maximum(row - col, 0.0) * decay), 0.0)
    inside = lax.broadcasted_iota(jnp.int32, (BLOCK, key_width), 0).astype(F32)
    rising = jnp.exp((inside + 1.0) * decay)
    falling = jnp.exp((BLOCK - 1.0 - inside) * decay)
    wide = lax.broadcasted_iota(jnp.int32, (BLOCK, value_width), 0).astype(F32)
    falling_wide = jnp.exp((BLOCK - 1.0 - wide) * decay)
    carry_decay = jnp.exp(jnp.full((key_width, value_width), BLOCK * 1.0, F32) * decay)
    zero = jnp.zeros((key_width, value_width), F32)

    def forward(n, entering):
        rows = pl.ds(pl.multiple_of(n * BLOCK, BLOCK), BLOCK)
        cosine, sine = cos_ref[rows, :], sin_ref[rows, :]
        q = q_ref[rows, :].astype(F32)
        k = k_ref[rows, :].astype(F32)
        rq = (q * cosine + pltpu.roll(q, half, 1) * sine).astype(BF16)
        rk = ((k * cosine + pltpu.roll(k, half, 1) * sine) * factor).astype(BF16)
        rq_ref[rows, :] = rq
        rk_ref[rows, :] = rk
        v, c = v_ref[rows, :], c_ref[rows, :]
        mixing = (dot_nt(c, v) * within).astype(BF16)
        mix_ref[rows, :] = mixing
        grad = dot_nn(mixing, rk) + rising * dot_nt(c, entering.astype(BF16))
        gq_ref[rows, :] = (grad * cosine - pltpu.roll(grad, half, 1) * sine).astype(BF16)
        decayed = (rk.astype(F32) * falling).astype(BF16)
        return entering * carry_decay + dot_tn(decayed, v)

    def backward(step, trailing):
        n = nblocks - 1 - step
        rows = pl.ds(pl.multiple_of(n * BLOCK, BLOCK), BLOCK)
        cosine, sine = cos_ref[rows, :], sin_ref[rows, :]
        rq, rk, mixing = rq_ref[rows, :], rk_ref[rows, :], mix_ref[rows, :]
        v, c = v_ref[rows, :], c_ref[rows, :]
        held = trailing.astype(BF16)
        scores = (dot_nt(rq, rk) * within).astype(BF16)
        grad = dot_tn(mixing, rq) + falling * dot_nt(v, held)
        back = (grad * cosine - pltpu.roll(grad, half, 1) * sine) * factor
        gk_ref[rows, :] = back.astype(BF16)
        gkt_ref[:, rows] = back.T.astype(BF16)
        gv_ref[rows, :] = (dot_tn(scores, c) + falling_wide * dot_nn(rk, held)).astype(BF16)
        decayed = (rq.astype(F32) * rising).astype(BF16)
        return trailing * carry_decay + dot_tn(decayed, c)

    unroll = min(nblocks, 8)
    lax.fori_loop(0, nblocks, forward, zero, unroll=unroll)
    lax.fori_loop(0, nblocks, backward, zero, unroll=unroll)


def retention_backward(queries, keys, values, cotan, decay, heads):
    seq_len = queries.shape[0]
    kw = queries.shape[1] // heads
    vw = values.shape[1] // heads
    cosine, sine = rotation_tables(seq_len, kw // 2)
    narrow = pl.BlockSpec((seq_len, kw), lambda h: (0, h))
    wide = pl.BlockSpec((seq_len, vw), lambda h: (0, h))
    table = pl.BlockSpec((seq_len, kw), lambda h: (0, 0))
    flops = 2 * seq_len * heads * BLOCK * (3 * kw + 2 * vw + 5 * vw)
    return pl.pallas_call(
        retention_kernel,
        grid=(heads,),
        in_specs=[pl.BlockSpec(memory_space=pltpu.SMEM), narrow, narrow, wide, wide, table, table],
        out_specs=[narrow, narrow, pl.BlockSpec((kw, seq_len), lambda h: (h, 0)), wide],
        out_shape=[
            jax.ShapeDtypeStruct(queries.shape, BF16),
            jax.ShapeDtypeStruct(queries.shape, BF16),
            jax.ShapeDtypeStruct(queries.shape[::-1], BF16),
            jax.ShapeDtypeStruct(values.shape, BF16),
        ],
        scratch_shapes=[
            pltpu.VMEM((seq_len, kw), BF16),
            pltpu.VMEM((seq_len, kw), BF16),
            pltpu.VMEM((seq_len, BLOCK), BF16),
        ],
        compiler_params=pltpu.CompilerParams(vmem_limit_bytes=VMEM_LIMIT),
        cost_estimate=pl.CostEstimate(
            flops=flops, bytes_accessed=8 * seq_len * heads * (kw + vw), transcendentals=0
        ),
        name="retention",
    )(decay, queries, keys, values, cotan, jnp.asarray(cosine), jnp.asarray(sine))


def remote(src, dst, send, recv, target):
    return pltpu.make_async_remote_copy(
        src_ref=src, dst_ref=dst, send_sem=send, recv_sem=recv,
        device_id=target, device_id_type=MESH,
    )


def greet(nsp, nz, s, z, core):
    barrier = pltpu.get_barrier_semaphore()
    others = [{"dp": z * CORES + 1 - core}]
    others += [{"sp": (s + j) % nsp} for j in range(1, nsp)]
    for other in others:
        pl.semaphore_signal(barrier, inc=1, device_id=other, device_id_type=MESH)

    @pl.when(z > 0)
    def _():
        below = {"dp": (z - 1) * CORES + core}
        pl.semaphore_signal(barrier, inc=1, device_id=below, device_id_type=MESH)

    @pl.when(z < nz - 1)
    def _():
        above = {"dp": (z + 1) * CORES + core}
        pl.semaphore_signal(barrier, inc=1, device_id=above, device_id_type=MESH)

    ends = jnp.where(z > 0, 1, 0) + jnp.where(z < nz - 1, 1, 0)
    pl.semaphore_wait(barrier, len(others) + ends)


TILE = 256
LANES = 128
COLS = 256
HOP = 1


def whole_kernel(
    nsp, nz, heads,
    decay_ref, tok_in, w_in, q_in, v_in, cot_in, cos_in, sin_in,
    gt_out, gq_out, gv_out, gw_out,
    cotv, tall, wall, call, q4, v8, cosv, sinv, rq, vals, mix, held, gk, gkt, gkall,
    keys, gq4, gv8, gt, gtf, acc, pwo, rp, lrecv, lsend, fin, xs, ys,
    within, rising, falling, carry, entering,
    load, cot_send, cot_recv, tok_send, tok_recv,
    up_send, up_recv, down_send, down_recv, pair_send, pair_recv, side_send, side_recv,
    gk_send, gk_recv, half_send, half_recv, line_send, line_recv,
    cast_send, cast_recv, gq_store, gv_store, gw_store, gt_store,
):
    s = lax.axis_index("sp")
    k = lax.axis_index("dp")
    z, core = k // CORES, k % CORES
    x, y = s % 2, s // 2
    xn, yn = y * 2 + (1 - x), (1 - y) * 2 + x
    diagonal = (1 - y) * 2 + (1 - x)
    partner = {"dp": z * CORES + 1 - core}
    up, down = {"dp": k + CORES}, {"dp": k - CORES}
    rows, width = tok_in.shape
    wrows = w_in.shape[0]
    seq_len, feats = gk.shape
    kw = feats // heads
    cwidth = call.shape[1]
    vw = cwidth // heads
    parts = vw // LANES
    nblocks = seq_len // BLOCK
    half = kw // 2
    factor = kw ** (-0.5)
    hrows = rows // 2
    nchunks = width // COLS
    pieces = heads
    prow = wrows // pieces

    far = jnp.maximum(z, nz - 1 - z)
    behind = jnp.where(z > s, nz - 1 - z, jnp.where(z < s, z, far))
    owner = z == s
    dx, dy = x != z % 2, y != z // 2
    on_x = dx & jnp.logical_not(dy)
    on_y = dy & jnp.logical_not(dx)
    on_d = dx & dy
    edge = (z == 0) | (z == nz - 1)
    corner = owner & edge
    side_x, side_y = on_x & edge, on_y & edge
    apart = jnp.maximum(z - s, s - z)
    opposite = apart == nz - 1
    yields_up = (s == 0) & (z == nz - 2)
    yields_down = (s == nz - 1) & (z == 1)
    farthest = jnp.where(z < nz // 2, nz - 1, 0)
    tardy = jnp.where(opposite, jnp.where(z == 0, nz - 2, 1), farthest)

    loads = [
        pltpu.make_async_copy(cot_in, cotv, load.at[0]),
        pltpu.make_async_copy(w_in, wall.at[pl.ds(pl.multiple_of(k * wrows, wrows), wrows), :], load.at[1]),
        pltpu.make_async_copy(tok_in, tall.at[pl.ds(pl.multiple_of(s * rows, rows), rows), :], load.at[2]),
        pltpu.make_async_copy(
            cot_in.at[:, pl.ds(pl.multiple_of(s * cwidth, cwidth), cwidth)],
            call.at[pl.ds(pl.multiple_of(s * rows, rows), rows), :], load.at[3],
        ),
        pltpu.make_async_copy(q_in, q4, load.at[4]),
        pltpu.make_async_copy(v_in, v8, load.at[5]),
        pltpu.make_async_copy(cos_in, cosv, load.at[6]),
        pltpu.make_async_copy(sin_in, sinv, load.at[7]),
    ]
    for copy in loads:
        copy.start()
    greet(nsp, nz, s, z, core)

    def received(ref, sem):
        remote(ref, ref, load.at[0], sem, partner).wait_recv()

    def sent(ref, sem):
        remote(ref, ref, sem, load.at[0], partner).wait_send()

    def cot_copy(j, h, source):
        peer = (s + j) % nsp
        columns = pl.ds(pl.multiple_of(peer * cwidth + h * vw, vw), vw)
        to = call.at[
            pl.ds(pl.multiple_of(source * rows, rows), rows), pl.ds(pl.multiple_of(h * vw, vw), vw)
        ]
        i = (j - 1) * heads + h
        return remote(cotv.at[:, columns], to, cot_send.at[0], cot_recv.at[i], {"sp": peer})

    loads[0].wait()
    for h in range(heads):
        for j in range(1, nsp):
            cot_copy(j, h, s).start()

    def piece(zb, c, p):
        start = pl.multiple_of((zb * CORES + c) * wrows + p * prow, prow)
        return wall.at[pl.ds(start, prow), :]

    def up_copy(d, p):
        ref, i = piece(z - d, core, p), d * pieces + p
        return remote(ref, ref, up_send.at[d], up_recv.at[i], up)

    def down_copy(d, p):
        ref, i = piece(z + d, core, p), d * pieces + p
        return remote(ref, ref, down_send.at[d], down_recv.at[i], down)

    def pair_copy(zb, p):
        ref = piece(zb, core, p)
        return remote(ref, ref, pair_send.at[0], pair_recv.at[zb], partner)

    def pair_wait(zb):
        received(wall.at[:wrows, :], pair_recv.at[zb])

    loads[1].wait()
    for p in range(pieces):
        @pl.when(z < nz - 1)
        def _():
            up_copy(0, p).start()

        @pl.when(z > 0)
        def _():
            down_copy(0, p).start()

        pair_copy(z, p).start()

    def goes_up(d):
        return (z >= d) & (z < nz - 1 if d < nz - 2 else (z < nz - 1) & (s != nz - 1))

    def goes_down(d):
        return (z + d < nz) & (z > 0 if d < nz - 2 else (z > 0) & (s != 0))

    def side_copy(p, target):
        ref = piece(nz - 1 - z, core, p)
        return remote(ref, ref, side_send.at[0], side_recv.at[0], {"sp": target})

    def rise_of(d, p):
        received(piece(z - d, core, p), up_recv.at[(d - 1) * pieces + p])
        pair_copy(z - d, p).start()

    def fall_of(d, p):
        received(piece(z + d, core, p), down_recv.at[(d - 1) * pieces + p])
        pair_copy(z + d, p).start()

    def relay_first(p):
        @pl.when(z > 0)
        def _():
            rise_of(1, p)

        @pl.when(goes_up(1) & (z >= s) & prompt(p, yields_up))
        def _():
            up_copy(1, p).start()

        @pl.when(z < nz - 1)
        def _():
            fall_of(1, p)

        @pl.when(goes_down(1) & (z <= s) & prompt(p, yields_down))
        def _():
            down_copy(1, p).start()

    def relay_inward(p):
        @pl.when(goes_up(1) & (z < s))
        def _():
            up_copy(1, p).start()

        @pl.when(goes_down(1) & (z > s))
        def _():
            down_copy(1, p).start()

    def relay_second(p):
        @pl.when((z >= 2) & (z > s))
        def _():
            rise_of(2, p)

        @pl.when(goes_up(2) & (z > s))
        def _():
            up_copy(2, p).start()

        @pl.when((z + 2 < nz) & (z < s))
        def _():
            fall_of(2, p)

        @pl.when(goes_down(2) & (z < s))
        def _():
            down_copy(2, p).start()

    def take_inward(p):
        @pl.when((z >= 2) & (z <= s))
        def _():
            rise_of(2, p)

        @pl.when(goes_up(2) & (z == s))
        def _():
            up_copy(2, p).start()

        @pl.when((z + 2 < nz) & (z >= s))
        def _():
            fall_of(2, p)

        @pl.when(goes_down(2) & (z == s))
        def _():
            down_copy(2, p).start()

    def relay_third(p):
        @pl.when((z == nz - 1) & (s != z))
        def _():
            rise_of(3, p)

        @pl.when((z == 0) & (s != z))
        def _():
            fall_of(3, p)

        @pl.when(side_x & (p < pieces // 2))
        def _():
            side_copy(p, xn).start()

        @pl.when(side_y & (p >= pieces // 2))
        def _():
            side_copy(p, yn).start()

    def prompt(p, yields):
        return jnp.logical_not(yields & (p > 0))

    def relay_rest():
        for p in range(1, pieces):
            @pl.when(yields_up)
            def _():
                up_copy(1, p).start()

            @pl.when(yields_down)
            def _():
                down_copy(1, p).start()

    def take_side():
        @pl.when(corner)
        def _():
            received(wall.at[:wrows, :], side_recv.at[0])
            for p in range(pieces):
                pair_copy(nz - 1 - z, p).start()

    def token(j, i, who, h, target):
        at = tall.at[
            pl.ds(pl.multiple_of(who * rows + h * hrows, hrows), hrows),
            pl.ds(pl.multiple_of(j * COLS, COLS), COLS),
        ]
        n = 2 * j + (0 if i < 2 else 1)
        return remote(at, at, tok_send.at[0], tok_recv.at[n], {"sp": target})

    def token_send(j, i):
        who, h, target = [
            (s, 0, xn), (s, 1, yn), (s, 1, xn), (s, 0, yn), (xn, 0, yn), (yn, 1, xn)
        ][i]
        return token(j, i, who, h, target)

    def token_wait(j, count, n):
        at = pl.ds(pl.multiple_of(j * COLS, COLS), COLS)
        received(tall.at[:count * hrows, at], tok_recv.at[2 * j + n])

    loads[2].wait()
    for j in range(2):
        for i in range(4):
            token_send(j, i).start()
    for copy in loads[3:]:
        copy.wait()

    def prepare(n, _):
        at = pl.ds(pl.multiple_of(n * BLOCK, BLOCK), BLOCK)
        cosine, sine = cosv[at, :], sinv[at, :]
        span = BLOCK * heads
        xs[...] = q4[pl.ds(pl.multiple_of(n * span, span), span), :].astype(F32)
        for h in range(heads):
            q = xs[pl.ds(h, BLOCK, stride=heads), :]
            rq[at, h * kw:(h + 1) * kw] = (q * cosine + pltpu.roll(q, half, 1) * sine).astype(BF16)
        span = BLOCK * heads * parts
        ys[...] = v8[pl.ds(pl.multiple_of(n * span, span), span), :].astype(F32)
        for h in range(heads):
            for i in range(parts):
                left = h * vw + i * LANES
                vals[at, left:left + LANES] = ys[
                    pl.ds(i * heads + h, BLOCK, stride=heads * parts), :
                ].astype(BF16)
        return 0

    lax.fori_loop(0, nblocks, prepare, 0)

    def key_head(h, _):
        relay_first(h)
        for j in range(1, nsp):
            cot_copy(j, h, (s - j + nsp) % nsp).wait_recv()
        kc = pl.ds(pl.multiple_of(h * kw, kw), kw)
        vc = pl.ds(pl.multiple_of(h * vw, vw), vw)
        decay = decay_ref[s * heads + h]
        row = lax.broadcasted_iota(jnp.int32, (BLOCK, BLOCK), 0).astype(F32)
        col = lax.broadcasted_iota(jnp.int32, (BLOCK, BLOCK), 1).astype(F32)
        inside = lax.broadcasted_iota(jnp.int32, (BLOCK, kw), 0).astype(F32)
        mask = jnp.where(row >= col, jnp.exp(jnp.maximum(row - col, 0.0) * decay), 0.0)
        rise = jnp.exp((inside + 1.0) * decay)
        fall = jnp.exp((BLOCK - 1.0 - inside) * decay)
        step = jnp.exp(jnp.full((8, vw), BLOCK * 1.0, F32) * decay)
        within[h] = mask
        rising[h] = rise
        falling[h] = fall
        carry[h] = step
        trailing = jnp.zeros((kw, vw), F32)
        for n in reversed(range(nblocks)):
            at = slice(n * BLOCK, (n + 1) * BLOCK)
            cosine, sine = cosv[at, :], sinv[at, :]
            q, v, c = rq[at, kc], vals[at, vc], call[at, vc]
            mixing = (dot_nt(c, v) * mask).astype(BF16)
            mix[at, pl.ds(pl.multiple_of(h * BLOCK, BLOCK), BLOCK)] = mixing
            trail = trailing.astype(BF16)
            held[h * nblocks + n] = trail
            grad = dot_tn(mixing, q) + fall * dot_nt(v, trail)
            back = (grad * cosine - pltpu.roll(grad, half, 1) * sine) * factor
            gk[at, kc] = back.astype(BF16)
            gkt[kc, at] = back.T.astype(BF16)
            decayed = (q.astype(F32) * rise).astype(BF16)
            trailing = trailing * step[0:1, :] + dot_tn(decayed, c)
        entering[h] = jnp.zeros((kw, vw), F32)
        return 0

    lax.fori_loop(0, heads, key_head, 0)

    def gk_copy(j, source):
        peer = (s + j) % nsp
        to = gkall.at[:, pl.ds(pl.multiple_of(source * feats, feats), feats)]
        return remote(
            gk.at[pl.ds(pl.multiple_of(peer * rows, rows), rows), :], to,
            gk_send.at[0], gk_recv.at[0], {"sp": peer},
        )

    def half_copy(j):
        return remote(pwo.at[j], rp.at[j], half_send.at[0], half_recv.at[j], partner)

    def line_copy(j, side, target):
        return remote(
            lsend.at[j], lrecv.at[side, j], line_send.at[0],
            line_recv.at[side * nchunks + j], target,
        )

    def cast_copy(j, h, target, last_leg=False):
        ref = fin.at[j, pl.ds(h * (wrows // 2), wrows // 2), :]
        sem = cast_recv.at[nchunks if last_leg else j]
        return remote(ref, ref, cast_send.at[0], sem, {"sp": target})

    def gradient_columns(j):
        token_wait(j, 4, 1)
        at = pl.ds(pl.multiple_of(j * COLS, COLS), COLS)
        theirs = pl.ds(pl.multiple_of((1 - core) * wrows, wrows), wrows)
        mine = pl.ds(pl.multiple_of(core * wrows, wrows), wrows)
        pwo[j] = dot_nn(gkt[theirs, :], tall[:, at]).astype(BF16)
        half_copy(j).start()
        acc[j] = dot_nn(gkt[mine, :], tall[:, at])

    def sum_line(j):
        half_copy(j).wait_recv()
        acc[j] = acc[j] + rp[j].astype(F32)

        @pl.when((z >= s) & (z < nz - 1))
        def _():
            line_copy(j, 1, down).wait_recv()
            acc[j] = acc[j] + lrecv[1, j].astype(F32)

        @pl.when((z <= s) & (z > 0))
        def _():
            line_copy(j, 0, up).wait_recv()
            acc[j] = acc[j] + lrecv[0, j].astype(F32)

        @pl.when(owner)
        def _():
            fin[j] = acc[j].astype(BF16)
            cast_copy(j, 0, xn).start()
            cast_copy(j, 1, yn).start()

        @pl.when(jnp.logical_not(owner))
        def _():
            lsend[j] = acc[j].astype(BF16)

        @pl.when(z > s)
        def _():
            line_copy(j, 1, down).start()

        @pl.when(z < s)
        def _():
            line_copy(j, 0, up).start()

    def make_keys():
        pair_wait(s)
        left = pl.ds(pl.multiple_of(s * feats, feats), feats)

        def tile(i, _):
            at = pl.ds(pl.multiple_of(i * TILE, TILE), TILE)
            keys[at, :] = dot_nt(tall[at, :], wall[left, :]).astype(BF16)
            return 0

        lax.fori_loop(0, seq_len // TILE, tile, 0)

    def gq_copy(n):
        span = BLOCK * heads
        at = pl.ds(pl.multiple_of(n * span, span), span)
        return pltpu.make_async_copy(gq4.at[at, :], gq_out.at[at, :], gq_store.at[0])

    def gv_copy(n):
        span = BLOCK * heads * parts
        at = pl.ds(pl.multiple_of(n * span, span), span)
        return pltpu.make_async_copy(gv8.at[at, :], gv_out.at[at, :], gv_store.at[0])

    def query_block(n):
        at = pl.ds(pl.multiple_of(n * BLOCK, BLOCK), BLOCK)
        cosine, sine = cosv[at, :], sinv[at, :]
        for h in range(heads):
            kc, vc = slice(h * kw, (h + 1) * kw), slice(h * vw, (h + 1) * vw)
            key = keys[at, kc].astype(F32)
            rk = ((key * cosine + pltpu.roll(key, half, 1) * sine) * factor).astype(BF16)
            q, v, c = rq[at, kc], vals[at, vc], call[at, vc]
            state = entering[h]
            grad = dot_nn(mix[at, h * BLOCK:(h + 1) * BLOCK], rk)
            grad = grad + rising[h] * dot_nt(c, state.astype(BF16))
            xs[pl.ds(h, BLOCK, stride=heads), :] = (
                grad * cosine - pltpu.roll(grad, half, 1) * sine
            )
            scores = (dot_nt(q, rk) * within[h]).astype(BF16)
            fall = falling[h]
            inner = dot_tn(scores, c)
            outer = dot_nn(rk, held[h * nblocks + n])
            for i in range(parts):
                lane = slice(i * LANES, (i + 1) * LANES)
                ys[pl.ds(i * heads + h, BLOCK, stride=heads * parts), :] = (
                    inner[:, lane] + fall * outer[:, lane]
                )
            decayed = (rk.astype(F32) * fall).astype(BF16)
            entering[h] = state * carry[h, 0:1, :] + dot_tn(decayed, v)
        span = BLOCK * heads
        gq4[pl.ds(pl.multiple_of(n * span, span), span), :] = xs[...].astype(BF16)
        span = BLOCK * heads * parts
        gv8[pl.ds(pl.multiple_of(n * span, span), span), :] = ys[...].astype(BF16)
        gq_copy(n).start()
        gv_copy(n).start()

    def gather_keys():
        received(gkall.at[:, :(nsp - 1) * feats], gk_recv.at[0])
        gkall[:, pl.ds(pl.multiple_of(s * feats, feats), feats)] = gk[
            pl.ds(pl.multiple_of(s * rows, rows), rows), :
        ]
        for zb in range(nz):
            @pl.when((zb != s) & (zb != tardy))
            def _():
                pair_wait(zb)

    def gt_copy(i):
        at = pl.ds(pl.multiple_of(i * TILE, TILE), TILE)
        return pltpu.make_async_copy(gt.at[:, at], gt_out.at[:, at], gt_store.at[0])

    def block_product(zb, at):
        inner = pl.ds(pl.multiple_of(zb * feats, feats), feats)
        return dot_nn(gkall[:, inner], wall[inner, at])

    def token_gradient(i):
        at = pl.ds(pl.multiple_of(i * TILE, TILE), TILE)
        total = block_product((tardy + 1) % nz, at)
        for j in range(2, nz):
            total = total + block_product((tardy + j) % nz, at)
        gtf[i] = total

    last = nchunks + 1 + (nz + 1) * HOP

    def turn(t, _):
        @pl.when(t < nchunks)
        def _():
            token_wait(t, 2, 0)
            token_send(t, 4).start()
            token_send(t, 5).start()

        @pl.when(t + 2 < nchunks)
        def _():
            for i in range(4):
                token_send(t + 2, i).start()

        @pl.when(t == nchunks - 1)
        def _():
            for j in range(1, nsp):
                gk_copy(j, s).start()

        @pl.when((t >= 1) & (t <= nchunks))
        def _():
            gradient_columns(t - 1)

        j = t - 2 - behind * HOP

        @pl.when((j >= 0) & (j < nchunks))
        def _():
            sum_line(j)

        jx = t - 2 - (far + 1) * HOP

        @pl.when(on_x & (jx >= 0) & (jx < nchunks))
        def _():
            received(fin.at[jx, :wrows // 2, :], cast_recv.at[jx])
            cast_copy(jx, 0, yn).start()

        @pl.when(on_y & (jx >= 0) & (jx < nchunks))
        def _():
            received(fin.at[jx, wrows // 2:, :], cast_recv.at[jx])
            cast_copy(jx, 1, xn).start()

        jd = t - 2 - (far + 2) * HOP

        @pl.when(on_d & (jd >= 0) & (jd < nchunks))
        def _():
            received(fin.at[jd], cast_recv.at[jd])
            cast_copy(jd, 0, xn, True).start()
            cast_copy(jd, 1, yn, True).start()

        @pl.when(t < pieces)
        def _():
            relay_inward(t)

        p = t - 2

        @pl.when((p >= 0) & (p < pieces) & jnp.logical_not(opposite))
        def _():
            relay_second(p)

        @pl.when((p >= 1) & (p <= pieces))
        def _():
            take_inward(p - 1)

        p = t - jnp.where(opposite, pieces, nchunks + 1)

        @pl.when((p >= 0) & (p < pieces))
        def _():
            relay_third(p)

        p = t - nchunks - 1

        @pl.when(opposite & (p >= 0) & (p < pieces))
        def _():
            relay_second(p)

        @pl.when(t == pieces + 2)
        def _():
            relay_rest()

        @pl.when(t == nchunks)
        def _():
            make_keys()

        n = (t - nchunks - 1) * 2

        @pl.when((n >= 0) & (n < nblocks))
        def _():
            query_block(n)
            query_block(n + 1)

        i = t - tile_step

        @pl.when(i == 0)
        def _():
            gather_keys()

        @pl.when((i >= 0) & (i < ntiles // 2))
        def _():
            token_gradient(2 * i)
            token_gradient(2 * i + 1)

        return 0

    ntiles = width // TILE
    tile_step = nchunks + HOP + 2
    lax.fori_loop(0, last + 1, turn, 0)
    take_side()

    @pl.when(tardy != s)
    def _():
        pair_wait(tardy)

    def complete(i, _):
        at = pl.ds(pl.multiple_of(i * TILE, TILE), TILE)
        gt[:, at] = (gtf[i] + block_product(tardy, at)).astype(BF16)
        gt_copy(i).start()
        return 0

    lax.fori_loop(0, ntiles, complete, 0)

    @pl.when(on_x | on_y)
    def _():
        received(fin.at[:nchunks // 2], cast_recv.at[nchunks])

    gw_copy = pltpu.make_async_copy(fin, gw_out, gw_store.at[0])
    gw_copy.start()

    sent(cotv.at[:, :(nsp - 1) * cwidth], cot_send.at[0])
    sent(tall.at[:6 * hrows, :], tok_send.at[0])
    sent(gk.at[:(nsp - 1) * rows, :], gk_send.at[0])
    sent(pwo, half_send.at[0])

    @pl.when(jnp.logical_not(owner))
    def _():
        sent(lsend, line_send.at[0])

    @pl.when(owner | on_d)
    def _():
        sent(fin, cast_send.at[0])

    @pl.when(on_x | on_y)
    def _():
        sent(fin.at[:nchunks // 2], cast_send.at[0])

    for d in range(nz - 1):
        @pl.when(goes_up(d))
        def _():
            sent(wall.at[:wrows, :], up_send.at[d])

        @pl.when(goes_down(d))
        def _():
            sent(wall.at[:wrows, :], down_send.at[d])

    sent(wall.at[:nz * wrows, :], pair_send.at[0])

    @pl.when(side_x | side_y)
    def _():
        sent(wall.at[:wrows // 2, :], side_send.at[0])

    pltpu.make_async_copy(gq4, gq_out, gq_store.at[0]).wait()
    pltpu.make_async_copy(gv8, gv_out, gv_store.at[0]).wait()
    pltpu.make_async_copy(gt, gt_out, gt_store.at[0]).wait()
    gw_copy.wait()


def whole(tokens, weight, queries, values, cotan, decay, nsp, ndp, heads):
    nz = ndp // CORES
    rows, width = tokens.shape
    wrows = weight.shape[0]
    seq_len = rows * nsp
    kw = queries.shape[1]
    feats = heads * kw
    cwidth = cotan.shape[1] // nsp
    vw = cwidth // heads
    nblocks = seq_len // BLOCK
    nchunks = width // COLS
    cosine, sine = rotation_tables(seq_len, kw // 2)
    dma = pltpu.SemaphoreType.DMA
    anywhere = pl.BlockSpec(memory_space=pl.ANY)

    def buffer(*shape):
        return pltpu.VMEM(shape, BF16)

    def wide(*shape):
        return pltpu.VMEM(shape, F32)

    return pl.pallas_call(
        functools.partial(whole_kernel, nsp, nz, heads),
        in_specs=[pl.BlockSpec(memory_space=pltpu.SMEM)] + [anywhere] * 7,
        out_specs=[anywhere] * 4,
        out_shape=[
            jax.ShapeDtypeStruct((rows, width), BF16),
            jax.ShapeDtypeStruct(queries.shape, BF16),
            jax.ShapeDtypeStruct(values.shape, BF16),
            jax.ShapeDtypeStruct((nchunks, wrows, COLS), BF16),
        ],
        scratch_shapes=[
            buffer(rows, nsp * cwidth),
            buffer(seq_len, width),
            buffer(wrows * ndp, width),
            buffer(seq_len, cwidth),
            buffer(*queries.shape),
            buffer(*values.shape),
            wide(seq_len, kw),
            wide(seq_len, kw),
            buffer(seq_len, feats),
            buffer(seq_len, cwidth),
            buffer(seq_len, heads * BLOCK),
            buffer(heads * nblocks, kw, vw),
            buffer(seq_len, feats),
            buffer(feats, seq_len),
            buffer(rows, nsp * feats),
            buffer(seq_len, feats),
            buffer(*queries.shape),
            buffer(*values.shape),
            buffer(rows, width),
            wide(width // TILE, rows, TILE),
            wide(nchunks, wrows, COLS),
            buffer(nchunks, wrows, COLS),
            buffer(nchunks, wrows, COLS),
            buffer(2, nchunks, wrows, COLS),
            buffer(nchunks, wrows, COLS),
            buffer(nchunks, wrows, COLS),
            wide(BLOCK * heads, kw),
            wide(BLOCK * heads * (vw // LANES), LANES),
            wide(heads, BLOCK, BLOCK),
            wide(heads, BLOCK, kw),
            wide(heads, BLOCK, kw),
            wide(heads, 8, vw),
            wide(heads, kw, vw),
            dma((8,)),
            dma((1,)), dma(((nsp - 1) * heads,)),
            dma((1,)), dma((2 * nchunks,)),
            dma((nz - 1,)), dma(((nz - 1) * heads,)),
            dma((nz - 1,)), dma(((nz - 1) * heads,)),
            dma((1,)), dma((nz,)),
            dma((1,)), dma((1,)),
            dma((1,)), dma((1,)),
            dma((1,)), dma((nchunks,)),
            dma((1,)), dma((2 * nchunks,)),
            dma((1,)), dma((nchunks + 1,)),
            dma((1,)), dma((1,)), dma((1,)), dma((1,)),
        ],
        compiler_params=pltpu.CompilerParams(
            has_side_effects=True, vmem_limit_bytes=VMEM_LIMIT, collective_id=0
        ),
        name="whole",
    )(decay, tokens, weight, queries, values, cotan, jnp.asarray(cosine), jnp.asarray(sine))


def finish_kernel(gt, gq, gv, gw, gt_out, gq_out, gv_out, gw_out):
    gt_out[...] = gt[...]
    gq_out[...] = gq[...]
    gv_out[...] = gv[...]
    for j in range(gw.shape[0]):
        gw_out[:, j * COLS:(j + 1) * COLS] = gw[j].astype(F32)


STEPS = 4


def finish(gt, gq, gv, gw):
    def flat(array):
        return pl.BlockSpec((array.shape[0] // STEPS, array.shape[1]), lambda i: (i, 0))

    chunks, wrows, cols = gw.shape
    shapes = [(gt.shape, BF16), (gq.shape, BF16), (gv.shape, BF16), ((wrows, chunks * cols), F32)]
    out_shape = [jax.ShapeDtypeStruct(*shape) for shape in shapes]
    return pl.pallas_call(
        finish_kernel,
        grid=(STEPS,),
        in_specs=[flat(gt), flat(gq), flat(gv)]
        + [pl.BlockSpec((chunks, wrows // STEPS, cols), lambda i: (0, i, 0))],
        out_specs=[flat(shape) for shape in out_shape],
        out_shape=out_shape,
        name="finish",
    )(gt, gq, gv, gw)


def gather_general(tokens, weight, cotan):
    gathered = lax.all_gather(weight, "dp", axis=0, tiled=True)
    rows = gathered.shape[0] // lax.axis_size("sp")
    chosen = lax.dynamic_slice_in_dim(gathered, lax.axis_index("sp") * rows, rows)
    return (
        lax.all_gather(tokens, "sp", axis=0, tiled=True),
        chosen,
        lax.all_to_all(cotan, "sp", split_axis=1, concat_axis=0, tiled=True),
    )


def scatter_general(partial_tokens, partial_weight):
    grad_tokens = lax.psum_scatter(
        partial_tokens, "sp", scatter_dimension=0, tiled=True
    ).astype(BF16)
    owned = lax.psum_scatter(
        partial_weight, "dp", scatter_dimension=0, tiled=True
    )
    everything = lax.all_gather(owned, ("sp", "dp"), axis=0, tiled=True)
    rows = everything.shape[0] // lax.axis_size("dp")
    return grad_tokens, lax.dynamic_slice_in_dim(
        everything, lax.axis_index("dp") * rows, rows
    )


def body(nsp, ndp, tokens, key_weight, queries, values, cotangent, log_decay):
    seq_len, heads, kw = queries.shape[1:]
    vw = values.shape[3]
    if nsp == 4 and ndp == CORES * nsp and kw == BLOCK:
        parts = vw // LANES
        flat = values.reshape(seq_len, heads, parts, LANES).transpose(0, 2, 1, 3)
        grad_tokens, grad_query, grad_value, weight_grad = whole(
            tokens[0], key_weight, queries.reshape(-1, kw), flat.reshape(-1, LANES),
            cotangent[0], log_decay, nsp, ndp, heads,
        )
        grad_tokens, grad_query, grad_value, weight_grad = finish(
            grad_tokens, grad_query, grad_value, weight_grad
        )
        grad_value = grad_value.reshape(seq_len, parts, heads, LANES).transpose(0, 2, 1, 3)
    else:
        all_tokens, weight, cotan = gather_general(tokens[0], key_weight, cotangent[0])
        keys = dot_nt(all_tokens, weight).astype(BF16)
        grad_query, grad_key, _, grad_value = retention_backward(
            queries.reshape(seq_len, -1), keys, values.reshape(seq_len, -1), cotan, log_decay, heads
        )
        grad_tokens, weight_grad = scatter_general(
            dot_nn(grad_key, weight), dot_tn(grad_key, all_tokens)
        )
    return (
        grad_tokens[None],
        grad_query.reshape(queries.shape),
        grad_value.reshape(values.shape),
        weight_grad,
    )


def solution(mesh):
    return jax.shard_map(
        functools.partial(body, mesh.shape["sp"], mesh.shape["dp"]),
        mesh=mesh,
        in_specs=(
            P("dp", "sp", None),
            P("dp", None),
            P("dp", None, "sp", None),
            P("dp", None, "sp", None),
            P("dp", "sp", None),
            P(),
        ),
        out_specs=(
            P("dp", "sp", None),
            P("dp", None, "sp", None),
            P("dp", None, "sp", None),
            P("dp", None),
        ),
        check_vma=False,
    )
```

```python
import functools

import jax
import jax.numpy as jnp
import numpy as np
from jax import lax
from jax.experimental import pallas as pl
from jax.experimental.pallas import tpu as pltpu
from jax.sharding import PartitionSpec as P

BLOCK = 128
CORES = 2
MESH = pl.DeviceIdType.MESH
F32 = jnp.float32
BF16 = jnp.bfloat16
VMEM_LIMIT = 60 * 1024 * 1024


def rotation_tables(seq_len, half):
    position = np.arange(seq_len, dtype=np.float32)
    frequency = (10000.0 ** (-np.arange(half, dtype=np.float32) / half)).astype(np.float32)
    angle = (position[:, None] * frequency[None, :]).astype(np.float32)
    cosine, sine = np.cos(angle), np.sin(angle)
    return (
        np.concatenate([cosine, cosine], axis=1).astype(np.float32),
        np.concatenate([-sine, sine], axis=1).astype(np.float32),
    )


def dot_nt(a, b):
    return lax.dot_general(a, b, (((1,), (1,)), ((), ())), preferred_element_type=F32)


def dot_tn(a, b):
    return lax.dot_general(a, b, (((0,), (0,)), ((), ())), preferred_element_type=F32)


def dot_nn(a, b):
    return lax.dot_general(a, b, (((1,), (0,)), ((), ())), preferred_element_type=F32)


def retention_kernel(
    decay_ref, q_ref, k_ref, v_ref, c_ref, cos_ref, sin_ref,
    gq_ref, gk_ref, gkt_ref, gv_ref, rq_ref, rk_ref, mix_ref,
):
    seq_len, key_width = q_ref.shape
    value_width = v_ref.shape[1]
    nblocks = seq_len // BLOCK
    half = key_width // 2
    factor = key_width ** (-0.5)
    decay = decay_ref[lax.axis_index("sp") * pl.num_programs(0) + pl.program_id(0)]
    row = lax.broadcasted_iota(jnp.int32, (BLOCK, BLOCK), 0).astype(F32)
    col = lax.broadcasted_iota(jnp.int32, (BLOCK, BLOCK), 1).astype(F32)
    within = jnp.where(row >= col, jnp.exp(jnp.maximum(row - col, 0.0) * decay), 0.0)
    inside = lax.broadcasted_iota(jnp.int32, (BLOCK, key_width), 0).astype(F32)
    rising = jnp.exp((inside + 1.0) * decay)
    falling = jnp.exp((BLOCK - 1.0 - inside) * decay)
    wide = lax.broadcasted_iota(jnp.int32, (BLOCK, value_width), 0).astype(F32)
    falling_wide = jnp.exp((BLOCK - 1.0 - wide) * decay)
    carry_decay = jnp.exp(jnp.full((key_width, value_width), BLOCK * 1.0, F32) * decay)
    zero = jnp.zeros((key_width, value_width), F32)

    def forward(n, entering):
        rows = pl.ds(pl.multiple_of(n * BLOCK, BLOCK), BLOCK)
        cosine, sine = cos_ref[rows, :], sin_ref[rows, :]
        q = q_ref[rows, :].astype(F32)
        k = k_ref[rows, :].astype(F32)
        rq = (q * cosine + pltpu.roll(q, half, 1) * sine).astype(BF16)
        rk = ((k * cosine + pltpu.roll(k, half, 1) * sine) * factor).astype(BF16)
        rq_ref[rows, :] = rq
        rk_ref[rows, :] = rk
        v, c = v_ref[rows, :], c_ref[rows, :]
        mixing = (dot_nt(c, v) * within).astype(BF16)
        mix_ref[rows, :] = mixing
        grad = dot_nn(mixing, rk) + rising * dot_nt(c, entering.astype(BF16))
        gq_ref[rows, :] = (grad * cosine - pltpu.roll(grad, half, 1) * sine).astype(BF16)
        decayed = (rk.astype(F32) * falling).astype(BF16)
        return entering * carry_decay + dot_tn(decayed, v)

    def backward(step, trailing):
        n = nblocks - 1 - step
        rows = pl.ds(pl.multiple_of(n * BLOCK, BLOCK), BLOCK)
        cosine, sine = cos_ref[rows, :], sin_ref[rows, :]
        rq, rk, mixing = rq_ref[rows, :], rk_ref[rows, :], mix_ref[rows, :]
        v, c = v_ref[rows, :], c_ref[rows, :]
        held = trailing.astype(BF16)
        scores = (dot_nt(rq, rk) * within).astype(BF16)
        grad = dot_tn(mixing, rq) + falling * dot_nt(v, held)
        back = (grad * cosine - pltpu.roll(grad, half, 1) * sine) * factor
        gk_ref[rows, :] = back.astype(BF16)
        gkt_ref[:, rows] = back.T.astype(BF16)
        gv_ref[rows, :] = (dot_tn(scores, c) + falling_wide * dot_nn(rk, held)).astype(BF16)
        decayed = (rq.astype(F32) * rising).astype(BF16)
        return trailing * carry_decay + dot_tn(decayed, c)

    unroll = min(nblocks, 8)
    lax.fori_loop(0, nblocks, forward, zero, unroll=unroll)
    lax.fori_loop(0, nblocks, backward, zero, unroll=unroll)


def retention_backward(queries, keys, values, cotan, decay, heads):
    seq_len = queries.shape[0]
    kw = queries.shape[1] // heads
    vw = values.shape[1] // heads
    cosine, sine = rotation_tables(seq_len, kw // 2)
    narrow = pl.BlockSpec((seq_len, kw), lambda h: (0, h))
    wide = pl.BlockSpec((seq_len, vw), lambda h: (0, h))
    table = pl.BlockSpec((seq_len, kw), lambda h: (0, 0))
    flops = 2 * seq_len * heads * BLOCK * (3 * kw + 2 * vw + 5 * vw)
    return pl.pallas_call(
        retention_kernel,
        grid=(heads,),
        in_specs=[pl.BlockSpec(memory_space=pltpu.SMEM), narrow, narrow, wide, wide, table, table],
        out_specs=[narrow, narrow, pl.BlockSpec((kw, seq_len), lambda h: (h, 0)), wide],
        out_shape=[
            jax.ShapeDtypeStruct(queries.shape, BF16),
            jax.ShapeDtypeStruct(queries.shape, BF16),
            jax.ShapeDtypeStruct(queries.shape[::-1], BF16),
            jax.ShapeDtypeStruct(values.shape, BF16),
        ],
        scratch_shapes=[
            pltpu.VMEM((seq_len, kw), BF16),
            pltpu.VMEM((seq_len, kw), BF16),
            pltpu.VMEM((seq_len, BLOCK), BF16),
        ],
        compiler_params=pltpu.CompilerParams(vmem_limit_bytes=VMEM_LIMIT),
        cost_estimate=pl.CostEstimate(
            flops=flops, bytes_accessed=8 * seq_len * heads * (kw + vw), transcendentals=0
        ),
        name="retention",
    )(decay, queries, keys, values, cotan, jnp.asarray(cosine), jnp.asarray(sine))


def remote(src, dst, send, recv, target):
    return pltpu.make_async_remote_copy(
        src_ref=src, dst_ref=dst, send_sem=send, recv_sem=recv,
        device_id=target, device_id_type=MESH,
    )


def greet(nsp, nz, s, z, core):
    barrier = pltpu.get_barrier_semaphore()
    others = [{"dp": z * CORES + 1 - core}]
    others += [{"sp": (s + j) % nsp} for j in range(1, nsp)]
    for other in others:
        pl.semaphore_signal(barrier, inc=1, device_id=other, device_id_type=MESH)

    @pl.when(z > 0)
    def _():
        below = {"dp": (z - 1) * CORES + core}
        pl.semaphore_signal(barrier, inc=1, device_id=below, device_id_type=MESH)

    @pl.when(z < nz - 1)
    def _():
        above = {"dp": (z + 1) * CORES + core}
        pl.semaphore_signal(barrier, inc=1, device_id=above, device_id_type=MESH)

    ends = jnp.where(z > 0, 1, 0) + jnp.where(z < nz - 1, 1, 0)
    pl.semaphore_wait(barrier, len(others) + ends)


TILE = 256
LANES = 128
COLS = 256
HOP = 2


def whole_kernel(
    nsp, nz, heads,
    decay_ref, tok_in, w_in, q_in, v_in, cot_in, cos_in, sin_in,
    gt_out, gq_out, gv_out, gw_out,
    cotv, tall, wall, call, q4, v8, cosv, sinv, rq, vals, mix, held, gk, gkt, gkall,
    keys, gq4, gv8, gt, gtf, acc, pwo, rp, lrecv, lsend, fin, xs, ys,
    within, rising, falling, carry, entering,
    load, cot_send, cot_recv, tok_send, tok_recv,
    up_send, up_recv, down_send, down_recv, pair_send, pair_recv, side_send, side_recv,
    gk_sent, gk_recv, half_send, half_recv, line_send, line_recv,
    cast_send, cast_recv, gq_store, gv_store, gw_store, gt_store,
):
    s = lax.axis_index("sp")
    k = lax.axis_index("dp")
    z, core = k // CORES, k % CORES
    x, y = s % 2, s // 2
    xn, yn = y * 2 + (1 - x), (1 - y) * 2 + x
    diagonal = (1 - y) * 2 + (1 - x)
    partner = {"dp": z * CORES + 1 - core}
    up, down = {"dp": k + CORES}, {"dp": k - CORES}
    rows, width = tok_in.shape
    wrows = w_in.shape[0]
    seq_len, feats = gk.shape
    kw = feats // heads
    cwidth = call.shape[1]
    vw = cwidth // heads
    parts = vw // LANES
    nblocks = seq_len // BLOCK
    half = kw // 2
    factor = kw ** (-0.5)
    hrows = rows // 2
    nchunks = width // COLS
    pieces = heads
    prow = wrows // pieces

    far = jnp.maximum(z, nz - 1 - z)
    behind = jnp.where(z > s, nz - 1 - z, jnp.where(z < s, z, far))
    owner = z == s
    dx, dy = x != z % 2, y != z // 2
    on_x = dx & jnp.logical_not(dy)
    on_y = dy & jnp.logical_not(dx)
    on_d = dx & dy
    edge = (z == 0) | (z == nz - 1)
    corner = owner & edge
    side_x, side_y = on_x & edge, on_y & edge
    apart = jnp.maximum(z - s, s - z)
    opposite = apart == nz - 1
    yields_up = (s == 0) & (z == nz - 2)
    yields_down = (s == nz - 1) & (z == 1)
    farthest = jnp.where(z < nz // 2, nz - 1, 0)
    tardy = jnp.where(opposite, jnp.where(z == 0, nz - 2, 1), farthest)

    loads = [
        pltpu.make_async_copy(cot_in, cotv, load.at[0]),
        pltpu.make_async_copy(w_in, wall.at[pl.ds(pl.multiple_of(k * wrows, wrows), wrows), :], load.at[1]),
        pltpu.make_async_copy(tok_in, tall.at[pl.ds(pl.multiple_of(s * rows, rows), rows), :], load.at[2]),
        pltpu.make_async_copy(
            cot_in.at[:, pl.ds(pl.multiple_of(s * cwidth, cwidth), cwidth)],
            call.at[pl.ds(pl.multiple_of(s * rows, rows), rows), :], load.at[3],
        ),
        pltpu.make_async_copy(q_in, q4, load.at[4]),
        pltpu.make_async_copy(v_in, v8, load.at[5]),
        pltpu.make_async_copy(cos_in, cosv, load.at[6]),
        pltpu.make_async_copy(sin_in, sinv, load.at[7]),
    ]
    for copy in loads:
        copy.start()
    greet(nsp, nz, s, z, core)

    def received(ref, sem):
        remote(ref, ref, load.at[0], sem, partner).wait_recv()

    def sent(ref, sem):
        remote(ref, ref, sem, load.at[0], partner).wait_send()

    def cot_copy(j, h, source):
        peer = (s + j) % nsp
        columns = pl.ds(pl.multiple_of(peer * cwidth + h * vw, vw), vw)
        to = call.at[
            pl.ds(pl.multiple_of(source * rows, rows), rows), pl.ds(pl.multiple_of(h * vw, vw), vw)
        ]
        i = (j - 1) * heads + h
        return remote(cotv.at[:, columns], to, cot_send.at[0], cot_recv.at[i], {"sp": peer})

    loads[0].wait()
    for h in range(heads):
        for j in range(1, nsp):
            cot_copy(j, h, s).start()

    def piece(zb, c, p):
        start = pl.multiple_of((zb * CORES + c) * wrows + p * prow, prow)
        return wall.at[pl.ds(start, prow), :]

    def up_copy(d, p):
        ref, i = piece(z - d, core, p), d * pieces + p
        return remote(ref, ref, up_send.at[d], up_recv.at[i], up)

    def down_copy(d, p):
        ref, i = piece(z + d, core, p), d * pieces + p
        return remote(ref, ref, down_send.at[d], down_recv.at[i], down)

    def pair_copy(zb, p):
        ref = piece(zb, core, p)
        return remote(ref, ref, pair_send.at[0], pair_recv.at[zb], partner)

    def pair_wait(zb):
        received(wall.at[:wrows, :], pair_recv.at[zb])

    loads[1].wait()
    for p in range(pieces):
        @pl.when(z < nz - 1)
        def _():
            up_copy(0, p).start()

        @pl.when(z > 0)
        def _():
            down_copy(0, p).start()

        pair_copy(z, p).start()

    def goes_up(d):
        return (z >= d) & (z < nz - 1 if d < nz - 2 else (z < nz - 1) & (s != nz - 1))

    def goes_down(d):
        return (z + d < nz) & (z > 0 if d < nz - 2 else (z > 0) & (s != 0))

    def side_copy(p, target):
        ref = piece(nz - 1 - z, core, p)
        return remote(ref, ref, side_send.at[0], side_recv.at[0], {"sp": target})

    def rise_of(d, p):
        received(piece(z - d, core, p), up_recv.at[(d - 1) * pieces + p])
        pair_copy(z - d, p).start()

    def fall_of(d, p):
        received(piece(z + d, core, p), down_recv.at[(d - 1) * pieces + p])
        pair_copy(z + d, p).start()

    def relay_first(p):
        @pl.when(z > 0)
        def _():
            rise_of(1, p)

        @pl.when(goes_up(1) & (z >= s) & prompt(p, yields_up))
        def _():
            up_copy(1, p).start()

        @pl.when(z < nz - 1)
        def _():
            fall_of(1, p)

        @pl.when(goes_down(1) & (z <= s) & prompt(p, yields_down))
        def _():
            down_copy(1, p).start()

    def relay_inward(p):
        @pl.when(goes_up(1) & (z < s))
        def _():
            up_copy(1, p).start()

        @pl.when(goes_down(1) & (z > s))
        def _():
            down_copy(1, p).start()

    def relay_second(p):
        @pl.when((z >= 2) & (z > s))
        def _():
            rise_of(2, p)

        @pl.when(goes_up(2) & (z > s))
        def _():
            up_copy(2, p).start()

        @pl.when((z + 2 < nz) & (z < s))
        def _():
            fall_of(2, p)

        @pl.when(goes_down(2) & (z < s))
        def _():
            down_copy(2, p).start()

    def take_inward(p):
        @pl.when((z >= 2) & (z <= s))
        def _():
            rise_of(2, p)

        @pl.when(goes_up(2) & (z == s))
        def _():
            up_copy(2, p).start()

        @pl.when((z + 2 < nz) & (z >= s))
        def _():
            fall_of(2, p)

        @pl.when(goes_down(2) & (z == s))
        def _():
            down_copy(2, p).start()

    def relay_third(p):
        @pl.when((z == nz - 1) & (s != z))
        def _():
            rise_of(3, p)

        @pl.when((z == 0) & (s != z))
        def _():
            fall_of(3, p)

        @pl.when(side_x & (p < pieces // 2))
        def _():
            side_copy(p, xn).start()

        @pl.when(side_y & (p >= pieces // 2))
        def _():
            side_copy(p, yn).start()

    def prompt(p, yields):
        return jnp.logical_not(yields & (p > 0))

    def relay_rest():
        for p in range(1, pieces):
            @pl.when(yields_up)
            def _():
                up_copy(1, p).start()

            @pl.when(yields_down)
            def _():
                down_copy(1, p).start()

    def take_side():
        @pl.when(corner)
        def _():
            received(wall.at[:wrows, :], side_recv.at[0])
            for p in range(pieces):
                pair_copy(nz - 1 - z, p).start()

    def token(j, i, who, h, target):
        at = tall.at[
            pl.ds(pl.multiple_of(who * rows + h * hrows, hrows), hrows),
            pl.ds(pl.multiple_of(j * COLS, COLS), COLS),
        ]
        n = 2 * j + (0 if i < 2 else 1)
        return remote(at, at, tok_send.at[0], tok_recv.at[n], {"sp": target})

    def token_send(j, i):
        who, h, target = [
            (s, 0, xn), (s, 1, yn), (s, 1, xn), (s, 0, yn), (xn, 0, yn), (yn, 1, xn)
        ][i]
        return token(j, i, who, h, target)

    def token_wait(j, count, n):
        at = pl.ds(pl.multiple_of(j * COLS, COLS), COLS)
        received(tall.at[:count * hrows, at], tok_recv.at[2 * j + n])

    loads[2].wait()
    for j in range(2):
        for i in range(4):
            token_send(j, i).start()
    for copy in loads[3:]:
        copy.wait()

    def prepare(n, _):
        at = pl.ds(pl.multiple_of(n * BLOCK, BLOCK), BLOCK)
        cosine, sine = cosv[at, :], sinv[at, :]
        span = BLOCK * heads
        xs[...] = q4[pl.ds(pl.multiple_of(n * span, span), span), :].astype(F32)
        for h in range(heads):
            q = xs[pl.ds(h, BLOCK, stride=heads), :]
            rq[at, h * kw:(h + 1) * kw] = (q * cosine + pltpu.roll(q, half, 1) * sine).astype(BF16)
        span = BLOCK * heads * parts
        ys[...] = v8[pl.ds(pl.multiple_of(n * span, span), span), :].astype(F32)
        for h in range(heads):
            for i in range(parts):
                left = h * vw + i * LANES
                vals[at, left:left + LANES] = ys[
                    pl.ds(i * heads + h, BLOCK, stride=heads * parts), :
                ].astype(BF16)
        return 0

    lax.fori_loop(0, nblocks, prepare, 0)

    def key_head(h, _):
        relay_first(h)
        for j in range(1, nsp):
            cot_copy(j, h, (s - j + nsp) % nsp).wait_recv()
        kc = pl.ds(pl.multiple_of(h * kw, kw), kw)
        vc = pl.ds(pl.multiple_of(h * vw, vw), vw)
        decay = decay_ref[s * heads + h]
        row = lax.broadcasted_iota(jnp.int32, (BLOCK, BLOCK), 0).astype(F32)
        col = lax.broadcasted_iota(jnp.int32, (BLOCK, BLOCK), 1).astype(F32)
        inside = lax.broadcasted_iota(jnp.int32, (BLOCK, kw), 0).astype(F32)
        mask = jnp.where(row >= col, jnp.exp(jnp.maximum(row - col, 0.0) * decay), 0.0)
        rise = jnp.exp((inside + 1.0) * decay)
        fall = jnp.exp((BLOCK - 1.0 - inside) * decay)
        step = jnp.exp(jnp.full((8, vw), BLOCK * 1.0, F32) * decay)
        within[h] = mask
        rising[h] = rise
        falling[h] = fall
        carry[h] = step
        trailing = jnp.zeros((kw, vw), F32)
        for n in reversed(range(nblocks)):
            at = slice(n * BLOCK, (n + 1) * BLOCK)
            cosine, sine = cosv[at, :], sinv[at, :]
            q, v, c = rq[at, kc], vals[at, vc], call[at, vc]
            mixing = (dot_nt(c, v) * mask).astype(BF16)
            mix[at, pl.ds(pl.multiple_of(h * BLOCK, BLOCK), BLOCK)] = mixing
            trail = trailing.astype(BF16)
            held[h * nblocks + n] = trail
            grad = dot_tn(mixing, q) + fall * dot_nt(v, trail)
            back = (grad * cosine - pltpu.roll(grad, half, 1) * sine) * factor
            gk[at, kc] = back.astype(BF16)
            gkt[kc, at] = back.T.astype(BF16)
            decayed = (q.astype(F32) * rise).astype(BF16)
            trailing = trailing * step[0:1, :] + dot_tn(decayed, c)
        entering[h] = jnp.zeros((kw, vw), F32)
        return 0

    lax.fori_loop(0, heads, key_head, 0)

    def gk_send_head(h):
        for j in range(1, nsp):
            peer = (s + j) % nsp
            source = gk.at[
                pl.ds(pl.multiple_of(peer * rows, rows), rows),
                pl.ds(pl.multiple_of(h * kw, kw), kw),
            ]
            to = gkall.at[:, pl.ds(pl.multiple_of(s * feats + h * kw, kw), kw)]
            remote(source, to, gk_sent.at[0], gk_recv.at[0], {"sp": peer}).start()

    def half_copy(j):
        return remote(pwo.at[j], rp.at[j], half_send.at[0], half_recv.at[j], partner)

    def line_copy(j, side, target):
        return remote(
            lsend.at[j], lrecv.at[side, j], line_send.at[0],
            line_recv.at[side * nchunks + j], target,
        )

    def cast_copy(j, h, target, last_leg=False):
        ref = fin.at[j, pl.ds(h * (wrows // 2), wrows // 2), :]
        sem = cast_recv.at[nchunks if last_leg else j]
        return remote(ref, ref, cast_send.at[0], sem, {"sp": target})

    def cast_side(j):
        @pl.when(on_x)
        def _():
            received(fin.at[j, :wrows // 2, :], cast_recv.at[j])
            cast_copy(j, 0, yn).start()

        @pl.when(on_y)
        def _():
            received(fin.at[j, wrows // 2:, :], cast_recv.at[j])
            cast_copy(j, 1, xn).start()

    def cast_across(j):
        @pl.when(on_d)
        def _():
            received(fin.at[j], cast_recv.at[j])
            cast_copy(j, 0, xn, True).start()
            cast_copy(j, 1, yn, True).start()

    def gradient_columns(j):
        token_wait(j, 4, 1)
        at = pl.ds(pl.multiple_of(j * COLS, COLS), COLS)
        theirs = pl.ds(pl.multiple_of((1 - core) * wrows, wrows), wrows)
        mine = pl.ds(pl.multiple_of(core * wrows, wrows), wrows)
        pwo[j] = dot_nn(gkt[theirs, :], tall[:, at]).astype(BF16)
        half_copy(j).start()
        acc[j] = dot_nn(gkt[mine, :], tall[:, at])

    def sum_line(j):
        half_copy(j).wait_recv()
        acc[j] = acc[j] + rp[j].astype(F32)

        @pl.when((z >= s) & (z < nz - 1))
        def _():
            line_copy(j, 1, down).wait_recv()
            acc[j] = acc[j] + lrecv[1, j].astype(F32)

        @pl.when((z <= s) & (z > 0))
        def _():
            line_copy(j, 0, up).wait_recv()
            acc[j] = acc[j] + lrecv[0, j].astype(F32)

        @pl.when(owner)
        def _():
            fin[j] = acc[j].astype(BF16)
            cast_copy(j, 0, xn).start()
            cast_copy(j, 1, yn).start()

        @pl.when(jnp.logical_not(owner))
        def _():
            lsend[j] = acc[j].astype(BF16)

        @pl.when(z > s)
        def _():
            line_copy(j, 1, down).start()

        @pl.when(z < s)
        def _():
            line_copy(j, 0, up).start()

    def make_keys():
        pair_wait(s)
        left = pl.ds(pl.multiple_of(s * feats, feats), feats)

        def tile(i, _):
            at = pl.ds(pl.multiple_of(i * TILE, TILE), TILE)
            keys[at, :] = dot_nt(tall[at, :], wall[left, :]).astype(BF16)
            return 0

        lax.fori_loop(0, seq_len // TILE, tile, 0)

    def gq_copy(n):
        span = BLOCK * heads
        at = pl.ds(pl.multiple_of(n * span, span), span)
        return pltpu.make_async_copy(gq4.at[at, :], gq_out.at[at, :], gq_store.at[0])

    def gv_copy(n):
        span = BLOCK * heads * parts
        at = pl.ds(pl.multiple_of(n * span, span), span)
        return pltpu.make_async_copy(gv8.at[at, :], gv_out.at[at, :], gv_store.at[0])

    def query_block(n):
        at = pl.ds(pl.multiple_of(n * BLOCK, BLOCK), BLOCK)
        cosine, sine = cosv[at, :], sinv[at, :]
        for h in range(heads):
            kc, vc = slice(h * kw, (h + 1) * kw), slice(h * vw, (h + 1) * vw)
            key = keys[at, kc].astype(F32)
            rk = ((key * cosine + pltpu.roll(key, half, 1) * sine) * factor).astype(BF16)
            q, v, c = rq[at, kc], vals[at, vc], call[at, vc]
            state = entering[h]
            grad = dot_nn(mix[at, h * BLOCK:(h + 1) * BLOCK], rk)
            grad = grad + rising[h] * dot_nt(c, state.astype(BF16))
            xs[pl.ds(h, BLOCK, stride=heads), :] = (
                grad * cosine - pltpu.roll(grad, half, 1) * sine
            )
            scores = (dot_nt(q, rk) * within[h]).astype(BF16)
            fall = falling[h]
            inner = dot_tn(scores, c)
            outer = dot_nn(rk, held[h * nblocks + n])
            for i in range(parts):
                lane = slice(i * LANES, (i + 1) * LANES)
                ys[pl.ds(i * heads + h, BLOCK, stride=heads * parts), :] = (
                    inner[:, lane] + fall * outer[:, lane]
                )
            decayed = (rk.astype(F32) * fall).astype(BF16)
            entering[h] = state * carry[h, 0:1, :] + dot_tn(decayed, v)
        span = BLOCK * heads
        gq4[pl.ds(pl.multiple_of(n * span, span), span), :] = xs[...].astype(BF16)
        span = BLOCK * heads * parts
        gv8[pl.ds(pl.multiple_of(n * span, span), span), :] = ys[...].astype(BF16)
        gq_copy(n).start()
        gv_copy(n).start()

    def gather_keys():
        received(gkall.at[:, :(nsp - 1) * feats], gk_recv.at[0])
        gkall[:, pl.ds(pl.multiple_of(s * feats, feats), feats)] = gk[
            pl.ds(pl.multiple_of(s * rows, rows), rows), :
        ]
        for zb in range(nz):
            @pl.when((zb != s) & (zb != tardy))
            def _():
                pair_wait(zb)

    def gt_copy(i):
        at = pl.ds(pl.multiple_of(i * TILE, TILE), TILE)
        return pltpu.make_async_copy(gt.at[:, at], gt_out.at[:, at], gt_store.at[0])

    def block_product(zb, at):
        inner = pl.ds(pl.multiple_of(zb * feats, feats), feats)
        return dot_nn(gkall[:, inner], wall[inner, at])

    def token_gradient(i):
        at = pl.ds(pl.multiple_of(i * TILE, TILE), TILE)
        total = block_product((tardy + 1) % nz, at)
        for j in range(2, nz):
            total = total + block_product((tardy + j) % nz, at)
        gtf[i] = total

    def complete(i):
        at = pl.ds(pl.multiple_of(i * TILE, TILE), TILE)
        gt[:, at] = (gtf[i] + block_product(tardy, at)).astype(BF16)
        gt_copy(i).start()

    last = nchunks + 1 + (nz + 1) * HOP

    def turn(t, _):
        @pl.when(t < nchunks)
        def _():
            token_wait(t, 2, 0)
            token_send(t, 4).start()
            token_send(t, 5).start()

        @pl.when(t + 2 < nchunks)
        def _():
            for i in range(4):
                token_send(t + 2, i).start()

        @pl.when((t >= 1) & (t <= nchunks))
        def _():
            gradient_columns(t - 1)

        j = t - 2 - behind * HOP

        @pl.when((j >= 0) & (j < nchunks))
        def _():
            sum_line(j)

        jx = t - 2 - (far + 1) * HOP

        @pl.when((jx >= 0) & (jx < nchunks))
        def _():
            cast_side(jx)

        jd = t - 2 - (far + 2) * HOP

        @pl.when((jd >= 0) & (jd < nchunks))
        def _():
            cast_across(jd)

        @pl.when((t >= nchunks - 1) & (t < nchunks - 1 + heads))
        def _():
            gk_send_head(t - (nchunks - 1))

        beat, on_beat = t // unit, t % unit == 0

        for p in range(pieces):
            when = jnp.where(patient, sum_step, sends[p]) if p == pieces - 1 else sends[p]

            @pl.when(t == when)
            def _():
                relay_inward(p)

            when = jnp.where(awaits, sum_step + 4, takes[p]) if p == pieces - 1 else takes[p]

            @pl.when(t == when)
            def _():
                take_inward(p)

        after = t - nchunks - 1
        slot = after // 2
        on_slot = (after >= 0) & (after < 2 * pieces) & (after % 2 == 0)
        ahead = jnp.where(opposite, beat - pieces, beat - 2)

        @pl.when(on_beat & (ahead >= 0) & (ahead < pieces))
        def _():
            @pl.when(opposite)
            def _():
                relay_third(ahead)

            @pl.when(jnp.logical_not(opposite))
            def _():
                relay_second(ahead)

        @pl.when(on_slot)
        def _():
            @pl.when(opposite)
            def _():
                relay_second(slot)

            @pl.when(jnp.logical_not(opposite))
            def _():
                relay_third(slot)

        @pl.when(t == unit * (pieces + 2))
        def _():
            relay_rest()

        @pl.when(t == nchunks)
        def _():
            make_keys()

        @pl.when((after >= 0) & (after < nblocks // 2))
        def _():
            query_block(2 * after)
            query_block(2 * after + 1)

        i = t - tile_step

        @pl.when(i == 0)
        def _():
            gather_keys()

        @pl.when((i >= 0) & (i < ntiles // 2))
        def _():
            token_gradient(2 * i)
            token_gradient(2 * i + 1)

        @pl.when(t == last - 3)
        def _():
            take_side()

        @pl.when(t == last - 2)
        def _():
            @pl.when(tardy != s)
            def _():
                pair_wait(tardy)

        @pl.when((t == last - 2) | (t == last - 1))
        def _():
            first = (t - (last - 2)) * (ntiles // 2)
            for i in range(ntiles // 2):
                complete(first + i)

        return 0

    ntiles = width // TILE
    tile_step = nchunks + 5
    unit = nchunks // 8
    sends = [unit * (p * (p + 3) // 4) for p in range(pieces)]
    takes = [unit * (2 * p + 3) for p in range(pieces)]
    sum_step = nchunks + 1 + HOP
    outer = (s == 0) | (s == nz - 1)
    patient = outer & (behind == 1) & jnp.logical_not(owner)
    awaits = outer & (behind == 2) & jnp.logical_not(owner)
    lax.fori_loop(0, last + 1, turn, 0)
    @pl.when(on_x | on_y)
    def _():
        received(fin.at[:nchunks // 2], cast_recv.at[nchunks])

    gw_copy = pltpu.make_async_copy(fin, gw_out, gw_store.at[0])
    gw_copy.start()

    sent(cotv.at[:, :(nsp - 1) * cwidth], cot_send.at[0])
    sent(tall.at[:6 * hrows, :], tok_send.at[0])
    sent(gk.at[:(nsp - 1) * rows, :], gk_sent.at[0])
    sent(pwo, half_send.at[0])

    @pl.when(jnp.logical_not(owner))
    def _():
        sent(lsend, line_send.at[0])

    @pl.when(owner | on_d)
    def _():
        sent(fin, cast_send.at[0])

    @pl.when(on_x | on_y)
    def _():
        sent(fin.at[:nchunks // 2], cast_send.at[0])

    for d in range(nz - 1):
        @pl.when(goes_up(d))
        def _():
            sent(wall.at[:wrows, :], up_send.at[d])

        @pl.when(goes_down(d))
        def _():
            sent(wall.at[:wrows, :], down_send.at[d])

    sent(wall.at[:nz * wrows, :], pair_send.at[0])

    @pl.when(side_x | side_y)
    def _():
        sent(wall.at[:wrows // 2, :], side_send.at[0])

    pltpu.make_async_copy(gq4, gq_out, gq_store.at[0]).wait()
    pltpu.make_async_copy(gv8, gv_out, gv_store.at[0]).wait()
    pltpu.make_async_copy(gt, gt_out, gt_store.at[0]).wait()
    gw_copy.wait()


def whole(tokens, weight, queries, values, cotan, decay, nsp, ndp, heads):
    nz = ndp // CORES
    rows, width = tokens.shape
    wrows = weight.shape[0]
    seq_len = rows * nsp
    kw = queries.shape[1]
    feats = heads * kw
    cwidth = cotan.shape[1] // nsp
    vw = cwidth // heads
    nblocks = seq_len // BLOCK
    nchunks = width // COLS
    cosine, sine = rotation_tables(seq_len, kw // 2)
    dma = pltpu.SemaphoreType.DMA
    anywhere = pl.BlockSpec(memory_space=pl.ANY)

    def buffer(*shape):
        return pltpu.VMEM(shape, BF16)

    def wide(*shape):
        return pltpu.VMEM(shape, F32)

    return pl.pallas_call(
        functools.partial(whole_kernel, nsp, nz, heads),
        in_specs=[pl.BlockSpec(memory_space=pltpu.SMEM)] + [anywhere] * 7,
        out_specs=[anywhere] * 4,
        out_shape=[
            jax.ShapeDtypeStruct((rows, width), BF16),
            jax.ShapeDtypeStruct(queries.shape, BF16),
            jax.ShapeDtypeStruct(values.shape, BF16),
            jax.ShapeDtypeStruct((nchunks, wrows, COLS), BF16),
        ],
        scratch_shapes=[
            buffer(rows, nsp * cwidth),
            buffer(seq_len, width),
            buffer(wrows * ndp, width),
            buffer(seq_len, cwidth),
            buffer(*queries.shape),
            buffer(*values.shape),
            wide(seq_len, kw),
            wide(seq_len, kw),
            buffer(seq_len, feats),
            buffer(seq_len, cwidth),
            buffer(seq_len, heads * BLOCK),
            buffer(heads * nblocks, kw, vw),
            buffer(seq_len, feats),
            buffer(feats, seq_len),
            buffer(rows, nsp * feats),
            buffer(seq_len, feats),
            buffer(*queries.shape),
            buffer(*values.shape),
            buffer(rows, width),
            wide(width // TILE, rows, TILE),
            wide(nchunks, wrows, COLS),
            buffer(nchunks, wrows, COLS),
            buffer(nchunks, wrows, COLS),
            buffer(2, nchunks, wrows, COLS),
            buffer(nchunks, wrows, COLS),
            buffer(nchunks, wrows, COLS),
            wide(BLOCK * heads, kw),
            wide(BLOCK * heads * (vw // LANES), LANES),
            wide(heads, BLOCK, BLOCK),
            wide(heads, BLOCK, kw),
            wide(heads, BLOCK, kw),
            wide(heads, 8, vw),
            wide(heads, kw, vw),
            dma((8,)),
            dma((1,)), dma(((nsp - 1) * heads,)),
            dma((1,)), dma((2 * nchunks,)),
            dma((nz - 1,)), dma(((nz - 1) * heads,)),
            dma((nz - 1,)), dma(((nz - 1) * heads,)),
            dma((1,)), dma((nz,)),
            dma((1,)), dma((1,)),
            dma((1,)), dma((1,)),
            dma((1,)), dma((nchunks,)),
            dma((1,)), dma((2 * nchunks,)),
            dma((1,)), dma((nchunks + 1,)),
            dma((1,)), dma((1,)), dma((1,)), dma((1,)),
        ],
        compiler_params=pltpu.CompilerParams(
            has_side_effects=True, vmem_limit_bytes=VMEM_LIMIT, collective_id=0
        ),
        name="whole",
    )(decay, tokens, weight, queries, values, cotan, jnp.asarray(cosine), jnp.asarray(sine))


def finish_kernel(gt, gq, gv, gw, gt_out, gq_out, gv_out, gw_out, bt, bq, bv, bw, bf, get, put):
    chunks, wrows = gw.shape[:2]
    reads, writes = [], []
    for source, held, target, count in (
        (gw, bw, None, 2), (gv, bv, gv_out, 4), (gq, bq, gq_out, 2), (gt, bt, gt_out, 2)
    ):
        axis = source.shape[0] // count
        for i in range(count):
            at = pl.ds(i * axis, axis)
            n = len(reads)
            reads.append(pltpu.make_async_copy(source.at[at], held.at[at], get.at[n]))
            if target is not None:
                writes.append(pltpu.make_async_copy(held.at[at], target.at[at], put.at[n]))
            else:
                into = pl.ds(i * axis * COLS, axis * COLS)
                writes.append(pltpu.make_async_copy(bf.at[:, into], gw_out.at[:, into], put.at[n]))
    for read in reads:
        read.start()
    for n, (read, write) in enumerate(zip(reads, writes)):
        read.wait()
        if n < 2:
            for j in range(n * chunks // 2, (n + 1) * chunks // 2):
                bf[:, j * COLS:(j + 1) * COLS] = bw[j].astype(F32)
        write.start()
    for write in writes:
        write.wait()


def finish(gt, gq, gv, gw):
    chunks, wrows, cols = gw.shape
    arrays = [gt, gq, gv, gw]
    total = (wrows, chunks * cols)
    anywhere = pl.BlockSpec(memory_space=pl.ANY)
    return pl.pallas_call(
        finish_kernel,
        in_specs=[anywhere] * 4,
        out_specs=[anywhere] * 4,
        out_shape=[jax.ShapeDtypeStruct(array.shape, BF16) for array in arrays[:3]]
        + [jax.ShapeDtypeStruct(total, F32)],
        scratch_shapes=[pltpu.VMEM(array.shape, BF16) for array in arrays]
        + [pltpu.VMEM(total, F32), pltpu.SemaphoreType.DMA((10,)), pltpu.SemaphoreType.DMA((10,))],
        compiler_params=pltpu.CompilerParams(vmem_limit_bytes=VMEM_LIMIT),
        name="finish",
    )(gt, gq, gv, gw)


def gather_general(tokens, weight, cotan):
    gathered = lax.all_gather(weight, "dp", axis=0, tiled=True)
    rows = gathered.shape[0] // lax.axis_size("sp")
    chosen = lax.dynamic_slice_in_dim(gathered, lax.axis_index("sp") * rows, rows)
    return (
        lax.all_gather(tokens, "sp", axis=0, tiled=True),
        chosen,
        lax.all_to_all(cotan, "sp", split_axis=1, concat_axis=0, tiled=True),
    )


def scatter_general(partial_tokens, partial_weight):
    grad_tokens = lax.psum_scatter(
        partial_tokens, "sp", scatter_dimension=0, tiled=True
    ).astype(BF16)
    owned = lax.psum_scatter(
        partial_weight, "dp", scatter_dimension=0, tiled=True
    )
    everything = lax.all_gather(owned, ("sp", "dp"), axis=0, tiled=True)
    rows = everything.shape[0] // lax.axis_size("dp")
    return grad_tokens, lax.dynamic_slice_in_dim(
        everything, lax.axis_index("dp") * rows, rows
    )


def body(nsp, ndp, tokens, key_weight, queries, values, cotangent, log_decay):
    seq_len, heads, kw = queries.shape[1:]
    vw = values.shape[3]
    if nsp == 4 and ndp == CORES * nsp and kw == BLOCK:
        parts = vw // LANES
        flat = values.reshape(seq_len, heads, parts, LANES).transpose(0, 2, 1, 3)
        grad_tokens, grad_query, grad_value, weight_grad = whole(
            tokens[0], key_weight, queries.reshape(-1, kw), flat.reshape(-1, LANES),
            cotangent[0], log_decay, nsp, ndp, heads,
        )
        grad_tokens, grad_query, grad_value, weight_grad = finish(
            grad_tokens, grad_query, grad_value, weight_grad
        )
        grad_value = grad_value.reshape(seq_len, parts, heads, LANES).transpose(0, 2, 1, 3)
    else:
        all_tokens, weight, cotan = gather_general(tokens[0], key_weight, cotangent[0])
        keys = dot_nt(all_tokens, weight).astype(BF16)
        grad_query, grad_key, _, grad_value = retention_backward(
            queries.reshape(seq_len, -1), keys, values.reshape(seq_len, -1), cotan, log_decay, heads
        )
        grad_tokens, weight_grad = scatter_general(
            dot_nn(grad_key, weight), dot_tn(grad_key, all_tokens)
        )
    return (
        grad_tokens[None],
        grad_query.reshape(queries.shape),
        grad_value.reshape(values.shape),
        weight_grad,
    )


def solution(mesh):
    return jax.shard_map(
        functools.partial(body, mesh.shape["sp"], mesh.shape["dp"]),
        mesh=mesh,
        in_specs=(
            P("dp", "sp", None),
            P("dp", None),
            P("dp", None, "sp", None),
            P("dp", None, "sp", None),
            P("dp", "sp", None),
            P(),
        ),
        out_specs=(
            P("dp", "sp", None),
            P("dp", None, "sp", None),
            P("dp", None, "sp", None),
            P("dp", None),
        ),
        check_vma=False,
    )
```

```python
import functools

import jax
import jax.numpy as jnp
import numpy as np
from jax import lax
from jax.experimental import pallas as pl
from jax.experimental.pallas import tpu as pltpu
from jax.sharding import PartitionSpec as P

BLOCK = 128
CORES = 2
MESH = pl.DeviceIdType.MESH
F32 = jnp.float32
BF16 = jnp.bfloat16
VMEM_LIMIT = 60 * 1024 * 1024


def rotation_tables(seq_len, half):
    position = np.arange(seq_len, dtype=np.float32)
    frequency = (10000.0 ** (-np.arange(half, dtype=np.float32) / half)).astype(np.float32)
    angle = (position[:, None] * frequency[None, :]).astype(np.float32)
    cosine, sine = np.cos(angle), np.sin(angle)
    return (
        np.concatenate([cosine, cosine], axis=1).astype(np.float32),
        np.concatenate([-sine, sine], axis=1).astype(np.float32),
    )


def dot_nt(a, b):
    return lax.dot_general(a, b, (((1,), (1,)), ((), ())), preferred_element_type=F32)


def dot_tn(a, b):
    return lax.dot_general(a, b, (((0,), (0,)), ((), ())), preferred_element_type=F32)


def dot_nn(a, b):
    return lax.dot_general(a, b, (((1,), (0,)), ((), ())), preferred_element_type=F32)


def retention_kernel(
    decay_ref, q_ref, k_ref, v_ref, c_ref, cos_ref, sin_ref,
    gq_ref, gk_ref, gkt_ref, gv_ref, rq_ref, rk_ref, mix_ref,
):
    seq_len, key_width = q_ref.shape
    value_width = v_ref.shape[1]
    nblocks = seq_len // BLOCK
    half = key_width // 2
    factor = key_width ** (-0.5)
    decay = decay_ref[lax.axis_index("sp") * pl.num_programs(0) + pl.program_id(0)]
    row = lax.broadcasted_iota(jnp.int32, (BLOCK, BLOCK), 0).astype(F32)
    col = lax.broadcasted_iota(jnp.int32, (BLOCK, BLOCK), 1).astype(F32)
    within = jnp.where(row >= col, jnp.exp(jnp.maximum(row - col, 0.0) * decay), 0.0)
    inside = lax.broadcasted_iota(jnp.int32, (BLOCK, key_width), 0).astype(F32)
    rising = jnp.exp((inside + 1.0) * decay)
    falling = jnp.exp((BLOCK - 1.0 - inside) * decay)
    wide = lax.broadcasted_iota(jnp.int32, (BLOCK, value_width), 0).astype(F32)
    falling_wide = jnp.exp((BLOCK - 1.0 - wide) * decay)
    carry_decay = jnp.exp(jnp.full((key_width, value_width), BLOCK * 1.0, F32) * decay)
    zero = jnp.zeros((key_width, value_width), F32)

    def forward(n, entering):
        rows = pl.ds(pl.multiple_of(n * BLOCK, BLOCK), BLOCK)
        cosine, sine = cos_ref[rows, :], sin_ref[rows, :]
        q = q_ref[rows, :].astype(F32)
        k = k_ref[rows, :].astype(F32)
        rq = (q * cosine + pltpu.roll(q, half, 1) * sine).astype(BF16)
        rk = ((k * cosine + pltpu.roll(k, half, 1) * sine) * factor).astype(BF16)
        rq_ref[rows, :] = rq
        rk_ref[rows, :] = rk
        v, c = v_ref[rows, :], c_ref[rows, :]
        mixing = (dot_nt(c, v) * within).astype(BF16)
        mix_ref[rows, :] = mixing
        grad = dot_nn(mixing, rk) + rising * dot_nt(c, entering.astype(BF16))
        gq_ref[rows, :] = (grad * cosine - pltpu.roll(grad, half, 1) * sine).astype(BF16)
        decayed = (rk.astype(F32) * falling).astype(BF16)
        return entering * carry_decay + dot_tn(decayed, v)

    def backward(step, trailing):
        n = nblocks - 1 - step
        rows = pl.ds(pl.multiple_of(n * BLOCK, BLOCK), BLOCK)
        cosine, sine = cos_ref[rows, :], sin_ref[rows, :]
        rq, rk, mixing = rq_ref[rows, :], rk_ref[rows, :], mix_ref[rows, :]
        v, c = v_ref[rows, :], c_ref[rows, :]
        held = trailing.astype(BF16)
        scores = (dot_nt(rq, rk) * within).astype(BF16)
        grad = dot_tn(mixing, rq) + falling * dot_nt(v, held)
        back = (grad * cosine - pltpu.roll(grad, half, 1) * sine) * factor
        gk_ref[rows, :] = back.astype(BF16)
        gkt_ref[:, rows] = back.T.astype(BF16)
        gv_ref[rows, :] = (dot_tn(scores, c) + falling_wide * dot_nn(rk, held)).astype(BF16)
        decayed = (rq.astype(F32) * rising).astype(BF16)
        return trailing * carry_decay + dot_tn(decayed, c)

    unroll = min(nblocks, 8)
    lax.fori_loop(0, nblocks, forward, zero, unroll=unroll)
    lax.fori_loop(0, nblocks, backward, zero, unroll=unroll)


def retention_backward(queries, keys, values, cotan, decay, heads):
    seq_len = queries.shape[0]
    kw = queries.shape[1] // heads
    vw = values.shape[1] // heads
    cosine, sine = rotation_tables(seq_len, kw // 2)
    narrow = pl.BlockSpec((seq_len, kw), lambda h: (0, h))
    wide = pl.BlockSpec((seq_len, vw), lambda h: (0, h))
    table = pl.BlockSpec((seq_len, kw), lambda h: (0, 0))
    flops = 2 * seq_len * heads * BLOCK * (3 * kw + 2 * vw + 5 * vw)
    return pl.pallas_call(
        retention_kernel,
        grid=(heads,),
        in_specs=[pl.BlockSpec(memory_space=pltpu.SMEM), narrow, narrow, wide, wide, table, table],
        out_specs=[narrow, narrow, pl.BlockSpec((kw, seq_len), lambda h: (h, 0)), wide],
        out_shape=[
            jax.ShapeDtypeStruct(queries.shape, BF16),
            jax.ShapeDtypeStruct(queries.shape, BF16),
            jax.ShapeDtypeStruct(queries.shape[::-1], BF16),
            jax.ShapeDtypeStruct(values.shape, BF16),
        ],
        scratch_shapes=[
            pltpu.VMEM((seq_len, kw), BF16),
            pltpu.VMEM((seq_len, kw), BF16),
            pltpu.VMEM((seq_len, BLOCK), BF16),
        ],
        compiler_params=pltpu.CompilerParams(vmem_limit_bytes=VMEM_LIMIT),
        cost_estimate=pl.CostEstimate(
            flops=flops, bytes_accessed=8 * seq_len * heads * (kw + vw), transcendentals=0
        ),
        name="retention",
    )(decay, queries, keys, values, cotan, jnp.asarray(cosine), jnp.asarray(sine))


def remote(src, dst, send, recv, target):
    return pltpu.make_async_remote_copy(
        src_ref=src, dst_ref=dst, send_sem=send, recv_sem=recv,
        device_id=target, device_id_type=MESH,
    )


def greet(nsp, nz, s, z, core):
    barrier = pltpu.get_barrier_semaphore()
    others = [{"dp": z * CORES + 1 - core}]
    others += [{"sp": (s + j) % nsp} for j in range(1, nsp)]
    for other in others:
        pl.semaphore_signal(barrier, inc=1, device_id=other, device_id_type=MESH)

    @pl.when(z > 0)
    def _():
        below = {"dp": (z - 1) * CORES + core}
        pl.semaphore_signal(barrier, inc=1, device_id=below, device_id_type=MESH)

    @pl.when(z < nz - 1)
    def _():
        above = {"dp": (z + 1) * CORES + core}
        pl.semaphore_signal(barrier, inc=1, device_id=above, device_id_type=MESH)

    ends = jnp.where(z > 0, 1, 0) + jnp.where(z < nz - 1, 1, 0)
    pl.semaphore_wait(barrier, len(others) + ends)


TILE = 256
LANES = 128
COLS = 256
HOP = 2
CAST = 3


def whole_kernel(
    nsp, nz, heads,
    decay_ref, tok_in, w_in, q_in, v_in, cot_in, cos_in, sin_in,
    gt_out, gq_out, gv_out, gw_out,
    cotv, tall, wall, call, q4, v8, cosv, sinv, rq, vals, mix, held, gk, gkt, gkall,
    keys, gq4, gv8, gt, gtf, acc, pwo, rp, lrecv, lsend, fin, xs, ys,
    within, rising, falling, carry, entering,
    load, cot_send, cot_recv, tok_send, tok_recv,
    up_send, up_recv, down_send, down_recv, pair_send, pair_recv, side_send, side_recv,
    gk_sent, gk_recv, half_send, half_recv, line_send, line_recv,
    cast_send, cast_recv, gq_store, gv_store, gw_store, gt_store,
):
    s = lax.axis_index("sp")
    k = lax.axis_index("dp")
    z, core = k // CORES, k % CORES
    x, y = s % 2, s // 2
    xn, yn = y * 2 + (1 - x), (1 - y) * 2 + x
    diagonal = (1 - y) * 2 + (1 - x)
    partner = {"dp": z * CORES + 1 - core}
    up, down = {"dp": k + CORES}, {"dp": k - CORES}
    rows, width = tok_in.shape
    wrows = w_in.shape[0]
    seq_len, feats = gk.shape
    kw = feats // heads
    cwidth = call.shape[1]
    vw = cwidth // heads
    parts = vw // LANES
    nblocks = seq_len // BLOCK
    half = kw // 2
    factor = kw ** (-0.5)
    hrows = rows // 2
    nchunks = width // COLS
    pieces = heads
    prow = wrows // pieces

    far = jnp.maximum(z, nz - 1 - z)
    behind = jnp.where(z > s, nz - 1 - z, jnp.where(z < s, z, far))
    owner = z == s
    dx, dy = x != z % 2, y != z // 2
    on_x = dx & jnp.logical_not(dy)
    on_y = dy & jnp.logical_not(dx)
    on_d = dx & dy
    edge = (z == 0) | (z == nz - 1)
    corner = owner & edge
    side_x, side_y = on_x & edge, on_y & edge
    apart = jnp.maximum(z - s, s - z)
    opposite = apart == nz - 1
    yields_up = (s == 0) & (z == nz - 2)
    yields_down = (s == nz - 1) & (z == 1)
    farthest = jnp.where(z < nz // 2, nz - 1, 0)
    tardy = jnp.where(opposite, jnp.where(z == 0, nz - 2, 1), farthest)

    loads = [
        pltpu.make_async_copy(cot_in, cotv, load.at[0]),
        pltpu.make_async_copy(w_in, wall.at[pl.ds(pl.multiple_of(k * wrows, wrows), wrows), :], load.at[1]),
        pltpu.make_async_copy(tok_in, tall.at[pl.ds(pl.multiple_of(s * rows, rows), rows), :], load.at[2]),
        pltpu.make_async_copy(
            cot_in.at[:, pl.ds(pl.multiple_of(s * cwidth, cwidth), cwidth)],
            call.at[pl.ds(pl.multiple_of(s * rows, rows), rows), :], load.at[3],
        ),
        pltpu.make_async_copy(q_in, q4, load.at[4]),
        pltpu.make_async_copy(v_in, v8, load.at[5]),
        pltpu.make_async_copy(cos_in, cosv, load.at[6]),
        pltpu.make_async_copy(sin_in, sinv, load.at[7]),
    ]
    for copy in loads:
        copy.start()
    greet(nsp, nz, s, z, core)

    def received(ref, sem):
        remote(ref, ref, load.at[0], sem, partner).wait_recv()

    def sent(ref, sem):
        remote(ref, ref, sem, load.at[0], partner).wait_send()

    def cot_copy(j, h, source):
        peer = (s + j) % nsp
        columns = pl.ds(pl.multiple_of(peer * cwidth + h * vw, vw), vw)
        to = call.at[
            pl.ds(pl.multiple_of(source * rows, rows), rows), pl.ds(pl.multiple_of(h * vw, vw), vw)
        ]
        i = (j - 1) * heads + h
        return remote(cotv.at[:, columns], to, cot_send.at[0], cot_recv.at[i], {"sp": peer})

    loads[0].wait()
    for h in range(heads):
        for j in range(1, nsp):
            cot_copy(j, h, s).start()

    def piece(zb, c, p):
        start = pl.multiple_of((zb * CORES + c) * wrows + p * prow, prow)
        return wall.at[pl.ds(start, prow), :]

    def up_copy(d, p):
        ref, i = piece(z - d, core, p), d * pieces + p
        return remote(ref, ref, up_send.at[d], up_recv.at[i], up)

    def down_copy(d, p):
        ref, i = piece(z + d, core, p), d * pieces + p
        return remote(ref, ref, down_send.at[d], down_recv.at[i], down)

    def pair_copy(zb, p):
        ref = piece(zb, core, p)
        return remote(ref, ref, pair_send.at[0], pair_recv.at[zb], partner)

    def pair_wait(zb):
        received(wall.at[:wrows, :], pair_recv.at[zb])

    loads[1].wait()
    for p in range(pieces):
        @pl.when(z < nz - 1)
        def _():
            up_copy(0, p).start()

        @pl.when(z > 0)
        def _():
            down_copy(0, p).start()

        pair_copy(z, p).start()

    def goes_up(d):
        return (z >= d) & (z < nz - 1 if d < nz - 2 else (z < nz - 1) & (s != nz - 1))

    def goes_down(d):
        return (z + d < nz) & (z > 0 if d < nz - 2 else (z > 0) & (s != 0))

    def side_copy(p, part, target):
        zb = nz - 1 - z
        start = pl.multiple_of((zb * CORES + core) * wrows + p * prow + part * (prow // 2), prow // 2)
        ref = wall.at[pl.ds(start, prow // 2), :]
        return remote(ref, ref, side_send.at[0], side_recv.at[0], {"sp": target})

    def rise_of(d, p):
        received(piece(z - d, core, p), up_recv.at[(d - 1) * pieces + p])
        pair_copy(z - d, p).start()

    def fall_of(d, p):
        received(piece(z + d, core, p), down_recv.at[(d - 1) * pieces + p])
        pair_copy(z + d, p).start()

    def relay_first(p):
        @pl.when(z > 0)
        def _():
            rise_of(1, p)

        @pl.when(goes_up(1) & (z >= s) & prompt(p, yields_up))
        def _():
            up_copy(1, p).start()

        @pl.when(z < nz - 1)
        def _():
            fall_of(1, p)

        @pl.when(goes_down(1) & (z <= s) & prompt(p, yields_down))
        def _():
            down_copy(1, p).start()

    def relay_inward(p):
        @pl.when(goes_up(1) & (z < s))
        def _():
            up_copy(1, p).start()

        @pl.when(goes_down(1) & (z > s))
        def _():
            down_copy(1, p).start()

    def relay_second(p):
        @pl.when((z >= 2) & (z > s))
        def _():
            rise_of(2, p)

        @pl.when(goes_up(2) & (z > s))
        def _():
            up_copy(2, p).start()

        @pl.when((z + 2 < nz) & (z < s))
        def _():
            fall_of(2, p)

        @pl.when(goes_down(2) & (z < s))
        def _():
            down_copy(2, p).start()

    def take_inward(p):
        @pl.when((z >= 2) & (z <= s))
        def _():
            rise_of(2, p)

        @pl.when(goes_up(2) & (z == s))
        def _():
            up_copy(2, p).start()

        @pl.when((z + 2 < nz) & (z >= s))
        def _():
            fall_of(2, p)

        @pl.when(goes_down(2) & (z == s))
        def _():
            down_copy(2, p).start()

    def relay_third(p):
        @pl.when((z == nz - 1) & (s != z))
        def _():
            rise_of(3, p)

        @pl.when((z == 0) & (s != z))
        def _():
            fall_of(3, p)

        @pl.when(side_x)
        def _():
            side_copy(p, 0, xn).start()

        @pl.when(side_y)
        def _():
            side_copy(p, 1, yn).start()

    def prompt(p, yields):
        return jnp.logical_not(yields & (p > 0))

    def relay_rest():
        for p in range(1, pieces):
            @pl.when(yields_up)
            def _():
                up_copy(1, p).start()

            @pl.when(yields_down)
            def _():
                down_copy(1, p).start()

    def take_side():
        @pl.when(corner)
        def _():
            received(wall.at[:wrows, :], side_recv.at[0])
            for p in range(pieces):
                pair_copy(nz - 1 - z, p).start()

    def token(j, i, who, h, target):
        at = tall.at[
            pl.ds(pl.multiple_of(who * rows + h * hrows, hrows), hrows),
            pl.ds(pl.multiple_of(j * COLS, COLS), COLS),
        ]
        n = 2 * j + (0 if i < 2 else 1)
        return remote(at, at, tok_send.at[0], tok_recv.at[n], {"sp": target})

    def token_send(j, i):
        who, h, target = [
            (s, 0, xn), (s, 1, yn), (s, 1, xn), (s, 0, yn), (xn, 0, yn), (yn, 1, xn)
        ][i]
        return token(j, i, who, h, target)

    def token_wait(j, count, n):
        at = pl.ds(pl.multiple_of(j * COLS, COLS), COLS)
        received(tall.at[:count * hrows, at], tok_recv.at[2 * j + n])

    loads[2].wait()
    for j in range(2):
        for i in range(4):
            token_send(j, i).start()
    for copy in loads[3:]:
        copy.wait()

    def prepare(n, _):
        at = pl.ds(pl.multiple_of(n * BLOCK, BLOCK), BLOCK)
        cosine, sine = cosv[at, :], sinv[at, :]
        span = BLOCK * heads
        xs[...] = q4[pl.ds(pl.multiple_of(n * span, span), span), :].astype(F32)
        for h in range(heads):
            q = xs[pl.ds(h, BLOCK, stride=heads), :]
            rq[at, h * kw:(h + 1) * kw] = (q * cosine + pltpu.roll(q, half, 1) * sine).astype(BF16)
        span = BLOCK * heads * parts
        ys[...] = v8[pl.ds(pl.multiple_of(n * span, span), span), :].astype(F32)
        for h in range(heads):
            for i in range(parts):
                left = h * vw + i * LANES
                vals[at, left:left + LANES] = ys[
                    pl.ds(i * heads + h, BLOCK, stride=heads * parts), :
                ].astype(BF16)
        return 0

    lax.fori_loop(0, nblocks, prepare, 0)

    def key_head(h, _):
        relay_first(h)
        for j in range(1, nsp):
            cot_copy(j, h, (s - j + nsp) % nsp).wait_recv()
        kc = pl.ds(pl.multiple_of(h * kw, kw), kw)
        vc = pl.ds(pl.multiple_of(h * vw, vw), vw)
        decay = decay_ref[s * heads + h]
        row = lax.broadcasted_iota(jnp.int32, (BLOCK, BLOCK), 0).astype(F32)
        col = lax.broadcasted_iota(jnp.int32, (BLOCK, BLOCK), 1).astype(F32)
        inside = lax.broadcasted_iota(jnp.int32, (BLOCK, kw), 0).astype(F32)
        mask = jnp.where(row >= col, jnp.exp(jnp.maximum(row - col, 0.0) * decay), 0.0)
        rise = jnp.exp((inside + 1.0) * decay)
        fall = jnp.exp((BLOCK - 1.0 - inside) * decay)
        step = jnp.exp(jnp.full((8, vw), BLOCK * 1.0, F32) * decay)
        within[h] = mask
        rising[h] = rise
        falling[h] = fall
        carry[h] = step
        trailing = jnp.zeros((kw, vw), F32)
        for n in reversed(range(nblocks)):
            at = slice(n * BLOCK, (n + 1) * BLOCK)
            cosine, sine = cosv[at, :], sinv[at, :]
            q, v, c = rq[at, kc], vals[at, vc], call[at, vc]
            mixing = (dot_nt(c, v) * mask).astype(BF16)
            mix[at, pl.ds(pl.multiple_of(h * BLOCK, BLOCK), BLOCK)] = mixing
            trail = trailing.astype(BF16)
            held[h * nblocks + n] = trail
            grad = dot_tn(mixing, q) + fall * dot_nt(v, trail)
            back = (grad * cosine - pltpu.roll(grad, half, 1) * sine) * factor
            gk[at, kc] = back.astype(BF16)
            gkt[kc, at] = back.T.astype(BF16)
            decayed = (q.astype(F32) * rise).astype(BF16)
            trailing = trailing * step[0:1, :] + dot_tn(decayed, c)
        entering[h] = jnp.zeros((kw, vw), F32)
        return 0

    lax.fori_loop(0, heads, key_head, 0)

    def gk_send_head(h):
        for j in range(1, nsp):
            peer = (s + j) % nsp
            source = gk.at[
                pl.ds(pl.multiple_of(peer * rows, rows), rows),
                pl.ds(pl.multiple_of(h * kw, kw), kw),
            ]
            to = gkall.at[:, pl.ds(pl.multiple_of(s * feats + h * kw, kw), kw)]
            remote(source, to, gk_sent.at[0], gk_recv.at[0], {"sp": peer}).start()

    def half_copy(j):
        return remote(pwo.at[j], rp.at[j], half_send.at[0], half_recv.at[j], partner)

    def line_copy(j, side, target):
        return remote(
            lsend.at[j], lrecv.at[side, j], line_send.at[0],
            line_recv.at[side * nchunks + j], target,
        )

    def cast_copy(j, h, target, last_leg=False):
        ref = fin.at[j, pl.ds(h * (wrows // 2), wrows // 2), :]
        sem = cast_recv.at[nchunks if last_leg else j]
        return remote(ref, ref, cast_send.at[0], sem, {"sp": target})

    def cast_side(j):
        @pl.when(on_x)
        def _():
            received(fin.at[j, :wrows // 2, :], cast_recv.at[j])
            cast_copy(j, 0, yn).start()

        @pl.when(on_y)
        def _():
            received(fin.at[j, wrows // 2:, :], cast_recv.at[j])
            cast_copy(j, 1, xn).start()

    def cast_across(j):
        @pl.when(on_d)
        def _():
            received(fin.at[j], cast_recv.at[j])
            cast_copy(j, 0, xn, True).start()
            cast_copy(j, 1, yn, True).start()

    def gradient_columns(j):
        token_wait(j, 4, 1)
        at = pl.ds(pl.multiple_of(j * COLS, COLS), COLS)
        theirs = pl.ds(pl.multiple_of((1 - core) * wrows, wrows), wrows)
        mine = pl.ds(pl.multiple_of(core * wrows, wrows), wrows)
        pwo[j] = dot_nn(gkt[theirs, :], tall[:, at]).astype(BF16)
        half_copy(j).start()
        acc[j] = dot_nn(gkt[mine, :], tall[:, at])

    def sum_line(j):
        half_copy(j).wait_recv()
        acc[j] = acc[j] + rp[j].astype(F32)

        @pl.when((z >= s) & (z < nz - 1))
        def _():
            line_copy(j, 1, down).wait_recv()
            acc[j] = acc[j] + lrecv[1, j].astype(F32)

        @pl.when((z <= s) & (z > 0))
        def _():
            line_copy(j, 0, up).wait_recv()
            acc[j] = acc[j] + lrecv[0, j].astype(F32)

        @pl.when(owner)
        def _():
            fin[j] = acc[j].astype(BF16)
            cast_copy(j, 0, xn).start()
            cast_copy(j, 1, yn).start()

        @pl.when(jnp.logical_not(owner))
        def _():
            lsend[j] = acc[j].astype(BF16)

        @pl.when(z > s)
        def _():
            line_copy(j, 1, down).start()

        @pl.when(z < s)
        def _():
            line_copy(j, 0, up).start()

    def make_keys():
        pair_wait(s)
        left = pl.ds(pl.multiple_of(s * feats, feats), feats)

        def tile(i, _):
            at = pl.ds(pl.multiple_of(i * TILE, TILE), TILE)
            keys[at, :] = dot_nt(tall[at, :], wall[left, :]).astype(BF16)
            return 0

        lax.fori_loop(0, seq_len // TILE, tile, 0)

    def gq_copy(n):
        span = BLOCK * heads
        at = pl.ds(pl.multiple_of(n * span, span), span)
        return pltpu.make_async_copy(gq4.at[at, :], gq_out.at[at, :], gq_store.at[0])

    def gv_copy(n):
        span = BLOCK * heads * parts
        at = pl.ds(pl.multiple_of(n * span, span), span)
        return pltpu.make_async_copy(gv8.at[at, :], gv_out.at[at, :], gv_store.at[0])

    def query_block(n):
        at = pl.ds(pl.multiple_of(n * BLOCK, BLOCK), BLOCK)
        cosine, sine = cosv[at, :], sinv[at, :]
        for h in range(heads):
            kc, vc = slice(h * kw, (h + 1) * kw), slice(h * vw, (h + 1) * vw)
            key = keys[at, kc].astype(F32)
            rk = ((key * cosine + pltpu.roll(key, half, 1) * sine) * factor).astype(BF16)
            q, v, c = rq[at, kc], vals[at, vc], call[at, vc]
            state = entering[h]
            grad = dot_nn(mix[at, h * BLOCK:(h + 1) * BLOCK], rk)
            grad = grad + rising[h] * dot_nt(c, state.astype(BF16))
            xs[pl.ds(h, BLOCK, stride=heads), :] = (
                grad * cosine - pltpu.roll(grad, half, 1) * sine
            )
            scores = (dot_nt(q, rk) * within[h]).astype(BF16)
            fall = falling[h]
            inner = dot_tn(scores, c)
            outer = dot_nn(rk, held[h * nblocks + n])
            for i in range(parts):
                lane = slice(i * LANES, (i + 1) * LANES)
                ys[pl.ds(i * heads + h, BLOCK, stride=heads * parts), :] = (
                    inner[:, lane] + fall * outer[:, lane]
                )
            decayed = (rk.astype(F32) * fall).astype(BF16)
            entering[h] = state * carry[h, 0:1, :] + dot_tn(decayed, v)
        span = BLOCK * heads
        gq4[pl.ds(pl.multiple_of(n * span, span), span), :] = xs[...].astype(BF16)
        span = BLOCK * heads * parts
        gv8[pl.ds(pl.multiple_of(n * span, span), span), :] = ys[...].astype(BF16)
        gq_copy(n).start()
        gv_copy(n).start()

    def gather_keys():
        received(gkall.at[:, :(nsp - 1) * feats], gk_recv.at[0])
        gkall[:, pl.ds(pl.multiple_of(s * feats, feats), feats)] = gk[
            pl.ds(pl.multiple_of(s * rows, rows), rows), :
        ]
        for zb in range(nz):
            @pl.when((zb != s) & (zb != tardy))
            def _():
                pair_wait(zb)

    def gt_copy(i):
        at = pl.ds(pl.multiple_of(i * TILE, TILE), TILE)
        return pltpu.make_async_copy(gt.at[:, at], gt_out.at[:, at], gt_store.at[0])

    def block_product(zb, at):
        inner = pl.ds(pl.multiple_of(zb * feats, feats), feats)
        return dot_nn(gkall[:, inner], wall[inner, at])

    def token_gradient(i):
        at = pl.ds(pl.multiple_of(i * TILE, TILE), TILE)
        total = block_product((tardy + 1) % nz, at)
        for j in range(2, nz):
            total = total + block_product((tardy + j) % nz, at)
        gtf[i] = total

    def complete(i):
        at = pl.ds(pl.multiple_of(i * TILE, TILE), TILE)
        gt[:, at] = (gtf[i] + block_product(tardy, at)).astype(BF16)
        gt_copy(i).start()

    last = nchunks + 1 + (nz - 1) * HOP + 2 * CAST

    def turn(t, _):
        @pl.when(t < nchunks)
        def _():
            token_wait(t, 2, 0)
            token_send(t, 4).start()
            token_send(t, 5).start()

        @pl.when(t + 2 < nchunks)
        def _():
            for i in range(4):
                token_send(t + 2, i).start()

        @pl.when((t >= 1) & (t <= nchunks))
        def _():
            gradient_columns(t - 1)

        j = t - 2 - behind * HOP

        @pl.when((j >= 0) & (j < nchunks))
        def _():
            sum_line(j)

        jx = t - 2 - far * HOP - CAST

        @pl.when((jx >= 0) & (jx < nchunks))
        def _():
            cast_side(jx)

        jd = t - 2 - far * HOP - 2 * CAST

        @pl.when((jd >= 0) & (jd < nchunks))
        def _():
            cast_across(jd)

        @pl.when((t >= nchunks) & (t < nchunks + heads))
        def _():
            gk_send_head(t - nchunks)

        beat, on_beat = t // unit, t % unit == 0

        for p in range(pieces):
            when = jnp.where(patient, sum_step, sends[p]) if p == pieces - 1 else sends[p]

            @pl.when(t == when)
            def _():
                relay_inward(p)

            when = jnp.where(awaits, sum_step + 4, takes[p]) if p == pieces - 1 else takes[p]

            @pl.when(t == when)
            def _():
                take_inward(p)

        after = t - nchunks - 1
        slot = after // 2
        on_slot = (after >= 0) & (after < 2 * pieces) & (after % 2 == 0)
        ahead = jnp.where(opposite, beat - pieces, beat - 2)

        @pl.when(on_beat & (ahead >= 0) & (ahead < pieces))
        def _():
            @pl.when(opposite)
            def _():
                relay_third(ahead)

            @pl.when(jnp.logical_not(opposite))
            def _():
                relay_second(ahead)

        @pl.when(on_slot)
        def _():
            @pl.when(opposite)
            def _():
                relay_second(slot)

            @pl.when(jnp.logical_not(opposite))
            def _():
                relay_third(slot)

        @pl.when(t == unit * (pieces + 2))
        def _():
            relay_rest()

        @pl.when(after == 0)
        def _():
            make_keys()

        @pl.when((after >= 1) & (after <= nblocks // 2))
        def _():
            query_block(2 * after - 2)
            query_block(2 * after - 1)

        i = t - tile_step

        @pl.when(i == 0)
        def _():
            gather_keys()

        @pl.when((i >= 0) & (i < ntiles // 2))
        def _():
            token_gradient(2 * i)
            token_gradient(2 * i + 1)

        @pl.when(t == last - 3)
        def _():
            take_side()

        @pl.when(t == last - 2)
        def _():
            @pl.when(tardy != s)
            def _():
                pair_wait(tardy)

        @pl.when((t == last - 2) | (t == last - 1))
        def _():
            first = (t - (last - 2)) * (ntiles // 2)
            for i in range(ntiles // 2):
                complete(first + i)

        return 0

    ntiles = width // TILE
    tile_step = nchunks + 5
    unit = nchunks // 8
    sends = [unit * p for p in range(pieces)]
    takes = [unit * (2 * p + 3) for p in range(pieces)]
    sum_step = nchunks + 1 + HOP
    outer = (s == 0) | (s == nz - 1)
    patient = outer & (behind == 1) & jnp.logical_not(owner)
    awaits = outer & (behind == 2) & jnp.logical_not(owner)
    lax.fori_loop(0, last + 1, turn, 0)
    @pl.when(on_x | on_y)
    def _():
        received(fin.at[:nchunks // 2], cast_recv.at[nchunks])

    gw_copy = pltpu.make_async_copy(fin, gw_out, gw_store.at[0])
    gw_copy.start()

    sent(cotv.at[:, :(nsp - 1) * cwidth], cot_send.at[0])
    sent(tall.at[:6 * hrows, :], tok_send.at[0])
    sent(gk.at[:(nsp - 1) * rows, :], gk_sent.at[0])
    sent(pwo, half_send.at[0])

    @pl.when(jnp.logical_not(owner))
    def _():
        sent(lsend, line_send.at[0])

    @pl.when(owner | on_d)
    def _():
        sent(fin, cast_send.at[0])

    @pl.when(on_x | on_y)
    def _():
        sent(fin.at[:nchunks // 2], cast_send.at[0])

    for d in range(nz - 1):
        @pl.when(goes_up(d))
        def _():
            sent(wall.at[:wrows, :], up_send.at[d])

        @pl.when(goes_down(d))
        def _():
            sent(wall.at[:wrows, :], down_send.at[d])

    sent(wall.at[:nz * wrows, :], pair_send.at[0])

    @pl.when(side_x | side_y)
    def _():
        sent(wall.at[:wrows // 2, :], side_send.at[0])

    pltpu.make_async_copy(gq4, gq_out, gq_store.at[0]).wait()
    pltpu.make_async_copy(gv8, gv_out, gv_store.at[0]).wait()
    pltpu.make_async_copy(gt, gt_out, gt_store.at[0]).wait()
    gw_copy.wait()


def whole(tokens, weight, queries, values, cotan, decay, nsp, ndp, heads):
    nz = ndp // CORES
    rows, width = tokens.shape
    wrows = weight.shape[0]
    seq_len = rows * nsp
    kw = queries.shape[1]
    feats = heads * kw
    cwidth = cotan.shape[1] // nsp
    vw = cwidth // heads
    nblocks = seq_len // BLOCK
    nchunks = width // COLS
    cosine, sine = rotation_tables(seq_len, kw // 2)
    dma = pltpu.SemaphoreType.DMA
    anywhere = pl.BlockSpec(memory_space=pl.ANY)

    def buffer(*shape):
        return pltpu.VMEM(shape, BF16)

    def wide(*shape):
        return pltpu.VMEM(shape, F32)

    return pl.pallas_call(
        functools.partial(whole_kernel, nsp, nz, heads),
        in_specs=[pl.BlockSpec(memory_space=pltpu.SMEM)] + [anywhere] * 7,
        out_specs=[anywhere] * 4,
        out_shape=[
            jax.ShapeDtypeStruct((rows, width), BF16),
            jax.ShapeDtypeStruct(queries.shape, BF16),
            jax.ShapeDtypeStruct(values.shape, BF16),
            jax.ShapeDtypeStruct((nchunks, wrows, COLS), BF16),
        ],
        scratch_shapes=[
            buffer(rows, nsp * cwidth),
            buffer(seq_len, width),
            buffer(wrows * ndp, width),
            buffer(seq_len, cwidth),
            buffer(*queries.shape),
            buffer(*values.shape),
            wide(seq_len, kw),
            wide(seq_len, kw),
            buffer(seq_len, feats),
            buffer(seq_len, cwidth),
            buffer(seq_len, heads * BLOCK),
            buffer(heads * nblocks, kw, vw),
            buffer(seq_len, feats),
            buffer(feats, seq_len),
            buffer(rows, nsp * feats),
            buffer(seq_len, feats),
            buffer(*queries.shape),
            buffer(*values.shape),
            buffer(rows, width),
            wide(width // TILE, rows, TILE),
            wide(nchunks, wrows, COLS),
            buffer(nchunks, wrows, COLS),
            buffer(nchunks, wrows, COLS),
            buffer(2, nchunks, wrows, COLS),
            buffer(nchunks, wrows, COLS),
            buffer(nchunks, wrows, COLS),
            wide(BLOCK * heads, kw),
            wide(BLOCK * heads * (vw // LANES), LANES),
            wide(heads, BLOCK, BLOCK),
            wide(heads, BLOCK, kw),
            wide(heads, BLOCK, kw),
            wide(heads, 8, vw),
            wide(heads, kw, vw),
            dma((8,)),
            dma((1,)), dma(((nsp - 1) * heads,)),
            dma((1,)), dma((2 * nchunks,)),
            dma((nz - 1,)), dma(((nz - 1) * heads,)),
            dma((nz - 1,)), dma(((nz - 1) * heads,)),
            dma((1,)), dma((nz,)),
            dma((1,)), dma((1,)),
            dma((1,)), dma((1,)),
            dma((1,)), dma((nchunks,)),
            dma((1,)), dma((2 * nchunks,)),
            dma((1,)), dma((nchunks + 1,)),
            dma((1,)), dma((1,)), dma((1,)), dma((1,)),
        ],
        compiler_params=pltpu.CompilerParams(
            has_side_effects=True, vmem_limit_bytes=VMEM_LIMIT, collective_id=0
        ),
        name="whole",
    )(decay, tokens, weight, queries, values, cotan, jnp.asarray(cosine), jnp.asarray(sine))


def finish_kernel(gt, gq, gv, gw, gt_out, gq_out, gv_out, gw_out, bt, bq, bv, bw, bf, get, put):
    chunks, wrows = gw.shape[:2]
    reads, writes = [], []
    for source, held, target, count in (
        (gw, bw, None, 2), (gv, bv, gv_out, 4), (gq, bq, gq_out, 2), (gt, bt, gt_out, 2)
    ):
        axis = source.shape[0] // count
        for i in range(count):
            at = pl.ds(i * axis, axis)
            n = len(reads)
            reads.append(pltpu.make_async_copy(source.at[at], held.at[at], get.at[n]))
            if target is not None:
                writes.append(pltpu.make_async_copy(held.at[at], target.at[at], put.at[n]))
            else:
                into = pl.ds(i * axis * COLS, axis * COLS)
                writes.append(pltpu.make_async_copy(bf.at[:, into], gw_out.at[:, into], put.at[n]))
    for read in reads:
        read.start()
    for n, (read, write) in enumerate(zip(reads, writes)):
        read.wait()
        if n < 2:
            for j in range(n * chunks // 2, (n + 1) * chunks // 2):
                bf[:, j * COLS:(j + 1) * COLS] = bw[j].astype(F32)
        write.start()
    for write in writes:
        write.wait()


def finish(gt, gq, gv, gw):
    chunks, wrows, cols = gw.shape
    arrays = [gt, gq, gv, gw]
    total = (wrows, chunks * cols)
    anywhere = pl.BlockSpec(memory_space=pl.ANY)
    return pl.pallas_call(
        finish_kernel,
        in_specs=[anywhere] * 4,
        out_specs=[anywhere] * 4,
        out_shape=[jax.ShapeDtypeStruct(array.shape, BF16) for array in arrays[:3]]
        + [jax.ShapeDtypeStruct(total, F32)],
        scratch_shapes=[pltpu.VMEM(array.shape, BF16) for array in arrays]
        + [pltpu.VMEM(total, F32), pltpu.SemaphoreType.DMA((10,)), pltpu.SemaphoreType.DMA((10,))],
        compiler_params=pltpu.CompilerParams(vmem_limit_bytes=VMEM_LIMIT),
        name="finish",
    )(gt, gq, gv, gw)


def gather_general(tokens, weight, cotan):
    gathered = lax.all_gather(weight, "dp", axis=0, tiled=True)
    rows = gathered.shape[0] // lax.axis_size("sp")
    chosen = lax.dynamic_slice_in_dim(gathered, lax.axis_index("sp") * rows, rows)
    return (
        lax.all_gather(tokens, "sp", axis=0, tiled=True),
        chosen,
        lax.all_to_all(cotan, "sp", split_axis=1, concat_axis=0, tiled=True),
    )


def scatter_general(partial_tokens, partial_weight):
    grad_tokens = lax.psum_scatter(
        partial_tokens, "sp", scatter_dimension=0, tiled=True
    ).astype(BF16)
    owned = lax.psum_scatter(
        partial_weight, "dp", scatter_dimension=0, tiled=True
    )
    everything = lax.all_gather(owned, ("sp", "dp"), axis=0, tiled=True)
    rows = everything.shape[0] // lax.axis_size("dp")
    return grad_tokens, lax.dynamic_slice_in_dim(
        everything, lax.axis_index("dp") * rows, rows
    )


def body(nsp, ndp, tokens, key_weight, queries, values, cotangent, log_decay):
    seq_len, heads, kw = queries.shape[1:]
    vw = values.shape[3]
    if nsp == 4 and ndp == CORES * nsp and kw == BLOCK:
        parts = vw // LANES
        flat = values.reshape(seq_len, heads, parts, LANES).transpose(0, 2, 1, 3)
        grad_tokens, grad_query, grad_value, weight_grad = whole(
            tokens[0], key_weight, queries.reshape(-1, kw), flat.reshape(-1, LANES),
            cotangent[0], log_decay, nsp, ndp, heads,
        )
        grad_tokens, grad_query, grad_value, weight_grad = finish(
            grad_tokens, grad_query, grad_value, weight_grad
        )
        grad_value = grad_value.reshape(seq_len, parts, heads, LANES).transpose(0, 2, 1, 3)
    else:
        all_tokens, weight, cotan = gather_general(tokens[0], key_weight, cotangent[0])
        keys = dot_nt(all_tokens, weight).astype(BF16)
        grad_query, grad_key, _, grad_value = retention_backward(
            queries.reshape(seq_len, -1), keys, values.reshape(seq_len, -1), cotan, log_decay, heads
        )
        grad_tokens, weight_grad = scatter_general(
            dot_nn(grad_key, weight), dot_tn(grad_key, all_tokens)
        )
    return (
        grad_tokens[None],
        grad_query.reshape(queries.shape),
        grad_value.reshape(values.shape),
        weight_grad,
    )


def solution(mesh):
    return jax.shard_map(
        functools.partial(body, mesh.shape["sp"], mesh.shape["dp"]),
        mesh=mesh,
        in_specs=(
            P("dp", "sp", None),
            P("dp", None),
            P("dp", None, "sp", None),
            P("dp", None, "sp", None),
            P("dp", "sp", None),
            P(),
        ),
        out_specs=(
            P("dp", "sp", None),
            P("dp", None, "sp", None),
            P("dp", None, "sp", None),
            P("dp", None),
        ),
        check_vma=False,
    )
```

```python
import functools

import jax
import jax.numpy as jnp
import numpy as np
from jax import lax
from jax.experimental import pallas as pl
from jax.experimental.pallas import tpu as pltpu
from jax.sharding import PartitionSpec as P

BLOCK = 128
CORES = 2
MESH = pl.DeviceIdType.MESH
F32 = jnp.float32
BF16 = jnp.bfloat16
VMEM_LIMIT = 60 * 1024 * 1024


def rotation_tables(seq_len, half):
    position = np.arange(seq_len, dtype=np.float32)
    frequency = (10000.0 ** (-np.arange(half, dtype=np.float32) / half)).astype(np.float32)
    angle = (position[:, None] * frequency[None, :]).astype(np.float32)
    cosine, sine = np.cos(angle), np.sin(angle)
    return (
        np.concatenate([cosine, cosine], axis=1).astype(np.float32),
        np.concatenate([-sine, sine], axis=1).astype(np.float32),
    )


def dot_nt(a, b):
    return lax.dot_general(a, b, (((1,), (1,)), ((), ())), preferred_element_type=F32)


def dot_tn(a, b):
    return lax.dot_general(a, b, (((0,), (0,)), ((), ())), preferred_element_type=F32)


def dot_nn(a, b):
    return lax.dot_general(a, b, (((1,), (0,)), ((), ())), preferred_element_type=F32)


def retention_kernel(
    decay_ref, q_ref, k_ref, v_ref, c_ref, cos_ref, sin_ref,
    gq_ref, gk_ref, gkt_ref, gv_ref, rq_ref, rk_ref, mix_ref,
):
    seq_len, key_width = q_ref.shape
    value_width = v_ref.shape[1]
    nblocks = seq_len // BLOCK
    half = key_width // 2
    factor = key_width ** (-0.5)
    decay = decay_ref[lax.axis_index("sp") * pl.num_programs(0) + pl.program_id(0)]
    row = lax.broadcasted_iota(jnp.int32, (BLOCK, BLOCK), 0).astype(F32)
    col = lax.broadcasted_iota(jnp.int32, (BLOCK, BLOCK), 1).astype(F32)
    within = jnp.where(row >= col, jnp.exp(jnp.maximum(row - col, 0.0) * decay), 0.0)
    inside = lax.broadcasted_iota(jnp.int32, (BLOCK, key_width), 0).astype(F32)
    rising = jnp.exp((inside + 1.0) * decay)
    falling = jnp.exp((BLOCK - 1.0 - inside) * decay)
    wide = lax.broadcasted_iota(jnp.int32, (BLOCK, value_width), 0).astype(F32)
    falling_wide = jnp.exp((BLOCK - 1.0 - wide) * decay)
    carry_decay = jnp.exp(jnp.full((key_width, value_width), BLOCK * 1.0, F32) * decay)
    zero = jnp.zeros((key_width, value_width), F32)

    def forward(n, entering):
        rows = pl.ds(pl.multiple_of(n * BLOCK, BLOCK), BLOCK)
        cosine, sine = cos_ref[rows, :], sin_ref[rows, :]
        q = q_ref[rows, :].astype(F32)
        k = k_ref[rows, :].astype(F32)
        rq = (q * cosine + pltpu.roll(q, half, 1) * sine).astype(BF16)
        rk = ((k * cosine + pltpu.roll(k, half, 1) * sine) * factor).astype(BF16)
        rq_ref[rows, :] = rq
        rk_ref[rows, :] = rk
        v, c = v_ref[rows, :], c_ref[rows, :]
        mixing = (dot_nt(c, v) * within).astype(BF16)
        mix_ref[rows, :] = mixing
        grad = dot_nn(mixing, rk) + rising * dot_nt(c, entering.astype(BF16))
        gq_ref[rows, :] = (grad * cosine - pltpu.roll(grad, half, 1) * sine).astype(BF16)
        decayed = (rk.astype(F32) * falling).astype(BF16)
        return entering * carry_decay + dot_tn(decayed, v)

    def backward(step, trailing):
        n = nblocks - 1 - step
        rows = pl.ds(pl.multiple_of(n * BLOCK, BLOCK), BLOCK)
        cosine, sine = cos_ref[rows, :], sin_ref[rows, :]
        rq, rk, mixing = rq_ref[rows, :], rk_ref[rows, :], mix_ref[rows, :]
        v, c = v_ref[rows, :], c_ref[rows, :]
        held = trailing.astype(BF16)
        scores = (dot_nt(rq, rk) * within).astype(BF16)
        grad = dot_tn(mixing, rq) + falling * dot_nt(v, held)
        back = (grad * cosine - pltpu.roll(grad, half, 1) * sine) * factor
        gk_ref[rows, :] = back.astype(BF16)
        gkt_ref[:, rows] = back.T.astype(BF16)
        gv_ref[rows, :] = (dot_tn(scores, c) + falling_wide * dot_nn(rk, held)).astype(BF16)
        decayed = (rq.astype(F32) * rising).astype(BF16)
        return trailing * carry_decay + dot_tn(decayed, c)

    unroll = min(nblocks, 8)
    lax.fori_loop(0, nblocks, forward, zero, unroll=unroll)
    lax.fori_loop(0, nblocks, backward, zero, unroll=unroll)


def retention_backward(queries, keys, values, cotan, decay, heads):
    seq_len = queries.shape[0]
    kw = queries.shape[1] // heads
    vw = values.shape[1] // heads
    cosine, sine = rotation_tables(seq_len, kw // 2)
    narrow = pl.BlockSpec((seq_len, kw), lambda h: (0, h))
    wide = pl.BlockSpec((seq_len, vw), lambda h: (0, h))
    table = pl.BlockSpec((seq_len, kw), lambda h: (0, 0))
    flops = 2 * seq_len * heads * BLOCK * (3 * kw + 2 * vw + 5 * vw)
    return pl.pallas_call(
        retention_kernel,
        grid=(heads,),
        in_specs=[pl.BlockSpec(memory_space=pltpu.SMEM), narrow, narrow, wide, wide, table, table],
        out_specs=[narrow, narrow, pl.BlockSpec((kw, seq_len), lambda h: (h, 0)), wide],
        out_shape=[
            jax.ShapeDtypeStruct(queries.shape, BF16),
            jax.ShapeDtypeStruct(queries.shape, BF16),
            jax.ShapeDtypeStruct(queries.shape[::-1], BF16),
            jax.ShapeDtypeStruct(values.shape, BF16),
        ],
        scratch_shapes=[
            pltpu.VMEM((seq_len, kw), BF16),
            pltpu.VMEM((seq_len, kw), BF16),
            pltpu.VMEM((seq_len, BLOCK), BF16),
        ],
        compiler_params=pltpu.CompilerParams(vmem_limit_bytes=VMEM_LIMIT),
        cost_estimate=pl.CostEstimate(
            flops=flops, bytes_accessed=8 * seq_len * heads * (kw + vw), transcendentals=0
        ),
        name="retention",
    )(decay, queries, keys, values, cotan, jnp.asarray(cosine), jnp.asarray(sine))


def remote(src, dst, send, recv, target):
    return pltpu.make_async_remote_copy(
        src_ref=src, dst_ref=dst, send_sem=send, recv_sem=recv,
        device_id=target, device_id_type=MESH,
    )


def greet(nsp, nz, s, z, core):
    barrier = pltpu.get_barrier_semaphore()
    others = [{"dp": z * CORES + 1 - core}]
    others += [{"sp": (s + j) % nsp} for j in range(1, nsp)]
    for other in others:
        pl.semaphore_signal(barrier, inc=1, device_id=other, device_id_type=MESH)

    @pl.when(z > 0)
    def _():
        below = {"dp": (z - 1) * CORES + core}
        pl.semaphore_signal(barrier, inc=1, device_id=below, device_id_type=MESH)

    @pl.when(z < nz - 1)
    def _():
        above = {"dp": (z + 1) * CORES + core}
        pl.semaphore_signal(barrier, inc=1, device_id=above, device_id_type=MESH)

    ends = jnp.where(z > 0, 1, 0) + jnp.where(z < nz - 1, 1, 0)
    pl.semaphore_wait(barrier, len(others) + ends)


TILE = 256
LANES = 128
COLS = 256
HOP = 2
CAST = 3


def whole_kernel(
    nsp, nz, heads,
    decay_ref, tok_in, w_in, q_in, v_in, cot_in, cos_in, sin_in,
    gt_out, gq_out, gv_out, gw_out,
    cotv, tall, wall, call, q4, v8, cosv, sinv, rq, vals, mix, held, gk, gkt, gkall,
    keys, gq4, gv8, gt, gtf, acc, pwo, rp, lrecv, lsend, fin, xs, ys,
    within, rising, falling, carry, entering,
    load, cot_send, cot_recv, tok_send, tok_recv,
    up_send, up_recv, down_send, down_recv, pair_send, pair_recv, side_send, side_recv,
    gk_sent, gk_recv, half_send, half_recv, line_send, line_recv,
    cast_send, cast_recv, gq_store, gv_store, gw_store, gt_store,
):
    s = lax.axis_index("sp")
    k = lax.axis_index("dp")
    z, core = k // CORES, k % CORES
    x, y = s % 2, s // 2
    xn, yn = y * 2 + (1 - x), (1 - y) * 2 + x
    diagonal = (1 - y) * 2 + (1 - x)
    partner = {"dp": z * CORES + 1 - core}
    up, down = {"dp": k + CORES}, {"dp": k - CORES}
    rows, width = tok_in.shape
    wrows = w_in.shape[0]
    seq_len, feats = gk.shape
    kw = feats // heads
    cwidth = call.shape[1]
    vw = cwidth // heads
    parts = vw // LANES
    nblocks = seq_len // BLOCK
    half = kw // 2
    factor = kw ** (-0.5)
    hrows = rows // 2
    nchunks = width // COLS
    pieces = heads
    prow = wrows // pieces

    far = jnp.maximum(z, nz - 1 - z)
    behind = jnp.where(z > s, nz - 1 - z, jnp.where(z < s, z, far))
    owner = z == s
    dx, dy = x != z % 2, y != z // 2
    on_x = dx & jnp.logical_not(dy)
    on_y = dy & jnp.logical_not(dx)
    on_d = dx & dy
    edge = (z == 0) | (z == nz - 1)
    corner = owner & edge
    side_x, side_y = on_x & edge, on_y & edge
    apart = jnp.maximum(z - s, s - z)
    opposite = apart == nz - 1
    yields_up = (s == 0) & (z == nz - 2)
    yields_down = (s == nz - 1) & (z == 1)
    farthest = jnp.where(z < nz // 2, nz - 1, 0)
    tardy = jnp.where(opposite, jnp.where(z == 0, nz - 2, 1), farthest)

    loads = [
        pltpu.make_async_copy(cot_in, cotv, load.at[0]),
        pltpu.make_async_copy(w_in, wall.at[pl.ds(pl.multiple_of(k * wrows, wrows), wrows), :], load.at[1]),
        pltpu.make_async_copy(tok_in, tall.at[pl.ds(pl.multiple_of(s * rows, rows), rows), :], load.at[2]),
        pltpu.make_async_copy(
            cot_in.at[:, pl.ds(pl.multiple_of(s * cwidth, cwidth), cwidth)],
            call.at[pl.ds(pl.multiple_of(s * rows, rows), rows), :], load.at[3],
        ),
        pltpu.make_async_copy(q_in, q4, load.at[4]),
        pltpu.make_async_copy(v_in, v8, load.at[5]),
        pltpu.make_async_copy(cos_in, cosv, load.at[6]),
        pltpu.make_async_copy(sin_in, sinv, load.at[7]),
    ]
    for copy in loads:
        copy.start()
    greet(nsp, nz, s, z, core)

    def received(ref, sem):
        remote(ref, ref, load.at[0], sem, partner).wait_recv()

    def sent(ref, sem):
        remote(ref, ref, sem, load.at[0], partner).wait_send()

    def cot_copy(j, h, source):
        peer = (s + j) % nsp
        columns = pl.ds(pl.multiple_of(peer * cwidth + h * vw, vw), vw)
        to = call.at[
            pl.ds(pl.multiple_of(source * rows, rows), rows), pl.ds(pl.multiple_of(h * vw, vw), vw)
        ]
        i = (j - 1) * heads + h
        return remote(cotv.at[:, columns], to, cot_send.at[0], cot_recv.at[i], {"sp": peer})

    loads[0].wait()
    for h in range(heads):
        for j in range(1, nsp):
            cot_copy(j, h, s).start()

    def piece(zb, c, p):
        start = pl.multiple_of((zb * CORES + c) * wrows + p * prow, prow)
        return wall.at[pl.ds(start, prow), :]

    def up_copy(d, p):
        ref, i = piece(z - d, core, p), d * pieces + p
        return remote(ref, ref, up_send.at[d], up_recv.at[i], up)

    def down_copy(d, p):
        ref, i = piece(z + d, core, p), d * pieces + p
        return remote(ref, ref, down_send.at[d], down_recv.at[i], down)

    def pair_copy(zb, p):
        ref = piece(zb, core, p)
        return remote(ref, ref, pair_send.at[0], pair_recv.at[zb], partner)

    def pair_wait(zb):
        received(wall.at[:wrows, :], pair_recv.at[zb])

    loads[1].wait()
    for p in range(pieces):
        @pl.when(z < nz - 1)
        def _():
            up_copy(0, p).start()

        @pl.when(z > 0)
        def _():
            down_copy(0, p).start()

        pair_copy(z, p).start()

    def goes_up(d):
        return (z >= d) & (z < nz - 1 if d < nz - 2 else (z < nz - 1) & (s != nz - 1))

    def goes_down(d):
        return (z + d < nz) & (z > 0 if d < nz - 2 else (z > 0) & (s != 0))

    def side_copy(p, part, target):
        zb = nz - 1 - z
        start = pl.multiple_of((zb * CORES + core) * wrows + p * prow + part * (prow // 2), prow // 2)
        ref = wall.at[pl.ds(start, prow // 2), :]
        return remote(ref, ref, side_send.at[0], side_recv.at[0], {"sp": target})

    def rise_of(d, p):
        received(piece(z - d, core, p), up_recv.at[(d - 1) * pieces + p])
        pair_copy(z - d, p).start()

    def fall_of(d, p):
        received(piece(z + d, core, p), down_recv.at[(d - 1) * pieces + p])
        pair_copy(z + d, p).start()

    def relay_first(p):
        @pl.when(z > 0)
        def _():
            rise_of(1, p)

        @pl.when(goes_up(1) & (z >= s) & prompt(p, yields_up))
        def _():
            up_copy(1, p).start()

        @pl.when(z < nz - 1)
        def _():
            fall_of(1, p)

        @pl.when(goes_down(1) & (z <= s) & prompt(p, yields_down))
        def _():
            down_copy(1, p).start()

    def relay_inward(p):
        @pl.when(goes_up(1) & (z < s))
        def _():
            up_copy(1, p).start()

        @pl.when(goes_down(1) & (z > s))
        def _():
            down_copy(1, p).start()

    def relay_second(p):
        @pl.when((z >= 2) & (z > s))
        def _():
            rise_of(2, p)

        @pl.when(goes_up(2) & (z > s))
        def _():
            up_copy(2, p).start()

        @pl.when((z + 2 < nz) & (z < s))
        def _():
            fall_of(2, p)

        @pl.when(goes_down(2) & (z < s))
        def _():
            down_copy(2, p).start()

    def take_inward(p):
        @pl.when((z >= 2) & (z <= s))
        def _():
            rise_of(2, p)

        @pl.when(goes_up(2) & (z == s))
        def _():
            up_copy(2, p).start()

        @pl.when((z + 2 < nz) & (z >= s))
        def _():
            fall_of(2, p)

        @pl.when(goes_down(2) & (z == s))
        def _():
            down_copy(2, p).start()

    def relay_third(p):
        @pl.when((z == nz - 1) & (s != z))
        def _():
            rise_of(3, p)

        @pl.when((z == 0) & (s != z))
        def _():
            fall_of(3, p)

        @pl.when(side_x)
        def _():
            side_copy(p, 0, xn).start()

        @pl.when(side_y)
        def _():
            side_copy(p, 1, yn).start()

    def prompt(p, yields):
        return jnp.logical_not(yields & (p > 0))

    def relay_rest():
        for p in range(1, pieces):
            @pl.when(yields_up)
            def _():
                up_copy(1, p).start()

            @pl.when(yields_down)
            def _():
                down_copy(1, p).start()

    def take_side():
        @pl.when(corner)
        def _():
            received(wall.at[:wrows, :], side_recv.at[0])
            for p in range(pieces):
                pair_copy(nz - 1 - z, p).start()

    def token(j, i, who, h, target):
        at = tall.at[
            pl.ds(pl.multiple_of(who * rows + h * hrows, hrows), hrows),
            pl.ds(pl.multiple_of(j * COLS, COLS), COLS),
        ]
        n = 2 * j + (0 if i < 2 else 1)
        return remote(at, at, tok_send.at[0], tok_recv.at[n], {"sp": target})

    def token_send(j, i):
        who, h, target = [
            (s, 0, xn), (s, 1, yn), (s, 1, xn), (s, 0, yn), (xn, 0, yn), (yn, 1, xn)
        ][i]
        return token(j, i, who, h, target)

    def token_wait(j, count, n):
        at = pl.ds(pl.multiple_of(j * COLS, COLS), COLS)
        received(tall.at[:count * hrows, at], tok_recv.at[2 * j + n])

    loads[2].wait()
    for j in range(2):
        for i in range(4):
            token_send(j, i).start()
    for copy in loads[3:]:
        copy.wait()

    def prepare(n, _):
        at = pl.ds(pl.multiple_of(n * BLOCK, BLOCK), BLOCK)
        cosine, sine = cosv[at, :], sinv[at, :]
        span = BLOCK * heads
        xs[...] = q4[pl.ds(pl.multiple_of(n * span, span), span), :].astype(F32)
        for h in range(heads):
            q = xs[pl.ds(h, BLOCK, stride=heads), :]
            rq[at, h * kw:(h + 1) * kw] = (q * cosine + pltpu.roll(q, half, 1) * sine).astype(BF16)
        span = BLOCK * heads * parts
        ys[...] = v8[pl.ds(pl.multiple_of(n * span, span), span), :].astype(F32)
        for h in range(heads):
            for i in range(parts):
                left = h * vw + i * LANES
                vals[at, left:left + LANES] = ys[
                    pl.ds(i * heads + h, BLOCK, stride=heads * parts), :
                ].astype(BF16)
        return 0

    lax.fori_loop(0, nblocks, prepare, 0)

    def key_head(h, _):
        relay_first(h)
        for j in range(1, nsp):
            cot_copy(j, h, (s - j + nsp) % nsp).wait_recv()
        kc = pl.ds(pl.multiple_of(h * kw, kw), kw)
        vc = pl.ds(pl.multiple_of(h * vw, vw), vw)
        decay = decay_ref[s * heads + h]
        row = lax.broadcasted_iota(jnp.int32, (BLOCK, BLOCK), 0).astype(F32)
        col = lax.broadcasted_iota(jnp.int32, (BLOCK, BLOCK), 1).astype(F32)
        inside = lax.broadcasted_iota(jnp.int32, (BLOCK, kw), 0).astype(F32)
        mask = jnp.where(row >= col, jnp.exp(jnp.maximum(row - col, 0.0) * decay), 0.0)
        rise = jnp.exp((inside + 1.0) * decay)
        fall = jnp.exp((BLOCK - 1.0 - inside) * decay)
        step = jnp.exp(jnp.full((8, vw), BLOCK * 1.0, F32) * decay)
        within[h] = mask
        rising[h] = rise
        falling[h] = fall
        carry[h] = step
        trailing = jnp.zeros((kw, vw), F32)
        for n in reversed(range(nblocks)):
            at = slice(n * BLOCK, (n + 1) * BLOCK)
            cosine, sine = cosv[at, :], sinv[at, :]
            q, v, c = rq[at, kc], vals[at, vc], call[at, vc]
            mixing = (dot_nt(c, v) * mask).astype(BF16)
            mix[at, pl.ds(pl.multiple_of(h * BLOCK, BLOCK), BLOCK)] = mixing
            trail = trailing.astype(BF16)
            held[h * nblocks + n] = trail
            grad = dot_tn(mixing, q) + fall * dot_nt(v, trail)
            back = (grad * cosine - pltpu.roll(grad, half, 1) * sine) * factor
            gk[at, kc] = back.astype(BF16)
            gkt[kc, at] = back.T.astype(BF16)
            decayed = (q.astype(F32) * rise).astype(BF16)
            trailing = trailing * step[0:1, :] + dot_tn(decayed, c)
        entering[h] = jnp.zeros((kw, vw), F32)
        return 0

    lax.fori_loop(0, heads, key_head, 0)

    def gk_send_head(h):
        for j in range(1, nsp):
            peer = (s + j) % nsp
            source = gk.at[
                pl.ds(pl.multiple_of(peer * rows, rows), rows),
                pl.ds(pl.multiple_of(h * kw, kw), kw),
            ]
            to = gkall.at[:, pl.ds(pl.multiple_of(s * feats + h * kw, kw), kw)]
            remote(source, to, gk_sent.at[0], gk_recv.at[0], {"sp": peer}).start()

    def half_copy(j):
        return remote(pwo.at[j], rp.at[j], half_send.at[0], half_recv.at[j], partner)

    def line_copy(j, side, target):
        return remote(
            lsend.at[j], lrecv.at[side, j], line_send.at[0],
            line_recv.at[side * nchunks + j], target,
        )

    def cast_copy(j, h, target, last_leg=False):
        ref = fin.at[j, pl.ds(h * (wrows // 2), wrows // 2), :]
        sem = cast_recv.at[nchunks if last_leg else j]
        return remote(ref, ref, cast_send.at[0], sem, {"sp": target})

    def cast_side(j):
        @pl.when(on_x)
        def _():
            received(fin.at[j, :wrows // 2, :], cast_recv.at[j])
            cast_copy(j, 0, yn).start()

        @pl.when(on_y)
        def _():
            received(fin.at[j, wrows // 2:, :], cast_recv.at[j])
            cast_copy(j, 1, xn).start()

    def cast_across(j):
        @pl.when(on_d)
        def _():
            received(fin.at[j], cast_recv.at[j])
            cast_copy(j, 0, xn, True).start()
            cast_copy(j, 1, yn, True).start()

    def gradient_columns(j):
        token_wait(j, 4, 1)
        at = pl.ds(pl.multiple_of(j * COLS, COLS), COLS)
        theirs = pl.ds(pl.multiple_of((1 - core) * wrows, wrows), wrows)
        mine = pl.ds(pl.multiple_of(core * wrows, wrows), wrows)
        pwo[j] = dot_nn(gkt[theirs, :], tall[:, at]).astype(BF16)
        half_copy(j).start()
        acc[j] = dot_nn(gkt[mine, :], tall[:, at])

    def sum_line(j):
        half_copy(j).wait_recv()
        acc[j] = acc[j] + rp[j].astype(F32)

        @pl.when((z >= s) & (z < nz - 1))
        def _():
            line_copy(j, 1, down).wait_recv()
            acc[j] = acc[j] + lrecv[1, j].astype(F32)

        @pl.when((z <= s) & (z > 0))
        def _():
            line_copy(j, 0, up).wait_recv()
            acc[j] = acc[j] + lrecv[0, j].astype(F32)

        @pl.when(owner)
        def _():
            fin[j] = acc[j].astype(BF16)
            cast_copy(j, 0, xn).start()
            cast_copy(j, 1, yn).start()

        @pl.when(jnp.logical_not(owner))
        def _():
            lsend[j] = acc[j].astype(BF16)

        @pl.when(z > s)
        def _():
            line_copy(j, 1, down).start()

        @pl.when(z < s)
        def _():
            line_copy(j, 0, up).start()

    def make_keys():
        pair_wait(s)
        left = pl.ds(pl.multiple_of(s * feats, feats), feats)

        def tile(i, _):
            at = pl.ds(pl.multiple_of(i * TILE, TILE), TILE)
            keys[at, :] = dot_nt(tall[at, :], wall[left, :]).astype(BF16)
            return 0

        lax.fori_loop(0, seq_len // TILE, tile, 0)

    def gq_copy(n):
        span = BLOCK * heads
        at = pl.ds(pl.multiple_of(n * span, span), span)
        return pltpu.make_async_copy(gq4.at[at, :], gq_out.at[at, :], gq_store.at[0])

    def gv_copy(n):
        span = BLOCK * heads * parts
        at = pl.ds(pl.multiple_of(n * span, span), span)
        return pltpu.make_async_copy(gv8.at[at, :], gv_out.at[at, :], gv_store.at[0])

    def query_block(n):
        at = pl.ds(pl.multiple_of(n * BLOCK, BLOCK), BLOCK)
        cosine, sine = cosv[at, :], sinv[at, :]
        for h in range(heads):
            kc, vc = slice(h * kw, (h + 1) * kw), slice(h * vw, (h + 1) * vw)
            key = keys[at, kc].astype(F32)
            rk = ((key * cosine + pltpu.roll(key, half, 1) * sine) * factor).astype(BF16)
            q, v, c = rq[at, kc], vals[at, vc], call[at, vc]
            state = entering[h]
            grad = dot_nn(mix[at, h * BLOCK:(h + 1) * BLOCK], rk)
            grad = grad + rising[h] * dot_nt(c, state.astype(BF16))
            xs[pl.ds(h, BLOCK, stride=heads), :] = (
                grad * cosine - pltpu.roll(grad, half, 1) * sine
            )
            scores = (dot_nt(q, rk) * within[h]).astype(BF16)
            fall = falling[h]
            inner = dot_tn(scores, c)
            outer = dot_nn(rk, held[h * nblocks + n])
            for i in range(parts):
                lane = slice(i * LANES, (i + 1) * LANES)
                ys[pl.ds(i * heads + h, BLOCK, stride=heads * parts), :] = (
                    inner[:, lane] + fall * outer[:, lane]
                )
            decayed = (rk.astype(F32) * fall).astype(BF16)
            entering[h] = state * carry[h, 0:1, :] + dot_tn(decayed, v)
        span = BLOCK * heads
        gq4[pl.ds(pl.multiple_of(n * span, span), span), :] = xs[...].astype(BF16)
        span = BLOCK * heads * parts
        gv8[pl.ds(pl.multiple_of(n * span, span), span), :] = ys[...].astype(BF16)
        gq_copy(n).start()
        gv_copy(n).start()

    def gather_keys():
        received(gkall.at[:, :(nsp - 1) * feats], gk_recv.at[0])
        gkall[:, pl.ds(pl.multiple_of(s * feats, feats), feats)] = gk[
            pl.ds(pl.multiple_of(s * rows, rows), rows), :
        ]
        for zb in range(nz):
            @pl.when((zb != s) & (zb != tardy))
            def _():
                pair_wait(zb)

    def gt_copy(i):
        at = pl.ds(pl.multiple_of(i * TILE, TILE), TILE)
        return pltpu.make_async_copy(gt.at[:, at], gt_out.at[:, at], gt_store.at[0])

    def block_product(zb, at):
        inner = pl.ds(pl.multiple_of(zb * feats, feats), feats)
        return dot_nn(gkall[:, inner], wall[inner, at])

    def token_gradient(i):
        at = pl.ds(pl.multiple_of(i * TILE, TILE), TILE)
        total = block_product((tardy + 1) % nz, at)
        for j in range(2, nz):
            total = total + block_product((tardy + j) % nz, at)
        gtf[i] = total

    def complete(i):
        at = pl.ds(pl.multiple_of(i * TILE, TILE), TILE)
        gt[:, at] = (gtf[i] + block_product(tardy, at)).astype(BF16)
        gt_copy(i).start()

    last = nchunks + 1 + (nz - 1) * HOP + 2 * CAST

    def turn(t, _):
        @pl.when(t < nchunks)
        def _():
            token_wait(t, 2, 0)
            token_send(t, 4).start()
            token_send(t, 5).start()

        @pl.when(t + 2 < nchunks)
        def _():
            for i in range(4):
                token_send(t + 2, i).start()

        @pl.when((t >= 1) & (t <= nchunks))
        def _():
            gradient_columns(t - 1)

        j = t - 2 - behind * HOP

        @pl.when((j >= 0) & (j < nchunks))
        def _():
            sum_line(j)

        jx = t - 2 - far * HOP - CAST

        @pl.when((jx >= 0) & (jx < nchunks))
        def _():
            cast_side(jx)

        jd = t - 2 - far * HOP - 2 * CAST

        @pl.when((jd >= 0) & (jd < nchunks))
        def _():
            cast_across(jd)

        @pl.when((t >= nchunks) & (t < nchunks + heads))
        def _():
            gk_send_head(t - nchunks)

        beat, on_beat = t // unit, t % unit == 0

        for p in range(pieces):
            when = jnp.where(patient, sum_step, sends[p]) if p == pieces - 1 else sends[p]

            @pl.when(t == when)
            def _():
                relay_inward(p)

            when = jnp.where(awaits, sum_step + 4, takes[p]) if p == pieces - 1 else takes[p]

            @pl.when(t == when)
            def _():
                take_inward(p)

        after = t - nchunks - 1
        slot = after // 2
        on_slot = (after >= 0) & (after < 2 * pieces) & (after % 2 == 0)
        ahead = jnp.where(opposite, beat - pieces, beat - 2)

        @pl.when(on_beat & (ahead >= 0) & (ahead < pieces))
        def _():
            @pl.when(opposite)
            def _():
                relay_third(ahead)

            @pl.when(jnp.logical_not(opposite))
            def _():
                relay_second(ahead)

        @pl.when(on_slot)
        def _():
            @pl.when(opposite)
            def _():
                relay_second(slot)

            @pl.when(jnp.logical_not(opposite))
            def _():
                relay_third(slot)

        @pl.when(t == unit * (pieces + 2))
        def _():
            relay_rest()

        @pl.when(after == 0)
        def _():
            make_keys()

        @pl.when((after >= 1) & (after <= nblocks // 2))
        def _():
            query_block(2 * after - 2)
            query_block(2 * after - 1)

        i = t - tile_step

        @pl.when(i == 0)
        def _():
            gather_keys()

        @pl.when((i >= 0) & (i < ntiles // 2))
        def _():
            token_gradient(2 * i)
            token_gradient(2 * i + 1)

        @pl.when(t == last - 3)
        def _():
            take_side()

        @pl.when(t == last - 2)
        def _():
            @pl.when(tardy != s)
            def _():
                pair_wait(tardy)

        @pl.when((t == last - 2) | (t == last - 1))
        def _():
            first = (t - (last - 2)) * (ntiles // 2)
            for i in range(ntiles // 2):
                complete(first + i)

        return 0

    ntiles = width // TILE
    tile_step = nchunks + 5
    unit = nchunks // 8
    sends = [unit * p for p in range(pieces)]
    takes = [unit * (3 + p + p // 2) for p in range(pieces)]
    sum_step = nchunks + 1 + HOP
    outer = (s == 0) | (s == nz - 1)
    patient = outer & (behind == 1) & jnp.logical_not(owner)
    awaits = outer & (behind == 2) & jnp.logical_not(owner)
    lax.fori_loop(0, last + 1, turn, 0)
    @pl.when(on_x | on_y)
    def _():
        received(fin.at[:nchunks // 2], cast_recv.at[nchunks])

    gw_copy = pltpu.make_async_copy(fin, gw_out, gw_store.at[0])
    gw_copy.start()

    sent(cotv.at[:, :(nsp - 1) * cwidth], cot_send.at[0])
    sent(tall.at[:6 * hrows, :], tok_send.at[0])
    sent(gk.at[:(nsp - 1) * rows, :], gk_sent.at[0])
    sent(pwo, half_send.at[0])

    @pl.when(jnp.logical_not(owner))
    def _():
        sent(lsend, line_send.at[0])

    @pl.when(owner | on_d)
    def _():
        sent(fin, cast_send.at[0])

    @pl.when(on_x | on_y)
    def _():
        sent(fin.at[:nchunks // 2], cast_send.at[0])

    for d in range(nz - 1):
        @pl.when(goes_up(d))
        def _():
            sent(wall.at[:wrows, :], up_send.at[d])

        @pl.when(goes_down(d))
        def _():
            sent(wall.at[:wrows, :], down_send.at[d])

    sent(wall.at[:nz * wrows, :], pair_send.at[0])

    @pl.when(side_x | side_y)
    def _():
        sent(wall.at[:wrows // 2, :], side_send.at[0])

    pltpu.make_async_copy(gq4, gq_out, gq_store.at[0]).wait()
    pltpu.make_async_copy(gv8, gv_out, gv_store.at[0]).wait()
    pltpu.make_async_copy(gt, gt_out, gt_store.at[0]).wait()
    gw_copy.wait()


def whole(tokens, weight, queries, values, cotan, decay, nsp, ndp, heads):
    nz = ndp // CORES
    rows, width = tokens.shape
    wrows = weight.shape[0]
    seq_len = rows * nsp
    kw = queries.shape[1]
    feats = heads * kw
    cwidth = cotan.shape[1] // nsp
    vw = cwidth // heads
    nblocks = seq_len // BLOCK
    nchunks = width // COLS
    cosine, sine = rotation_tables(seq_len, kw // 2)
    dma = pltpu.SemaphoreType.DMA
    anywhere = pl.BlockSpec(memory_space=pl.ANY)

    def buffer(*shape):
        return pltpu.VMEM(shape, BF16)

    def wide(*shape):
        return pltpu.VMEM(shape, F32)

    return pl.pallas_call(
        functools.partial(whole_kernel, nsp, nz, heads),
        in_specs=[pl.BlockSpec(memory_space=pltpu.SMEM)] + [anywhere] * 7,
        out_specs=[anywhere] * 4,
        out_shape=[
            jax.ShapeDtypeStruct((rows, width), BF16),
            jax.ShapeDtypeStruct(queries.shape, BF16),
            jax.ShapeDtypeStruct(values.shape, BF16),
            jax.ShapeDtypeStruct((nchunks, wrows, COLS), BF16),
        ],
        scratch_shapes=[
            buffer(rows, nsp * cwidth),
            buffer(seq_len, width),
            buffer(wrows * ndp, width),
            buffer(seq_len, cwidth),
            buffer(*queries.shape),
            buffer(*values.shape),
            wide(seq_len, kw),
            wide(seq_len, kw),
            buffer(seq_len, feats),
            buffer(seq_len, cwidth),
            buffer(seq_len, heads * BLOCK),
            buffer(heads * nblocks, kw, vw),
            buffer(seq_len, feats),
            buffer(feats, seq_len),
            buffer(rows, nsp * feats),
            buffer(seq_len, feats),
            buffer(*queries.shape),
            buffer(*values.shape),
            buffer(rows, width),
            wide(width // TILE, rows, TILE),
            wide(nchunks, wrows, COLS),
            buffer(nchunks, wrows, COLS),
            buffer(nchunks, wrows, COLS),
            buffer(2, nchunks, wrows, COLS),
            buffer(nchunks, wrows, COLS),
            buffer(nchunks, wrows, COLS),
            wide(BLOCK * heads, kw),
            wide(BLOCK * heads * (vw // LANES), LANES),
            wide(heads, BLOCK, BLOCK),
            wide(heads, BLOCK, kw),
            wide(heads, BLOCK, kw),
            wide(heads, 8, vw),
            wide(heads, kw, vw),
            dma((8,)),
            dma((1,)), dma(((nsp - 1) * heads,)),
            dma((1,)), dma((2 * nchunks,)),
            dma((nz - 1,)), dma(((nz - 1) * heads,)),
            dma((nz - 1,)), dma(((nz - 1) * heads,)),
            dma((1,)), dma((nz,)),
            dma((1,)), dma((1,)),
            dma((1,)), dma((1,)),
            dma((1,)), dma((nchunks,)),
            dma((1,)), dma((2 * nchunks,)),
            dma((1,)), dma((nchunks + 1,)),
            dma((1,)), dma((1,)), dma((1,)), dma((1,)),
        ],
        compiler_params=pltpu.CompilerParams(
            has_side_effects=True, vmem_limit_bytes=VMEM_LIMIT, collective_id=0
        ),
        name="whole",
    )(decay, tokens, weight, queries, values, cotan, jnp.asarray(cosine), jnp.asarray(sine))


def finish_kernel(gt, gq, gv, gw, gt_out, gq_out, gv_out, gw_out, bt, bq, bv, bw, bf, get, put):
    chunks, wrows = gw.shape[:2]
    reads, writes = [], []
    for source, held, target, count in (
        (gw, bw, None, 2), (gv, bv, gv_out, 4), (gq, bq, gq_out, 2), (gt, bt, gt_out, 2)
    ):
        axis = source.shape[0] // count
        for i in range(count):
            at = pl.ds(i * axis, axis)
            n = len(reads)
            reads.append(pltpu.make_async_copy(source.at[at], held.at[at], get.at[n]))
            if target is not None:
                writes.append(pltpu.make_async_copy(held.at[at], target.at[at], put.at[n]))
            else:
                into = pl.ds(i * axis * COLS, axis * COLS)
                writes.append(pltpu.make_async_copy(bf.at[:, into], gw_out.at[:, into], put.at[n]))
    for read in reads:
        read.start()
    for n, (read, write) in enumerate(zip(reads, writes)):
        read.wait()
        if n < 2:
            for j in range(n * chunks // 2, (n + 1) * chunks // 2):
                bf[:, j * COLS:(j + 1) * COLS] = bw[j].astype(F32)
        write.start()
    for write in writes:
        write.wait()


def finish(gt, gq, gv, gw):
    chunks, wrows, cols = gw.shape
    arrays = [gt, gq, gv, gw]
    total = (wrows, chunks * cols)
    anywhere = pl.BlockSpec(memory_space=pl.ANY)
    return pl.pallas_call(
        finish_kernel,
        in_specs=[anywhere] * 4,
        out_specs=[anywhere] * 4,
        out_shape=[jax.ShapeDtypeStruct(array.shape, BF16) for array in arrays[:3]]
        + [jax.ShapeDtypeStruct(total, F32)],
        scratch_shapes=[pltpu.VMEM(array.shape, BF16) for array in arrays]
        + [pltpu.VMEM(total, F32), pltpu.SemaphoreType.DMA((10,)), pltpu.SemaphoreType.DMA((10,))],
        compiler_params=pltpu.CompilerParams(vmem_limit_bytes=VMEM_LIMIT),
        name="finish",
    )(gt, gq, gv, gw)


def gather_general(tokens, weight, cotan):
    gathered = lax.all_gather(weight, "dp", axis=0, tiled=True)
    rows = gathered.shape[0] // lax.axis_size("sp")
    chosen = lax.dynamic_slice_in_dim(gathered, lax.axis_index("sp") * rows, rows)
    return (
        lax.all_gather(tokens, "sp", axis=0, tiled=True),
        chosen,
        lax.all_to_all(cotan, "sp", split_axis=1, concat_axis=0, tiled=True),
    )


def scatter_general(partial_tokens, partial_weight):
    grad_tokens = lax.psum_scatter(
        partial_tokens, "sp", scatter_dimension=0, tiled=True
    ).astype(BF16)
    owned = lax.psum_scatter(
        partial_weight, "dp", scatter_dimension=0, tiled=True
    )
    everything = lax.all_gather(owned, ("sp", "dp"), axis=0, tiled=True)
    rows = everything.shape[0] // lax.axis_size("dp")
    return grad_tokens, lax.dynamic_slice_in_dim(
        everything, lax.axis_index("dp") * rows, rows
    )


def body(nsp, ndp, tokens, key_weight, queries, values, cotangent, log_decay):
    seq_len, heads, kw = queries.shape[1:]
    vw = values.shape[3]
    if nsp == 4 and ndp == CORES * nsp and kw == BLOCK:
        parts = vw // LANES
        flat = values.reshape(seq_len, heads, parts, LANES).transpose(0, 2, 1, 3)
        grad_tokens, grad_query, grad_value, weight_grad = whole(
            tokens[0], key_weight, queries.reshape(-1, kw), flat.reshape(-1, LANES),
            cotangent[0], log_decay, nsp, ndp, heads,
        )
        grad_tokens, grad_query, grad_value, weight_grad = finish(
            grad_tokens, grad_query, grad_value, weight_grad
        )
        grad_value = grad_value.reshape(seq_len, parts, heads, LANES).transpose(0, 2, 1, 3)
    else:
        all_tokens, weight, cotan = gather_general(tokens[0], key_weight, cotangent[0])
        keys = dot_nt(all_tokens, weight).astype(BF16)
        grad_query, grad_key, _, grad_value = retention_backward(
            queries.reshape(seq_len, -1), keys, values.reshape(seq_len, -1), cotan, log_decay, heads
        )
        grad_tokens, weight_grad = scatter_general(
            dot_nn(grad_key, weight), dot_tn(grad_key, all_tokens)
        )
    return (
        grad_tokens[None],
        grad_query.reshape(queries.shape),
        grad_value.reshape(values.shape),
        weight_grad,
    )


def solution(mesh):
    return jax.shard_map(
        functools.partial(body, mesh.shape["sp"], mesh.shape["dp"]),
        mesh=mesh,
        in_specs=(
            P("dp", "sp", None),
            P("dp", None),
            P("dp", None, "sp", None),
            P("dp", None, "sp", None),
            P("dp", "sp", None),
            P(),
        ),
        out_specs=(
            P("dp", "sp", None),
            P("dp", None, "sp", None),
            P("dp", None, "sp", None),
            P("dp", None),
        ),
        check_vma=False,
    )
```
